128 devices in a mesh: sp: 32 (over z, y, core), tp: 4 (over x).
Axes of the slice: x: 4, y: 4, z: 4, core: 2. Of those that a mesh axis runs over, the one named last changes fastest.
Arguments:
- middle_stream: bfloat16 [6144, 2048], P('sp', 'tp'), may hold values from -6 to 6
- output_gradient: bfloat16 [6144, 2048], P('sp', 'tp'), may hold values from -6 to 6
- routes: int32 [6144, 2], P('sp'), may hold values from 0 to 31, all different within a row; in each aligned block of 192 rows (0 to 191, 192 to 383, ...) at most 18 rows name the same one
- chosen_expert_weight: float32 [6144, 2], P('sp'), may hold values from 0.2 to 1
- expert_gate_weight: bfloat16 [32, 2048, 3584], P('sp', None, 'tp'), may hold values from -0.125 to 0.125
- expert_up_weight: bfloat16 [32, 2048, 3584], P('sp', None, 'tp'), may hold values from -0.125 to 0.125
- expert_down_weight: bfloat16 [32, 3584, 2048], P('sp', 'tp'), may hold values from -0.09375 to 0.09375
- recurrent_output_weight: bfloat16 [2048, 1024], P(None, 'tp'), may hold values from -0.1875 to 0.1875
- recurrence_input: bfloat16 [6144, 1024], P('sp', 'tp'), may hold values from -8 to 8
- output_gate_logits: bfloat16 [6144, 1024], P('sp', 'tp'), may hold values from -6 to 6
- recurrence_gate_weight: bfloat16 [8, 128, 128], replicated, may hold values from -0.5 to 0.5
- input_gate_weight: bfloat16 [8, 128, 128], replicated, may hold values from -0.5 to 0.5
- channel_decay_param: float32 [1024], P('tp'), may hold values from 4 to 13
- extra_log_decay: float32 [6144, 1024], P('sp', 'tp'), may hold values from -0.7 to 0
Outputs:
- grad_gate: bfloat16 [32, 2048, 3584], P('sp', None, 'tp')
- grad_up: bfloat16 [32, 2048, 3584], P('sp', None, 'tp')
- grad_down: bfloat16 [32, 3584, 2048], P('sp', 'tp')
- grad_out_proj: float32 [2048, 1024], P('sp', 'tp')
- grad_input: float32 [6144, 1024], P('sp', 'tp')
- grad_gate_pre: float32 [6144, 1024], P('sp', 'tp')
The draws below stay inside these ranges and needn't reach their ends.
Inputs may be any that keep to these rules, and one draw needn't show every extreme that they name: `routes`: in the rows of one index of sp no expert is named more than 18 times, a bound that some block reaches in some of them; the entries of a row differ.
All inputs are finite; a program needn't handle non-finite values.
Results may differ from the reference program's by a relative error of at most 0.017.
Values may be sent and summed in bfloat16 or wider, within the bound.
A program may use at most 128 MiB of HBM per device.

```python
import math
import jax
import jax.numpy as jnp
import numpy as np
from jax import lax

D = 2048
FF = 3584
BLOCKS = 8
BW = 128
TOP = 2
TOK_DEV = 192
CHANNEL_COUNT = 1024
SEQUENCE_TOKENS = 6144
EXPERTS = 32
CAP = 18
N_SP = 32
N_TP = 4


def draw_recurrence_input(key, part):
    initial_key, second_key = jax.random.split(jax.random.fold_in(key, 11))
    base_draw = jnp.clip(jax.random.normal(initial_key, (SEQUENCE_TOKENS, CHANNEL_COUNT), jnp.float32), -4.0, 4.0)
    factor = jnp.exp(jax.random.uniform(second_key, (SEQUENCE_TOKENS // TOK_DEV, 1, 1), jnp.float32, math.log(0.5), math.log(2.0)))
    scaled = (base_draw.reshape(SEQUENCE_TOKENS // TOK_DEV, TOK_DEV, CHANNEL_COUNT) * factor).reshape(SEQUENCE_TOKENS, CHANNEL_COUNT)
    return scaled.astype(jnp.bfloat16)


def draw_channel_decay_param(key, part):
    initial_key, second_key, third_key = jax.random.split(jax.random.fold_in(key, 23), 3)
    fast_share = 0.5
    fast_pick = jax.random.uniform(initial_key, (CHANNEL_COUNT,), jnp.float32) < fast_share
    fast_rate = jnp.exp(jax.random.uniform(second_key, (CHANNEL_COUNT,), jnp.float32, math.log(0.003), math.log(0.01)))
    slow_rate = jnp.exp(jax.random.uniform(third_key, (CHANNEL_COUNT,), jnp.float32, math.log(0.05), math.log(0.3))) / SEQUENCE_TOKENS
    chosen = jnp.where(fast_pick, fast_rate, slow_rate)
    return (-jnp.log(jnp.expm1(chosen))).astype(jnp.float32)


def draw_extra_log_decay(key, part):
    initial_key, second_key = jax.random.split(jax.random.fold_in(key, 37))
    spike_mask = jax.random.uniform(initial_key, (SEQUENCE_TOKENS, CHANNEL_COUNT), jnp.float32) < 4.0 / SEQUENCE_TOKENS
    loss_history = jax.random.uniform(second_key, (SEQUENCE_TOKENS, CHANNEL_COUNT), jnp.float32, math.log(0.5), math.log(0.8))
    return jnp.where(spike_mask, loss_history, 0.0).astype(jnp.float32)


def strengthened(array, key, source, target, shards_of, factor):
    owner, partner = [(jnp.arange(array.shape[axis_at]) // (array.shape[axis_at] // shards_of)).reshape([-1 if axis == axis_at else 1 for axis in range(array.ndim)]) for axis_at in (source, target)]
    chosen = jax.random.permutation(key, shards_of)[partner]
    strong = (owner == chosen) | (owner == (partner + shards_of // 2) % shards_of)
    return jnp.where(strong, factor * array, array)


def steps_of(key, shape, cuts, smallest, top_value):
    loudness = 1.0
    for axis_at, shards_of in cuts:
        draws = jax.random.uniform(jax.random.fold_in(jax.random.fold_in(key, 6), axis_at), (shards_of,), jnp.float32, smallest / len(cuts), top_value / len(cuts))
        loudness = loudness * jnp.repeat(jnp.exp(draws), shape[axis_at] // shards_of).reshape((-1,) + (1,) * (len(shape) - 1 - axis_at))
    return loudness


def shared_out(key, own, number, rows, number_of, top, reach, skew):
    ranking = jax.random.permutation(key, number_of)
    heavy_load, ordinary = portions_of(number_of, rows * top, reach, skew, True), portions_of(number_of, rows * top, reach, skew, False)
    places = jnp.arange(number_of)

    def named(tallies, turn):
        used = int((tallies > 0).sum())
        fixed = max(1, used // 4)
        shifted = fixed + (places - fixed + turn * (used - fixed)) % max(1, number_of - fixed)
        return jnp.zeros((number_of,), jnp.int32).at[ranking[jnp.where(places < fixed, places, shifted)]].set(jnp.asarray(tallies, jnp.int32))

    tallies = jnp.where(number % 4 == 0, named(heavy_load, number // 4), named(ordinary, number - number // 4 - 1))
    mixed = jax.random.permutation(jax.random.fold_in(own, 3), number_of)
    source_of, taker = mixed[0:number_of // 2 * 2:2], mixed[1:number_of // 2 * 2:2]
    slack = jnp.minimum(tallies[source_of] - 1, reach - tallies[taker]) // 2
    slack = jnp.where((source_of == ranking[0]) | (taker == ranking[0]) | (tallies[taker] == 0), 0, jnp.maximum(slack, 0))
    shifted = jax.random.randint(jax.random.fold_in(own, 4), (number_of // 2,), 0, 1 << 20) % (slack + 1)
    tallies = tallies.at[source_of].add(-shifted).at[taker].add(shifted)
    labels = jnp.searchsorted(jnp.cumsum(tallies), jnp.arange(rows * top), side="right").astype(jnp.int32)
    listing = labels.reshape(top, rows).T
    listing = listing[jax.random.permutation(jax.random.fold_in(own, 1), rows)]
    turn = jax.random.randint(jax.random.fold_in(own, 2), (rows, 1), 0, top)
    return jnp.take_along_axis(listing, (jnp.arange(top)[None, :] + turn) % top, axis=1)


def portions_of(amount, total, bound, slope, full):
    portions = [(1 << 20) // math.isqrt(grade ** slope) + 1 for grade in range(1, amount + 1)]
    largest = bound if full else min(bound, max(-(-total // amount), total * portions[0] // sum(portions)))
    least = 1 if total - largest >= amount - 1 else 0
    holding, spare = [largest] + [least] * (amount - 1), total - largest - least * (amount - 1)
    while spare > 0:
        candidates = [i for i in range(1, amount) if holding[i] < largest] or [i for i in range(1, amount) if holding[i] < bound]
        whole, budget = sum([portions[i] for i in candidates]), spare
        for i in candidates:
            more = min(bound - holding[i], max(1, budget * portions[i] // whole), spare)
            holding[i] = holding[i] + more
            spare = spare - more
    return np.array(holding)


def bell_draw(stream_key, dims, width, bound, cuts=(), kind=jnp.bfloat16):
    array = jax.random.normal(stream_key, dims, jnp.float32) * width
    if len(cuts) > 0:
        array = steps_of(stream_key, dims, cuts, -0.22, 0.18) * array
    return jnp.clip(array, min=-bound, max=bound).astype(kind)


def noise_with(rng, dims, width, most, cuts, heavy, kind=jnp.bfloat16):
    array = width * jax.random.normal(rng, dims, jnp.float32)
    if cuts:
        array = array * steps_of(rng, dims, cuts, -0.22, 0.18)
    return jnp.clip(strengthened(array, jax.random.fold_in(rng, 3), *heavy), -most, most).astype(kind)


def setup_inputs(seed: int = 0) -> dict:
    streams_of = jax.random.split(jax.random.key(seed), 15)
    middle_stream = bell_draw(streams_of[0], (SEQUENCE_TOKENS, D), 1.0, 6.0, ((0, 32), (1, 4)))
    output_gradient = noise_with(streams_of[1], (SEQUENCE_TOKENS, D), 1.0, 6.0, ((0, 32), (1, 4)), (0, 1, 32, 2.75))
    routes_keys = jax.random.split(jax.random.fold_in(streams_of[2], 1), SEQUENCE_TOKENS // TOK_DEV)
    routes_turns = jax.random.permutation(jax.random.fold_in(streams_of[2], 3), SEQUENCE_TOKENS // TOK_DEV)
    routes = jax.vmap(lambda own, number: shared_out(jax.random.fold_in(streams_of[2], 2), own, number, TOK_DEV, EXPERTS, TOP, CAP, 1))(routes_keys, routes_turns).reshape((SEQUENCE_TOKENS, TOP))
    chosen_expert_weight = jnp.clip(0.2 + 0.8 * jax.random.uniform(streams_of[3], (SEQUENCE_TOKENS, TOP), jnp.float32) ** steps_of(streams_of[3], (SEQUENCE_TOKENS, TOP), ((0, 32),), -0.2, 0.2), 0.2, 1.0)
    expert_gate_weight = bell_draw(streams_of[4], (EXPERTS, D, FF), D ** -0.5, 0.125, ((0, 32), (2, 4)))
    expert_up_weight = bell_draw(streams_of[5], (EXPERTS, D, FF), D ** -0.5, 0.125, ((0, 32), (2, 4)))
    expert_down_weight = bell_draw(streams_of[6], (EXPERTS, FF, D), FF ** -0.5, 0.09375, ((0, 32), (1, 4)))
    recurrent_output_weight = bell_draw(streams_of[7], (D, CHANNEL_COUNT), CHANNEL_COUNT ** -0.5, 0.1875, ((1, 4),))
    recurrence_input = draw_recurrence_input(jax.random.fold_in(streams_of[14], 71), 0)
    output_gate_logits = bell_draw(streams_of[9], (SEQUENCE_TOKENS, CHANNEL_COUNT), 1.0, 6.0, ((0, 32), (1, 4)))
    recurrence_gate_weight = bell_draw(streams_of[10], (BLOCKS, BW, BW), BW ** -0.5, 0.5)
    input_gate_weight = bell_draw(streams_of[11], (BLOCKS, BW, BW), BW ** -0.5, 0.5)
    channel_decay_param = draw_channel_decay_param(jax.random.fold_in(streams_of[14], 71), 0)
    extra_log_decay = draw_extra_log_decay(jax.random.fold_in(streams_of[14], 71), 0)
    return {"middle_stream": middle_stream, "output_gradient": output_gradient, "routes": routes, "chosen_expert_weight": chosen_expert_weight, "expert_gate_weight": expert_gate_weight, "expert_up_weight": expert_up_weight, "expert_down_weight": expert_down_weight, "recurrent_output_weight": recurrent_output_weight, "recurrence_input": recurrence_input, "output_gate_logits": output_gate_logits, "recurrence_gate_weight": recurrence_gate_weight, "input_gate_weight": input_gate_weight, "channel_decay_param": channel_decay_param, "extra_log_decay": extra_log_decay}


def combine_linear(earlier, latter):
    return (earlier[0] * latter[0], latter[0] * earlier[1] + latter[1])

def linear_scan(factor, driven):
    return lax.associative_scan(combine_linear, (factor, driven), axis=0)

def gelu_parts(output_gate_logits):
    gate_float = output_gate_logits.astype(jnp.float32)
    return jax.jvp(jax.nn.gelu, (gate_float,), (jnp.ones_like(gate_float),))

def expert_backward(inputs, cotangent, gate_weight, up_weight, down_weight):
    gate_act = jnp.dot(inputs, gate_weight, preferred_element_type=jnp.float32)
    up_act = jnp.dot(inputs, up_weight, preferred_element_type=jnp.float32)
    sigmoid_gate = jax.nn.sigmoid(gate_act)
    silu_act = gate_act * sigmoid_gate
    hidden = (silu_act * up_act).astype(jnp.bfloat16)
    d_hidden = lax.dot_general(cotangent, down_weight, (((1,), (1,)), ((), ())), preferred_element_type=jnp.float32)
    grad_down = lax.dot_general(hidden, cotangent, (((0,), (0,)), ((), ())), preferred_element_type=jnp.float32)
    d_gate = (d_hidden * up_act * sigmoid_gate * (1.0 + gate_act * (1.0 - sigmoid_gate))).astype(jnp.bfloat16)
    d_up = (d_hidden * silu_act).astype(jnp.bfloat16)
    grad_gate = lax.dot_general(inputs, d_gate, (((0,), (0,)), ((), ())), preferred_element_type=jnp.float32)
    grad_up = lax.dot_general(inputs, d_up, (((0,), (0,)), ((), ())), preferred_element_type=jnp.float32)
    return (grad_gate.astype(jnp.bfloat16), grad_up.astype(jnp.bfloat16), grad_down.astype(jnp.bfloat16), d_gate, d_up)

def reference(middle_stream, output_gradient, routes, chosen_expert_weight, expert_gate_weight, expert_up_weight, expert_down_weight, recurrent_output_weight, recurrence_input, output_gate_logits, recurrence_gate_weight, input_gate_weight, channel_decay_param, extra_log_decay):
    tokens, model_width = middle_stream.shape
    top_count = routes.shape[1]
    routed = routes.reshape(-1)
    onehot = (routed[:, None] == jnp.arange(EXPERTS, dtype=jnp.int32)[None, :]).astype(jnp.int32)
    onehot = onehot.reshape(N_SP, TOK_DEV * top_count, EXPERTS)
    slot_rank = (lax.optimization_barrier(jnp.sum(jnp.cumsum(onehot, axis=1) * onehot, axis=2)) - 1).reshape(-1)
    source = jnp.arange(tokens * top_count, dtype=jnp.int32) // (TOK_DEV * top_count)
    buffer_place = (source * CAP + slot_rank).astype(jnp.int32)
    slot_table = jnp.full((EXPERTS, N_SP * CAP), tokens * top_count, jnp.int32)
    slot_table = slot_table.at[routed, buffer_place].set(jnp.arange(tokens * top_count, dtype=jnp.int32))
    zero_row = jnp.zeros((1, model_width), jnp.bfloat16)
    pair_rows = jnp.broadcast_to(middle_stream[:, None, :], (tokens, top_count, model_width)).reshape(-1, model_width)
    pair_rows = jnp.concatenate([pair_rows, zero_row], axis=0)
    pair_cot = (chosen_expert_weight[:, :, None] * output_gradient.astype(jnp.float32)[:, None, :]).astype(jnp.bfloat16)
    pair_cot = jnp.concatenate([pair_cot.reshape(-1, model_width), zero_row], axis=0)

    def one_expert(packed):
        table_row, gate_weight, up_weight, down_weight = packed
        inputs = pair_rows[table_row]
        cotangent = pair_cot[table_row]
        grad_gate, grad_up, grad_down, d_gate, d_up = expert_backward(inputs, cotangent, gate_weight, up_weight, down_weight)
        slot_rows = inputs.shape[0]
        quarter = gate_weight.shape[1] // N_TP
        gate_q = d_gate.astype(jnp.float32).reshape(slot_rows, N_TP, quarter)
        up_q = d_up.astype(jnp.float32).reshape(slot_rows, N_TP, quarter)
        gate_wq = gate_weight.astype(jnp.float32).reshape(model_width, N_TP, quarter)
        up_wq = up_weight.astype(jnp.float32).reshape(model_width, N_TP, quarter)
        partial_value = jnp.einsum('rqf,dqf->qrd', gate_q, gate_wq) + jnp.einsum('rqf,dqf->qrd', up_q, up_wq)
        rounded = lax.optimization_barrier(partial_value.astype(jnp.bfloat16)).astype(jnp.float32)
        slot_grad = lax.optimization_barrier(jnp.sum(rounded, axis=0)).astype(jnp.bfloat16)
        return (grad_gate, grad_up, grad_down, slot_grad)
    grad_gate, grad_up, grad_down, slot_grad = lax.map(one_expert, (slot_table, expert_gate_weight, expert_up_weight, expert_down_weight))
    slot_back = jnp.zeros((tokens * top_count + 1, model_width), jnp.bfloat16)
    slot_back = slot_back.at[slot_table.reshape(-1)].set(slot_grad.reshape(-1, model_width))
    arrived = slot_back[:-1].astype(jnp.float32).reshape(tokens, top_count, model_width)
    residual_grad = (output_gradient.astype(jnp.float32) + lax.optimization_barrier(jnp.sum(arrived, axis=1))).astype(jnp.bfloat16)
    mixer_grad = jnp.dot(residual_grad, recurrent_output_weight, preferred_element_type=jnp.float32)
    channels = recurrence_input.shape[1]
    blocks, block_width = (recurrence_gate_weight.shape[0], recurrence_gate_weight.shape[1])
    u_float = recurrence_input.astype(jnp.float32)
    u_blocks = u_float.reshape(tokens, blocks, block_width)
    forget_gate = jax.nn.sigmoid(jnp.einsum('tnb,nbc->tnc', u_blocks, recurrence_gate_weight.astype(jnp.float32)).reshape(tokens, channels))
    admit_gate = jax.nn.sigmoid(jnp.einsum('tnb,nbc->tnc', u_blocks, input_gate_weight.astype(jnp.float32)).reshape(tokens, channels))
    baseline_rate = jax.nn.softplus(-channel_decay_param)
    decay_logarithm = -8.0 * forget_gate * baseline_rate[None, :] + extra_log_decay
    decay_step = jnp.exp(decay_logarithm)
    input_scale = jnp.sqrt(-jnp.expm1(2.0 * decay_logarithm))
    driven = u_float * admit_gate * input_scale
    _, states = linear_scan(decay_step, driven)
    prev_states = jnp.concatenate([jnp.zeros((1, channels), jnp.float32), states[:-1]], axis=0)
    gelu_val, gelu_der = gelu_parts(output_gate_logits)
    lru_out = (states * gelu_val).astype(jnp.bfloat16)
    grad_out_proj = lax.dot_general(residual_grad, lru_out, (((0,), (0,)), ((), ())), preferred_element_type=jnp.float32)
    grad_gate_pre = mixer_grad * states * gelu_der
    state_in = mixer_grad * gelu_val
    next_decay = jnp.concatenate([decay_step[1:], jnp.zeros((1, channels), jnp.float32)], axis=0)
    _, flipped = linear_scan(next_decay[::-1], state_in[::-1])
    state_grad = flipped[::-1]
    d_log = state_grad * (prev_states * decay_step - u_float * admit_gate * decay_step * decay_step / input_scale)
    d_recall = (d_log * (-8.0 * baseline_rate[None, :]) * forget_gate * (1.0 - forget_gate)).astype(jnp.bfloat16)
    d_admit = (state_grad * u_float * input_scale * admit_gate * (1.0 - admit_gate)).astype(jnp.bfloat16)
    back_recall = jnp.einsum('tnc,nbc->tnb', d_recall.astype(jnp.float32).reshape(tokens, blocks, block_width), recurrence_gate_weight.astype(jnp.float32))
    back_admit = jnp.einsum('tnc,nbc->tnb', d_admit.astype(jnp.float32).reshape(tokens, blocks, block_width), input_gate_weight.astype(jnp.float32))
    grad_input = state_grad * admit_gate * input_scale + (back_recall + back_admit).reshape(tokens, channels)
    return (grad_gate, grad_up, grad_down, grad_out_proj, grad_input, grad_gate_pre)
```

```python
import functools

import jax
import jax.numpy as jnp
from jax import lax
from jax.experimental import pallas as pl
from jax.experimental.pallas import tpu as pltpu
from jax.sharding import PartitionSpec as P

BF16 = jnp.bfloat16
F32 = jnp.float32
MESH = pl.DeviceIdType.MESH
LANE = 128
MAIN = 16


def mm(a, b, ca=1, cb=0):
    return lax.dot_general(a, b, (((ca,), (cb,)), ((), ())), preferred_element_type=F32)


def iota(shape, dim):
    return lax.broadcasted_iota(jnp.int32, shape, dim).astype(F32)


def copy_to(src, dst, send_sem, recv_sem, sp, tp):
    return pltpu.make_async_remote_copy(
        src_ref=src,
        dst_ref=dst,
        send_sem=send_sem,
        recv_sem=recv_sem,
        device_id=(sp, tp),
        device_id_type=MESH,
    )


def greet(targets):
    barrier = pltpu.get_barrier_semaphore()
    for sp, tp in targets:
        pl.semaphore_signal(barrier, inc=1, device_id=(sp, tp), device_id_type=MESH)


def met(count):
    pl.semaphore_wait(pltpu.get_barrier_semaphore(), count)


def shifted(value, by, fill, row):
    rows = value.shape[0]
    if by > 0:
        return jnp.where(row >= by, pltpu.roll(value, by, 0), fill)
    return jnp.where(row < rows + by, pltpu.roll(value, rows + by, 0), fill)


def scan_rows(gain, value, sign):
    rows = value.shape[0]
    row = lax.broadcasted_iota(jnp.int32, value.shape, 0)
    step = 1
    while step < rows:
        value = value + gain * shifted(value, sign * step, 0.0, row)
        gain = gain * shifted(gain, sign * step, 1.0, row)
        step *= 2
    return gain, value


def log1p_of(z):
    series = z * (1.0 - z * (0.5 - z * (1.0 / 3.0 - z * (0.25 - z * (0.2 - z / 6.0)))))
    return jnp.where(z < 0.03, series, jnp.log(1.0 + z))


def one_less_exp(y):
    part = 1.0 + y / 7.0
    for k in (6.0, 5.0, 4.0, 3.0, 2.0):
        part = 1.0 + (y / k) * part
    return jnp.where(y > -0.5, -y * part, 1.0 - jnp.exp(y))


def gelu_both(x):
    c = 0.7978845608028654
    t = jnp.tanh(c * (x + 0.044715 * x * x * x))
    value = 0.5 * x * (1.0 + t)
    slope = 0.5 * (1.0 + t) + 0.5 * x * (1.0 - t * t) * c * (1.0 + 3.0 * 0.044715 * x * x)
    return value, slope


def dispatch_kernel(
    n_sp,
    x_ref,
    g_ref,
    rt_ref,
    wt_ref,
    u_ref,
    ogl_ref,
    wr_ref,
    wi_ref,
    cdp_ref,
    eld_ref,
    rows_ref,
    cot_ref,
    rec_ref,
    lru_ref,
    gain_ref,
    send,
    recv,
    ext,
    stat,
    stats,
    d_send,
    d_recv,
    own_sem,
    r_send,
    l_send,
    y_send,
    fl_recv,
    fr_recv,
    ff_recv,
    s_send,
    s_recv,
):
    me, tp = lax.axis_index("sp"), lax.axis_index("tp")
    right, left, far = (lax.rem(tp + k, 4) for k in (1, 3, 2))
    tokens, feat = x_ref.shape
    extra = 2
    groups = 8
    per = n_sp // groups
    greet([(lax.rem(me + d, n_sp), tp) for d in range(1, n_sp)] + [(me, right), (me, left)])

    r0 = rt_ref[0:1, :].astype(F32)
    r1 = rt_ref[1:2, :].astype(F32)
    w0 = wt_ref[0:1, :]
    w1 = wt_ref[1:2, :]
    expert = iota((n_sp, tokens), 0)
    h0 = expert == r0
    h1 = expert == r1
    held = (h0 | h1).astype(F32).astype(BF16)
    before = (iota((tokens, tokens), 0) < iota((tokens, tokens), 1)).astype(F32).astype(BF16)
    rank = mm(held, before)
    k0 = jnp.sum(jnp.where(h0, rank, 0.0), axis=0, keepdims=True)
    k1 = jnp.sum(jnp.where(h1, rank, 0.0), axis=0, keepdims=True)
    m0 = jnp.where(k0 < MAIN, r0 * MAIN + k0, -1.0)
    m1 = jnp.where(k1 < MAIN, r1 * MAIN + k1, -1.0)
    e0 = jnp.where(k0 < MAIN, -1.0, r0 * extra + k0 - MAIN)
    e1 = jnp.where(k1 < MAIN, -1.0, r1 * extra + k1 - MAIN)
    x = x_ref[...]
    g = g_ref[...]
    block = 128
    for at in range(0, n_sp * MAIN, block):
        slot = iota((block, tokens), 0) + float(at)
        p0 = slot == m0
        p1 = slot == m1
        pick = (p0 | p1).astype(F32).astype(BF16)
        weight = jnp.sum(jnp.where(p0, w0, 0.0) + jnp.where(p1, w1, 0.0), axis=1, keepdims=True)
        send[at : at + block, 0:feat] = mm(pick, x).astype(BF16)
        send[at : at + block, feat : 2 * feat] = (mm(pick, g) * weight).astype(BF16)
    slot = iota((n_sp * extra, tokens), 0)
    p0 = slot == e0
    p1 = slot == e1
    pick = (p0 | p1).astype(F32).astype(BF16)
    weight = jnp.sum(jnp.where(p0, w0, 0.0) + jnp.where(p1, w1, 0.0), axis=1, keepdims=True)
    ex = mm(pick, x)
    eg = mm(pick, g) * weight
    cuts = feat // LANE
    for b in range(cuts):
        ext[pl.ds(b, n_sp * extra, stride=2 * cuts), :] = ex[:, b * LANE : (b + 1) * LANE]
        ext[pl.ds(cuts + b, n_sp * extra, stride=2 * cuts), :] = eg[:, b * LANE : (b + 1) * LANE]
    send[:, 2 * feat : 2 * feat + LANE] = ext[...].astype(BF16)

    met(n_sp + 1)

    def dispatch(peer, sem):
        return copy_to(
            send.at[pl.ds(pl.multiple_of(peer * MAIN, MAIN), MAIN)],
            recv.at[tp, pl.ds(pl.multiple_of(me * MAIN, MAIN), MAIN)],
            d_send.at[sem],
            d_recv.at[me],
            peer,
            tp,
        )

    def arrival(source):
        return copy_to(
            send.at[pl.ds(0, MAIN)],
            recv.at[tp, pl.ds(pl.multiple_of(source * MAIN, MAIN), MAIN)],
            d_send.at[0],
            d_recv.at[source],
            source,
            tp,
        )

    own = pltpu.make_async_copy(
        send.at[pl.ds(pl.multiple_of(me * MAIN, MAIN), MAIN)],
        recv.at[tp, pl.ds(pl.multiple_of(me * MAIN, MAIN), MAIN)],
        own_sem,
    )
    own.start()
    sends = [dispatch(lax.rem(me + n_sp - d, n_sp), d) for d in range(1, n_sp)]
    for s in sends:
        s.start()

    u = u_ref[...]
    uf = u.astype(F32)
    blocks = u.shape[1] // LANE
    pre_r = []
    pre_i = []
    for b in range(blocks):
        ub = u[:, b * LANE : (b + 1) * LANE]
        pre_r.append(mm(ub, wr_ref[tp * blocks + b]))
        pre_i.append(mm(ub, wi_ref[tp * blocks + b]))
    forget = jax.nn.sigmoid(jnp.concatenate(pre_r, axis=1))
    admit = jax.nn.sigmoid(jnp.concatenate(pre_i, axis=1))
    p = cdp_ref[...]
    base = jnp.maximum(-p, 0.0) + log1p_of(jnp.exp(-jnp.abs(p)))
    log_decay = -8.0 * forget * base + eld_ref[...]
    decay = jnp.exp(log_decay)
    scale = jnp.sqrt(one_less_exp(2.0 * log_decay))
    gain, local = scan_rows(decay, uf * admit * scale, 1)
    stat[0, 0:1, :] = gain[tokens - 1 : tokens, :]
    stat[0, 1:2, :] = local[tokens - 1 : tokens, :]
    stats[me, 0:1, :] = gain[tokens - 1 : tokens, :]
    stats[me, 1:2, :] = local[tokens - 1 : tokens, :]
    told = [
        copy_to(
            stat.at[0], stats.at[me], s_send.at[d], s_recv.at[me], lax.rem(me + n_sp - d, n_sp), tp
        )
        for d in range(1, n_sp)
    ]
    for s in told:
        s.start()

    size = per * MAIN
    g0 = me // per

    def span(i):
        start = lax.rem(g0 + i, groups) * size
        return pl.ds(pl.multiple_of(start, size), size)

    def pass_on(quarter, i, send_sem, recv_sem, to):
        return copy_to(
            recv.at[quarter, span(i)], recv.at[quarter, span(i)], send_sem, recv_sem, me, to
        )

    started = []

    def relay(i):
        if i % 2 == 0:
            pass_on(left, i, l_send.at[i], fl_recv.at[i], right).wait_recv()
            c = pass_on(left, i, y_send.at[i], ff_recv.at[i], right)
        else:
            pass_on(right, i, r_send.at[i], fr_recv.at[i], left).wait_recv()
            c = pass_on(right, i, y_send.at[i], ff_recv.at[i], left)
        c.start()
        started.append(c)

    for i in range(groups):
        if i == 0:
            own.wait()
        for k in range(per):
            source = lax.rem(g0 + i, groups) * per + k
            if i == 0:

                @pl.when(source != me)
                def _():
                    arrival(source).wait_recv()
            else:
                arrival(source).wait_recv()
        for c in (
            pass_on(tp, i, r_send.at[i], fl_recv.at[i], right),
            pass_on(tp, i, l_send.at[i], fr_recv.at[i], left),
        ):
            c.start()
            started.append(c)
        if i > 0:
            relay(i - 1)

    for d in range(1, n_sp):
        source = lax.rem(me + d, n_sp)
        copy_to(stat.at[0], stats.at[source], s_send.at[0], s_recv.at[source], source, tp).wait_recv()
    carry = jnp.zeros((1, u.shape[1]), F32)
    for s in range(n_sp):
        carry = jnp.where(s < me, stats[s, 0:1, :] * carry + stats[s, 1:2, :], carry)
    gain_ref[...] = stats[...]
    states = local + gain * carry
    row = lax.broadcasted_iota(jnp.int32, states.shape, 0)
    prev = jnp.where(row == 0, carry, pltpu.roll(states, 1, 0))
    gelu, slope = gelu_both(ogl_ref[...].astype(F32))
    lru_ref[...] = (states * gelu).astype(BF16)
    rec_ref[0] = decay
    rec_ref[1] = gelu
    rec_ref[2] = states * slope
    rec_ref[3] = admit * scale
    rec_ref[4] = (
        (prev * decay - uf * admit * decay * decay / scale) * (-8.0 * base) * forget * (1.0 - forget)
    )
    rec_ref[5] = uf * scale * admit * (1.0 - admit)

    relay(groups - 1)
    for i in range(groups):
        if i % 2 == 1:
            pass_on(left, i, l_send.at[i], fl_recv.at[i], right).wait_recv()
        else:
            pass_on(right, i, r_send.at[i], fr_recv.at[i], left).wait_recv()
    for i in range(groups):
        pass_on(far, i, y_send.at[i], ff_recv.at[i], right).wait_recv()

    for q in range(4):
        rows_ref[0 : n_sp * MAIN, q * feat : (q + 1) * feat] = recv[q, :, 0:feat]
        cot_ref[0 : n_sp * MAIN, q * feat : (q + 1) * feat] = recv[q, :, feat : 2 * feat]
        ext[...] = recv[q, :, 2 * feat : 2 * feat + LANE].astype(F32)
        for b in range(cuts):
            at = q * feat + b * LANE
            rows_ref[n_sp * MAIN :, at : at + LANE] = ext[
                pl.ds(b, n_sp * extra, stride=2 * cuts), :
            ].astype(BF16)
            cot_ref[n_sp * MAIN :, at : at + LANE] = ext[
                pl.ds(cuts + b, n_sp * extra, stride=2 * cuts), :
            ].astype(BF16)

    for c in sends + told + started:
        c.wait_send()


def dispatch(n_sp, x, g, rt, wt, u, ogl, wr, wi, cdp, eld):
    tokens, feat = x.shape
    chans = u.shape[1]
    slots = n_sp * (MAIN + 2)
    width = 2 * feat + LANE
    vmem = pl.BlockSpec(memory_space=pltpu.VMEM)
    dma = pltpu.SemaphoreType.DMA
    return pl.pallas_call(
        functools.partial(dispatch_kernel, n_sp),
        out_shape=(
            jax.ShapeDtypeStruct((slots, 4 * feat), BF16),
            jax.ShapeDtypeStruct((slots, 4 * feat), BF16),
            jax.ShapeDtypeStruct((6, tokens, chans), F32),
            jax.ShapeDtypeStruct((tokens, chans), BF16),
            jax.ShapeDtypeStruct((n_sp, 2, chans), F32),
        ),
        in_specs=[vmem] * 10,
        out_specs=(vmem,) * 5,
        scratch_shapes=[
            pltpu.VMEM((n_sp * MAIN, width), BF16),
            pltpu.VMEM((4, n_sp * MAIN, width), BF16),
            pltpu.VMEM((n_sp * MAIN, LANE), F32),
            pltpu.VMEM((1, 2, chans), F32),
            pltpu.VMEM((n_sp, 2, chans), F32),
            dma((n_sp,)),
            dma((n_sp,)),
            dma,
            dma((8,)),
            dma((8,)),
            dma((8,)),
            dma((8,)),
            dma((8,)),
            dma((8,)),
            dma((n_sp,)),
            dma((n_sp,)),
        ],
        compiler_params=pltpu.CompilerParams(
            collective_id=0, has_side_effects=True, vmem_limit_bytes=60 * 1024 * 1024
        ),
        name="dispatch",
    )(x, g, rt, wt, u, ogl, wr, wi, cdp, eld)


def tail_kernel(
    n_sp,
    sg_ref,
    og_ref,
    routes_ref,
    wout_ref,
    wr_ref,
    wi_ref,
    rec_ref,
    lru_ref,
    gain_ref,
    gop_ref,
    gin_ref,
    ggp_ref,
    rext,
    arr,
    arrx,
    full,
    prod,
    pair,
    summed,
    owned,
    term,
    terms,
    m_send,
    m_recv,
    x_send,
    x_recv,
    own_sems,
    a_send,
    fl_recv,
    fr_recv,
    ff_recv,
    p_sems,
    o_send,
    o_recv,
    t_send,
    t_recv,
):
    me, tp = lax.axis_index("sp"), lax.axis_index("tp")
    right, left, far = (lax.rem(tp + k, 4) for k in (1, 3, 2))
    core = lax.rem(me, 2)
    chip = me // 2
    partner = me + 1 - 2 * core
    chips = n_sp // 2
    tokens, feat = og_ref.shape
    extra = 2
    cuts = feat // LANE
    xrows = extra * cuts
    greet([(lax.rem(me + d, n_sp), tp) for d in range(1, n_sp)] + [(me, right), (me, left)])

    main = n_sp * MAIN
    sx = sg_ref[main:, :].astype(F32)
    for b in range(cuts):
        rext[pl.ds(b, n_sp * extra, stride=cuts), :] = sx[:, b * LANE : (b + 1) * LANE]
    r0 = routes_ref[:, 0:1].astype(F32)
    r1 = routes_ref[:, 1:2].astype(F32)
    expert = iota((tokens, n_sp), 1)
    h0 = expert == r0
    h1 = expert == r1
    held = (h0 | h1).astype(F32).astype(BF16)
    before = (iota((tokens, tokens), 1) < iota((tokens, tokens), 0)).astype(F32).astype(BF16)
    rank = mm(before, held)
    k0 = jnp.sum(jnp.where(h0, rank, 0.0), axis=1, keepdims=True)
    k1 = jnp.sum(jnp.where(h1, rank, 0.0), axis=1, keepdims=True)
    m0 = jnp.where(k0 < MAIN, r0 * MAIN + k0, -1.0)
    m1 = jnp.where(k1 < MAIN, r1 * MAIN + k1, -1.0)
    e0 = jnp.where(k0 < MAIN, -1.0, r0 * extra + k0 - MAIN)
    e1 = jnp.where(k1 < MAIN, -1.0, r1 * extra + k1 - MAIN)
    slot = iota((tokens, main), 1)
    pick = ((slot == m0) | (slot == m1)).astype(F32).astype(BF16)
    slot = iota((tokens, n_sp * extra), 1)
    pickx = ((slot == e0) | (slot == e1)).astype(F32).astype(BF16)

    met(n_sp + 1)

    def rows_of(index, size):
        return pl.ds(pl.multiple_of(index * size, size), size)

    own = [
        pltpu.make_async_copy(
            sg_ref.at[rows_of(me, MAIN)], arr.at[rows_of(me, MAIN)], own_sems.at[0]
        ),
        pltpu.make_async_copy(
            rext.at[rows_of(me, xrows)], arrx.at[rows_of(me, xrows)], own_sems.at[1]
        ),
    ]
    sends = []
    for d in range(1, n_sp):
        peer = lax.rem(me + d, n_sp)
        sends.append(
            copy_to(
                sg_ref.at[rows_of(peer, MAIN)],
                arr.at[rows_of(me, MAIN)],
                m_send.at[d],
                m_recv.at[me],
                peer,
                tp,
            )
        )
        sends.append(
            copy_to(
                rext.at[rows_of(peer, xrows)],
                arrx.at[rows_of(me, xrows)],
                x_send.at[d],
                x_recv.at[me],
                peer,
                tp,
            )
        )
    for c in own + sends:
        c.start()
    for c in own:
        c.wait()
    for d in range(1, n_sp):
        source = lax.rem(me + n_sp - d, n_sp)
        copy_to(
            sg_ref.at[rows_of(source, MAIN)],
            arr.at[rows_of(source, MAIN)],
            m_send.at[d],
            m_recv.at[source],
            source,
            tp,
        ).wait_recv()
        copy_to(
            rext.at[rows_of(source, xrows)],
            arrx.at[rows_of(source, xrows)],
            x_send.at[d],
            x_recv.at[source],
            source,
            tp,
        ).wait_recv()
    back = mm(pick, arr[...])
    backx = jnp.concatenate(
        [mm(pickx, arrx[pl.ds(b, n_sp * extra, stride=cuts), :].astype(BF16)) for b in range(cuts)],
        axis=1,
    )
    full[tp] = (og_ref[...].astype(F32) + (back + backx)).astype(BF16)

    half = tokens // 2

    def piece(quarter, h, send_sem, recv_sem, to):
        ref = full.at[quarter, pl.ds(h * half, half)]
        return copy_to(ref, ref, send_sem, recv_sem, me, to)

    for h in (0, 1):
        sends.append(piece(tp, h, a_send.at[h], fl_recv.at[h], right))
        sends.append(piece(tp, 1 - h, a_send.at[3 - h], fr_recv.at[1 - h], left))
        sends[-2].start()
        sends[-1].start()

    lru = lru_ref[...]

    def use(quarter):
        part = full[quarter]
        wide = mm(part, lru, 0, 0).astype(BF16)
        prod[pl.ds(quarter * (chips // 4), chips // 4)] = wide.reshape(
            chips // 4, 2, wide.shape[0] // (chips // 2), wide.shape[1]
        )
        return mm(part, wout_ref[pl.ds(pl.multiple_of(quarter * feat, feat), feat), :])

    mixer = use(tp)
    piece(left, 0, a_send.at[0], fl_recv.at[0], right).wait_recv()
    sends.append(piece(left, 0, a_send.at[4], ff_recv.at[0], right))
    sends[-1].start()
    piece(right, 1, a_send.at[0], fr_recv.at[1], left).wait_recv()
    sends.append(piece(right, 1, a_send.at[5], ff_recv.at[1], left))
    sends[-1].start()
    piece(left, 1, a_send.at[0], fl_recv.at[1], right).wait_recv()
    mixer = mixer + use(left)
    piece(right, 0, a_send.at[0], fr_recv.at[0], left).wait_recv()
    mixer = mixer + use(right)
    piece(far, 0, a_send.at[0], ff_recv.at[0], right).wait_recv()
    piece(far, 1, a_send.at[0], ff_recv.at[1], left).wait_recv()
    mixer = mixer + use(far)

    trade = copy_to(prod.at[:, 1 - core], pair, p_sems.at[0], p_sems.at[1], partner, tp)
    trade.start()

    decay = rec_ref[0]
    row = lax.broadcasted_iota(jnp.int32, decay.shape, 0)
    ggp_ref[...] = mixer * rec_ref[2]
    gain, tail = scan_rows(shifted(decay, -1, 1.0, row), mixer * rec_ref[1], -1)
    last = decay[0:1, :] * tail[0:1, :]
    term[0] = last
    terms[me] = last
    for d in range(1, n_sp):
        sends.append(
            copy_to(
                term.at[0], terms.at[me], t_send.at[d], t_recv.at[me], lax.rem(me + d, n_sp), tp
            )
        )
        sends[-1].start()

    trade.wait()
    summed[...] = (prod[:, core].astype(F32) + pair[...].astype(F32)).astype(BF16)
    for d in range(1, chips):
        to = lax.rem(chip + d, chips)
        sends.append(
            copy_to(
                summed.at[to], owned.at[chip], o_send.at[d], o_recv.at[chip], to * 2 + core, tp
            )
        )
        sends[-1].start()
    owned[chip] = summed[chip]

    for d in range(1, n_sp):
        source = lax.rem(me + n_sp - d, n_sp)
        copy_to(term.at[0], terms.at[source], t_send.at[d], t_recv.at[source], source, tp).wait_recv()
    later = jnp.zeros_like(last)
    for s in range(n_sp - 1, -1, -1):
        later = jnp.where(s > me, gain_ref[s, 0:1, :] * later + terms[s], later)
    grad = tail + gain * later
    d_recall = (grad * rec_ref[4]).astype(BF16)
    d_admit = (grad * rec_ref[5]).astype(BF16)
    direct = grad * rec_ref[3]
    blocks = direct.shape[1] // LANE
    for b in range(blocks):
        cols = slice(b * LANE, (b + 1) * LANE)
        gin_ref[:, cols] = (
            direct[:, cols]
            + mm(d_recall[:, cols], wr_ref[tp * blocks + b], 1, 1)
            + mm(d_admit[:, cols], wi_ref[tp * blocks + b], 1, 1)
        )

    for d in range(1, chips):
        source = lax.rem(chip + chips - d, chips)
        copy_to(
            summed.at[source],
            owned.at[source],
            o_send.at[d],
            o_recv.at[source],
            source * 2 + core,
            tp,
        ).wait_recv()
    total = owned[0].astype(F32)
    for j in range(1, chips):
        total = total + owned[j].astype(F32)
    gop_ref[...] = total
    for c in sends:
        c.wait_send()


def tail(n_sp, sg, og, routes, wout, wr, wi, rec, lru, gains):
    tokens, feat = og.shape
    chans = lru.shape[1]
    chips = n_sp // 2
    share = wout.shape[0] // n_sp
    vmem = pl.BlockSpec(memory_space=pltpu.VMEM)
    dma = pltpu.SemaphoreType.DMA
    xrows = 2 * feat // LANE
    return pl.pallas_call(
        functools.partial(tail_kernel, n_sp),
        out_shape=(
            jax.ShapeDtypeStruct((share, chans), F32),
            jax.ShapeDtypeStruct((tokens, chans), F32),
            jax.ShapeDtypeStruct((tokens, chans), F32),
        ),
        in_specs=[vmem] * 9,
        out_specs=(vmem,) * 3,
        scratch_shapes=[
            pltpu.VMEM((n_sp * xrows, LANE), F32),
            pltpu.VMEM((n_sp * MAIN, feat), BF16),
            pltpu.VMEM((n_sp * xrows, LANE), F32),
            pltpu.VMEM((4, tokens, feat), BF16),
            pltpu.VMEM((chips, 2, share, chans), BF16),
            pltpu.VMEM((chips, share, chans), BF16),
            pltpu.VMEM((chips, share, chans), BF16),
            pltpu.VMEM((chips, share, chans), BF16),
            pltpu.VMEM((1, 1, chans), F32),
            pltpu.VMEM((n_sp, 1, chans), F32),
            dma((n_sp,)),
            dma((n_sp,)),
            dma((n_sp,)),
            dma((n_sp,)),
            dma((2,)),
            dma((6,)),
            dma((2,)),
            dma((2,)),
            dma((2,)),
            dma((2,)),
            dma((chips,)),
            dma((chips,)),
            dma((n_sp,)),
            dma((n_sp,)),
        ],
        compiler_params=pltpu.CompilerParams(
            collective_id=1, has_side_effects=True, vmem_limit_bytes=40 * 1024 * 1024
        ),
        name="tail",
    )(sg, og, routes, wout, wr, wi, rec, lru, gains)


def summed_over_tp(parts):
    fwd = [(k, (k + 1) % 4) for k in range(4)]
    bwd = [(k, (k + 3) % 4) for k in range(4)]
    here, right, far, left = parts
    half = here.shape[0] // 2
    far_a = lax.ppermute(far[:half], "tp", fwd)
    far_b = lax.ppermute(far[half:], "tp", bwd)
    right_b = lax.ppermute(right[half:], "tp", fwd)
    left_a = lax.ppermute(left[:half], "tp", bwd)
    right_a = lax.ppermute((right[:half].astype(F32) + far_a.astype(F32)).astype(BF16), "tp", fwd)
    left_b = lax.ppermute((left[half:].astype(F32) + far_b.astype(F32)).astype(BF16), "tp", bwd)
    top = here[:half].astype(F32) + (right_a.astype(F32) + left_a.astype(F32))
    low = here[half:].astype(F32) + (right_b.astype(F32) + left_b.astype(F32))
    return jnp.concatenate([top, low], axis=0).astype(BF16)


def per_device(
    n_sp,
    middle_stream,
    output_gradient,
    routes,
    chosen_expert_weight,
    expert_gate_weight,
    expert_up_weight,
    expert_down_weight,
    recurrent_output_weight,
    recurrence_input,
    output_gate_logits,
    recurrence_gate_weight,
    input_gate_weight,
    channel_decay_param,
    extra_log_decay,
):
    feat = middle_stream.shape[1]
    inputs, cotangent, rec, lru, gains = dispatch(
        n_sp,
        middle_stream,
        output_gradient,
        routes.T,
        chosen_expert_weight.T,
        recurrence_input,
        output_gate_logits,
        recurrence_gate_weight,
        input_gate_weight,
        channel_decay_param[None],
        extra_log_decay,
    )
    gate_weight, up_weight, down_weight = (
        expert_gate_weight[0],
        expert_up_weight[0],
        expert_down_weight[0],
    )
    gate_act = mm(inputs, gate_weight)
    up_act = mm(inputs, up_weight)
    sigmoid_gate = jax.nn.sigmoid(gate_act)
    silu_act = gate_act * sigmoid_gate
    hidden = (silu_act * up_act).astype(BF16)
    d_hidden = mm(cotangent, down_weight, 1, 1)
    d_gate = (d_hidden * up_act * sigmoid_gate * (1.0 + gate_act * (1.0 - sigmoid_gate))).astype(
        BF16
    )
    d_up = (d_hidden * silu_act).astype(BF16)
    partial = (mm(d_gate, gate_weight, 1, 1) + mm(d_up, up_weight, 1, 1)).astype(BF16)
    tp = lax.axis_index("tp")
    parts = [
        lax.dynamic_slice_in_dim(partial, lax.rem(tp + k, 4) * feat, feat, 1) for k in range(4)
    ]
    slot_grad = summed_over_tp(parts)
    grad_down = mm(hidden, cotangent, 0, 0).astype(BF16)
    grad_gate = mm(inputs, d_gate, 0, 0).astype(BF16)
    grad_up = mm(inputs, d_up, 0, 0).astype(BF16)
    grad_out_proj, grad_input, grad_gate_pre = tail(
        n_sp,
        slot_grad,
        output_gradient,
        routes,
        recurrent_output_weight,
        recurrence_gate_weight,
        input_gate_weight,
        rec,
        lru,
        gains,
    )
    return (
        grad_gate[None],
        grad_up[None],
        grad_down[None],
        grad_out_proj,
        grad_input,
        grad_gate_pre,
    )


def solution(mesh):
    placed = (
        P("sp", "tp"),
        P("sp", "tp"),
        P("sp", None),
        P("sp", None),
        P("sp", None, "tp"),
        P("sp", None, "tp"),
        P("sp", "tp", None),
        P(None, "tp"),
        P("sp", "tp"),
        P("sp", "tp"),
        P(),
        P(),
        P("tp"),
        P("sp", "tp"),
    )
    return jax.shard_map(
        functools.partial(per_device, mesh.shape["sp"]),
        mesh=mesh,
        in_specs=placed,
        out_specs=(
            P("sp", None, "tp"),
            P("sp", None, "tp"),
            P("sp", "tp", None),
            P("sp", "tp"),
            P("sp", "tp"),
            P("sp", "tp"),
        ),
        check_vma=False,
    )
```

```python
import functools

import jax
import jax.numpy as jnp
from jax import lax
from jax.experimental import pallas as pl
from jax.experimental.pallas import tpu as pltpu
from jax.sharding import PartitionSpec as P

BF16 = jnp.bfloat16
F32 = jnp.float32
MESH = pl.DeviceIdType.MESH
LANE = 128
MAIN = 16


def mm(a, b, ca=1, cb=0):
    return lax.dot_general(a, b, (((ca,), (cb,)), ((), ())), preferred_element_type=F32)


def iota(shape, dim):
    return lax.broadcasted_iota(jnp.int32, shape, dim).astype(F32)


def copy_to(src, dst, send_sem, recv_sem, sp, tp):
    return pltpu.make_async_remote_copy(
        src_ref=src,
        dst_ref=dst,
        send_sem=send_sem,
        recv_sem=recv_sem,
        device_id=(sp, tp),
        device_id_type=MESH,
    )


def greet(targets):
    barrier = pltpu.get_barrier_semaphore()
    for sp, tp in targets:
        pl.semaphore_signal(barrier, inc=1, device_id=(sp, tp), device_id_type=MESH)


def met(count):
    pl.semaphore_wait(pltpu.get_barrier_semaphore(), count)


def in_blocks(body, total, size=256):
    def step(n, c):
        body(pl.multiple_of(n * size, size), size)
        return c

    lax.fori_loop(0, total // size, step, 0)
    if total % size:
        body(total - total % size, total % size)


def shifted(value, by, fill, row):
    rows = value.shape[0]
    if by > 0:
        return jnp.where(row >= by, pltpu.roll(value, by, 0), fill)
    return jnp.where(row < rows + by, pltpu.roll(value, rows + by, 0), fill)


def scan_rows(gain, value, sign):
    rows = value.shape[0]
    row = lax.broadcasted_iota(jnp.int32, value.shape, 0)
    step = 1
    while step < rows:
        value = value + gain * shifted(value, sign * step, 0.0, row)
        gain = gain * shifted(gain, sign * step, 1.0, row)
        step *= 2
    return gain, value


def log1p_of(z):
    series = z * (1.0 - z * (0.5 - z * (1.0 / 3.0 - z * (0.25 - z * (0.2 - z / 6.0)))))
    return jnp.where(z < 0.03, series, jnp.log(1.0 + z))


def one_less_exp(y):
    part = 1.0 + y / 7.0
    for k in (6.0, 5.0, 4.0, 3.0, 2.0):
        part = 1.0 + (y / k) * part
    return jnp.where(y > -0.5, -y * part, 1.0 - jnp.exp(y))


def gelu_both(x):
    c = 0.7978845608028654
    t = jnp.tanh(c * (x + 0.044715 * x * x * x))
    value = 0.5 * x * (1.0 + t)
    slope = 0.5 * (1.0 + t) + 0.5 * x * (1.0 - t * t) * c * (1.0 + 3.0 * 0.044715 * x * x)
    return value, slope


def dispatch_kernel(
    n_sp,
    x_ref,
    g_ref,
    rt_ref,
    wt_ref,
    u_ref,
    ogl_ref,
    wr_ref,
    wi_ref,
    cdp_ref,
    eld_ref,
    wg_ref,
    wu_ref,
    wd_ref,
    rows_out,
    cot_out,
    hid_out,
    dg_out,
    du_out,
    own_out,
    fwd_out,
    bwd_out,
    rec_out,
    lru_out,
    gain_out,
    send,
    recv,
    ext,
    stat,
    stats,
    wg,
    wu,
    wd,
    rows_ref,
    cot_ref,
    acc_g,
    acc_u,
    acc_d,
    hid,
    dg,
    du,
    far_out,
    far_in,
    own_sum,
    fwd_sum,
    bwd_sum,
    rec_ref,
    lru_ref,
    w_sems,
    out_sems,
    f_send,
    f_recv,
    d_send,
    d_recv,
    own_sem,
    r_send,
    l_send,
    y_send,
    fl_recv,
    fr_recv,
    ff_recv,
    s_send,
    s_recv,
):
    me, tp = lax.axis_index("sp"), lax.axis_index("tp")
    right, left, far = (lax.rem(tp + k, 4) for k in (1, 3, 2))
    tokens, feat = x_ref.shape
    extra = 2
    groups = 8
    per = n_sp // groups
    loads = [
        pltpu.make_async_copy(src.at[0], dst, w_sems.at[i])
        for i, (src, dst) in enumerate(((wg_ref, wg), (wu_ref, wu), (wd_ref, wd)))
    ]
    for c in loads:
        c.start()
    greet([(lax.rem(me + d, n_sp), tp) for d in range(1, n_sp)] + [(me, right), (me, left)])

    r0 = rt_ref[0:1, :].astype(F32)
    r1 = rt_ref[1:2, :].astype(F32)
    w0 = wt_ref[0:1, :]
    w1 = wt_ref[1:2, :]
    expert = iota((n_sp, tokens), 0)
    h0 = expert == r0
    h1 = expert == r1
    held = (h0 | h1).astype(F32).astype(BF16)
    before = (iota((tokens, tokens), 0) < iota((tokens, tokens), 1)).astype(F32).astype(BF16)
    rank = mm(held, before)
    k0 = jnp.sum(jnp.where(h0, rank, 0.0), axis=0, keepdims=True)
    k1 = jnp.sum(jnp.where(h1, rank, 0.0), axis=0, keepdims=True)
    m0 = jnp.where(k0 < MAIN, r0 * MAIN + k0, -1.0)
    m1 = jnp.where(k1 < MAIN, r1 * MAIN + k1, -1.0)
    e0 = jnp.where(k0 < MAIN, -1.0, r0 * extra + k0 - MAIN)
    e1 = jnp.where(k1 < MAIN, -1.0, r1 * extra + k1 - MAIN)
    x = x_ref[...]
    g = g_ref[...]
    block = 128
    for at in range(0, n_sp * MAIN, block):
        slot = iota((block, tokens), 0) + float(at)
        p0 = slot == m0
        p1 = slot == m1
        pick = (p0 | p1).astype(F32).astype(BF16)
        weight = jnp.sum(jnp.where(p0, w0, 0.0) + jnp.where(p1, w1, 0.0), axis=1, keepdims=True)
        send[at : at + block, 0:feat] = mm(pick, x).astype(BF16)
        send[at : at + block, feat : 2 * feat] = (mm(pick, g) * weight).astype(BF16)
    slot = iota((n_sp * extra, tokens), 0)
    p0 = slot == e0
    p1 = slot == e1
    pick = (p0 | p1).astype(F32).astype(BF16)
    weight = jnp.sum(jnp.where(p0, w0, 0.0) + jnp.where(p1, w1, 0.0), axis=1, keepdims=True)
    ex = mm(pick, x)
    eg = mm(pick, g) * weight
    cuts = feat // LANE
    for b in range(cuts):
        ext[pl.ds(b, n_sp * extra, stride=2 * cuts), :] = ex[:, b * LANE : (b + 1) * LANE]
        ext[pl.ds(cuts + b, n_sp * extra, stride=2 * cuts), :] = eg[:, b * LANE : (b + 1) * LANE]
    send[:, 2 * feat : 2 * feat + LANE] = ext[...].astype(BF16)

    met(n_sp + 1)

    def dispatch(peer, sem):
        return copy_to(
            send.at[pl.ds(pl.multiple_of(peer * MAIN, MAIN), MAIN)],
            recv.at[tp, pl.ds(pl.multiple_of(me * MAIN, MAIN), MAIN)],
            d_send.at[sem],
            d_recv.at[me],
            peer,
            tp,
        )

    def arrival(source):
        return copy_to(
            send.at[pl.ds(0, MAIN)],
            recv.at[tp, pl.ds(pl.multiple_of(source * MAIN, MAIN), MAIN)],
            d_send.at[0],
            d_recv.at[source],
            source,
            tp,
        )

    own = pltpu.make_async_copy(
        send.at[pl.ds(pl.multiple_of(me * MAIN, MAIN), MAIN)],
        recv.at[tp, pl.ds(pl.multiple_of(me * MAIN, MAIN), MAIN)],
        own_sem,
    )
    own.start()
    sends = []
    for i in range(groups):
        for k in range(per):
            if i + k > 0:
                to = lax.rem(me // per + groups - i, groups) * per + lax.rem(me + k, per)
                sends.append(dispatch(to, i * per + k))
    for s in sends:
        s.start()

    u = u_ref[...]
    uf = u.astype(F32)
    blocks = u.shape[1] // LANE
    pre_r = []
    pre_i = []
    for b in range(blocks):
        ub = u[:, b * LANE : (b + 1) * LANE]
        pre_r.append(mm(ub, wr_ref[tp * blocks + b]))
        pre_i.append(mm(ub, wi_ref[tp * blocks + b]))
    forget = jax.nn.sigmoid(jnp.concatenate(pre_r, axis=1))
    admit = jax.nn.sigmoid(jnp.concatenate(pre_i, axis=1))
    p = cdp_ref[...]
    base = jnp.maximum(-p, 0.0) + log1p_of(jnp.exp(-jnp.abs(p)))
    log_decay = -8.0 * forget * base + eld_ref[...]
    decay = jnp.exp(log_decay)
    scale = jnp.sqrt(one_less_exp(2.0 * log_decay))
    gain, local = scan_rows(decay, uf * admit * scale, 1)
    stat[0, 0:1, :] = gain[tokens - 1 : tokens, :]
    stat[0, 1:2, :] = local[tokens - 1 : tokens, :]
    stats[me, 0:1, :] = gain[tokens - 1 : tokens, :]
    stats[me, 1:2, :] = local[tokens - 1 : tokens, :]
    told = [
        copy_to(
            stat.at[0], stats.at[me], s_send.at[d], s_recv.at[me], lax.rem(me + n_sp - d, n_sp), tp
        )
        for d in range(1, n_sp)
    ]
    for s in told:
        s.start()

    size = per * MAIN
    g0 = me // per

    def span(i):
        start = lax.rem(g0 + i, groups) * size
        return pl.ds(pl.multiple_of(start, size), size)

    def pass_on(quarter, i, send_sem, recv_sem, to):
        return copy_to(
            recv.at[quarter, span(i)], recv.at[quarter, span(i)], send_sem, recv_sem, me, to
        )

    started = []
    hidden = wg.shape[1]

    def quarter(k, first):
        cols = pl.ds(pl.multiple_of(k * feat, feat), feat)
        rows_ref[0 : n_sp * MAIN, cols] = recv[k, :, 0:feat]
        cot_ref[0 : n_sp * MAIN, cols] = recv[k, :, feat : 2 * feat]
        ext[...] = recv[k, :, 2 * feat : 2 * feat + LANE].astype(F32)
        for b in range(cuts):
            at = pl.ds(pl.multiple_of(k * feat + b * LANE, LANE), LANE)
            rows_ref[n_sp * MAIN :, at] = ext[pl.ds(b, n_sp * extra, stride=2 * cuts), :].astype(
                BF16
            )
            cot_ref[n_sp * MAIN :, at] = ext[
                pl.ds(cuts + b, n_sp * extra, stride=2 * cuts), :
            ].astype(BF16)

        def columns(at, size):
            here = pl.ds(at, size)
            for acc, made in (
                (acc_g, lambda: mm(rows_ref[:, cols], wg[cols, here])),
                (acc_u, lambda: mm(rows_ref[:, cols], wu[cols, here])),
                (acc_d, lambda: mm(cot_ref[:, cols], wd[here, cols], 1, 1)),
            ):
                acc[:, here] = made() if first else acc[:, here] + made()

        in_blocks(columns, hidden)

    def relay(i):
        if i % 2 == 0:
            pass_on(left, i, l_send.at[i], fl_recv.at[i], right).wait_recv()
            c = pass_on(left, i, y_send.at[i], ff_recv.at[i], right)
        else:
            pass_on(right, i, r_send.at[i], fr_recv.at[i], left).wait_recv()
            c = pass_on(right, i, y_send.at[i], ff_recv.at[i], left)
        c.start()
        started.append(c)

    for i in range(groups):
        if i == 0:
            own.wait()
        for k in range(per):
            source = lax.rem(g0 + i, groups) * per + k
            if i == 0:

                @pl.when(source != me)
                def _():
                    arrival(source).wait_recv()
            else:
                arrival(source).wait_recv()
        for c in (
            pass_on(tp, i, r_send.at[i], fl_recv.at[i], right),
            pass_on(tp, i, l_send.at[i], fr_recv.at[i], left),
        ):
            c.start()
            started.append(c)

    for c in loads:
        c.wait()
    quarter(tp, True)
    for i in range(groups):
        relay(i)
    for d in range(1, n_sp):
        source = lax.rem(me + d, n_sp)
        copy_to(stat.at[0], stats.at[source], s_send.at[0], s_recv.at[source], source, tp).wait_recv()
    carry = jnp.zeros((1, u.shape[1]), F32)
    for s in range(n_sp):
        carry = jnp.where(s < me, stats[s, 0:1, :] * carry + stats[s, 1:2, :], carry)
    states = local + gain * carry
    row = lax.broadcasted_iota(jnp.int32, states.shape, 0)
    prev = jnp.where(row == 0, carry, pltpu.roll(states, 1, 0))
    gelu, slope = gelu_both(ogl_ref[...].astype(F32))
    lru_ref[...] = (states * gelu).astype(BF16)
    rec_ref[0] = decay
    rec_ref[1] = gelu
    rec_ref[2] = states * slope
    rec_ref[3] = admit * scale
    rec_ref[4] = (
        (prev * decay - uf * admit * decay * decay / scale) * (-8.0 * base) * forget * (1.0 - forget)
    )
    rec_ref[5] = uf * scale * admit * (1.0 - admit)

    for i in range(1, groups, 2):
        pass_on(left, i, l_send.at[i], fl_recv.at[i], right).wait_recv()
    quarter(left, False)
    for i in range(0, groups, 2):
        pass_on(right, i, r_send.at[i], fr_recv.at[i], left).wait_recv()
    quarter(right, False)
    for i in range(groups):
        pass_on(far, i, y_send.at[i], ff_recv.at[i], right).wait_recv()
    quarter(far, False)
    outs = []

    def put(src, dst):
        outs.append(pltpu.make_async_copy(src, dst, out_sems.at[len(outs)]))
        outs[-1].start()

    put(rows_ref, rows_out)
    put(cot_ref, cot_out)
    put(rec_ref, rec_out)
    put(lru_ref, lru_out)
    put(stats, gain_out)
    strip = 32

    def activate(i, c):
        at = pl.ds(pl.multiple_of(i * strip, strip), strip)
        gate = acc_g[at, :]
        up = acc_u[at, :]
        d_hidden = acc_d[at, :]
        sig = jax.nn.sigmoid(gate)
        silu = gate * sig
        hid[at, :] = (silu * up).astype(BF16)
        dg[at, :] = (d_hidden * up * sig * (1.0 + gate * (1.0 - sig))).astype(BF16)
        du[at, :] = (d_hidden * silu).astype(BF16)
        return c

    slots = rows_ref.shape[0]
    lax.fori_loop(0, slots // strip, activate, 0)
    put(hid, hid_out)
    put(dg, dg_out)
    put(du, du_out)

    def back_to(k, store):
        def columns(at, size):
            here = pl.ds(pl.multiple_of(k * feat + at, LANE), size)
            store(at, size, mm(dg[...], wg[here, :], 1, 1) + mm(du[...], wu[here, :], 1, 1))

        in_blocks(columns, feat)

    def into(ref, kind):
        def store(at, size, value):
            ref[:, pl.ds(at, size)] = value.astype(kind)

        return store

    half = slots // 2
    back_to(far, into(far_out, BF16))
    top, low = pl.ds(0, half), pl.ds(half, half)
    for n, (rows, to) in enumerate(((top, right), (low, left))):
        c = copy_to(far_out.at[rows], far_in.at[rows], f_send.at[n], f_recv.at[n], me, to)
        c.start()
        started.append(c)
    back_to(tp, into(own_sum, BF16))
    put(own_sum, own_out)
    back_to(right, into(acc_g, F32))
    back_to(left, into(acc_u, F32))
    fwd_sum[half:, :] = acc_g[half:, 0:feat].astype(BF16)
    bwd_sum[0:half, :] = acc_u[0:half, 0:feat].astype(BF16)
    for c in started[-2:]:
        c.wait_recv()
    fwd_sum[0:half, :] = (acc_g[0:half, 0:feat] + far_in[0:half, :].astype(F32)).astype(BF16)
    bwd_sum[half:, :] = (acc_u[half:, 0:feat] + far_in[half:, :].astype(F32)).astype(BF16)
    put(fwd_sum, fwd_out)
    put(bwd_sum, bwd_out)
    for c in outs:
        c.wait()
    for c in sends + told + started:
        c.wait_send()


def dispatch(n_sp, x, g, rt, wt, u, ogl, wr, wi, cdp, eld, wg, wu, wd):
    tokens, feat = x.shape
    chans = u.shape[1]
    slots = n_sp * (MAIN + 2)
    width = 2 * feat + LANE
    hidden = wg.shape[2]
    shape = jax.ShapeDtypeStruct
    anywhere = pl.BlockSpec(memory_space=pl.ANY)
    vmem = pl.BlockSpec(memory_space=pltpu.VMEM)
    dma = pltpu.SemaphoreType.DMA
    return pl.pallas_call(
        functools.partial(dispatch_kernel, n_sp),
        out_shape=(
            shape((slots, 4 * feat), BF16),
            shape((slots, 4 * feat), BF16),
            shape((slots, hidden), BF16),
            shape((slots, hidden), BF16),
            shape((slots, hidden), BF16),
            shape((slots, feat), BF16),
            shape((slots, feat), BF16),
            shape((slots, feat), BF16),
            shape((6, tokens, chans), F32),
            shape((tokens, chans), BF16),
            shape((n_sp, 2, chans), F32),
        ),
        in_specs=[vmem] * 10 + [anywhere] * 3,
        out_specs=(anywhere,) * 11,
        scratch_shapes=[
            pltpu.VMEM((n_sp * MAIN, width), BF16),
            pltpu.VMEM((4, n_sp * MAIN, width), BF16),
            pltpu.VMEM((n_sp * MAIN, LANE), F32),
            pltpu.VMEM((1, 2, chans), F32),
            pltpu.VMEM((n_sp, 2, chans), F32),
            pltpu.VMEM((4 * feat, hidden), BF16),
            pltpu.VMEM((4 * feat, hidden), BF16),
            pltpu.VMEM((hidden, 4 * feat), BF16),
            pltpu.VMEM((slots, 4 * feat), BF16),
            pltpu.VMEM((slots, 4 * feat), BF16),
            pltpu.VMEM((slots, hidden), F32),
            pltpu.VMEM((slots, hidden), F32),
            pltpu.VMEM((slots, hidden), F32),
            pltpu.VMEM((slots, hidden), BF16),
            pltpu.VMEM((slots, hidden), BF16),
            pltpu.VMEM((slots, hidden), BF16),
            pltpu.VMEM((slots, feat), BF16),
            pltpu.VMEM((slots, feat), BF16),
            pltpu.VMEM((slots, feat), BF16),
            pltpu.VMEM((slots, feat), BF16),
            pltpu.VMEM((slots, feat), BF16),
            pltpu.VMEM((6, tokens, chans), F32),
            pltpu.VMEM((tokens, chans), BF16),
            dma((3,)),
            dma((11,)),
            dma((2,)),
            dma((2,)),
            dma((n_sp,)),
            dma((n_sp,)),
            dma,
            dma((8,)),
            dma((8,)),
            dma((8,)),
            dma((8,)),
            dma((8,)),
            dma((8,)),
            dma((n_sp,)),
            dma((n_sp,)),
        ],
        compiler_params=pltpu.CompilerParams(
            collective_id=0, has_side_effects=True, vmem_limit_bytes=60 * 1024 * 1024
        ),
        name="dispatch",
    )(x, g, rt, wt, u, ogl, wr, wi, cdp, eld, wg, wu, wd)


def tail_kernel(
    n_sp,
    own_ref,
    fwd_ref,
    bwd_ref,
    og_ref,
    routes_ref,
    wout_ref,
    wr_ref,
    wi_ref,
    rec_ref,
    lru_ref,
    gain_ref,
    gop_ref,
    gin_ref,
    ggp_ref,
    sg_ref,
    rext,
    arr,
    arrx,
    full,
    prod,
    pair,
    summed,
    owned,
    term,
    terms,
    m_send,
    m_recv,
    x_send,
    x_recv,
    own_sems,
    a_send,
    fl_recv,
    fr_recv,
    ff_recv,
    p_sems,
    o_send,
    o_recv,
    t_send,
    t_recv,
):
    me, tp = lax.axis_index("sp"), lax.axis_index("tp")
    right, left, far = (lax.rem(tp + k, 4) for k in (1, 3, 2))
    core = lax.rem(me, 2)
    chip = me // 2
    partner = me + 1 - 2 * core
    chips = n_sp // 2
    tokens, feat = og_ref.shape
    extra = 2
    cuts = feat // LANE
    xrows = extra * cuts
    greet([(lax.rem(me + d, n_sp), tp) for d in range(1, n_sp)] + [(me, right), (me, left)])

    main = n_sp * MAIN
    sg_ref[...] = (
        own_ref[...].astype(F32) + (fwd_ref[...].astype(F32) + bwd_ref[...].astype(F32))
    ).astype(BF16)
    sx = sg_ref[main:, :].astype(F32)
    for b in range(cuts):
        rext[pl.ds(b, n_sp * extra, stride=cuts), :] = sx[:, b * LANE : (b + 1) * LANE]
    r0 = routes_ref[:, 0:1].astype(F32)
    r1 = routes_ref[:, 1:2].astype(F32)
    expert = iota((tokens, n_sp), 1)
    h0 = expert == r0
    h1 = expert == r1
    held = (h0 | h1).astype(F32).astype(BF16)
    before = (iota((tokens, tokens), 1) < iota((tokens, tokens), 0)).astype(F32).astype(BF16)
    rank = mm(before, held)
    k0 = jnp.sum(jnp.where(h0, rank, 0.0), axis=1, keepdims=True)
    k1 = jnp.sum(jnp.where(h1, rank, 0.0), axis=1, keepdims=True)
    m0 = jnp.where(k0 < MAIN, r0 * MAIN + k0, -1.0)
    m1 = jnp.where(k1 < MAIN, r1 * MAIN + k1, -1.0)
    e0 = jnp.where(k0 < MAIN, -1.0, r0 * extra + k0 - MAIN)
    e1 = jnp.where(k1 < MAIN, -1.0, r1 * extra + k1 - MAIN)
    slot = iota((tokens, main), 1)
    pick = ((slot == m0) | (slot == m1)).astype(F32).astype(BF16)
    slot = iota((tokens, n_sp * extra), 1)
    pickx = ((slot == e0) | (slot == e1)).astype(F32).astype(BF16)

    met(n_sp + 1)

    def rows_of(index, size):
        return pl.ds(pl.multiple_of(index * size, size), size)

    own = [
        pltpu.make_async_copy(
            sg_ref.at[rows_of(me, MAIN)], arr.at[rows_of(me, MAIN)], own_sems.at[0]
        ),
        pltpu.make_async_copy(
            rext.at[rows_of(me, xrows)], arrx.at[rows_of(me, xrows)], own_sems.at[1]
        ),
    ]
    sends = []
    for d in range(1, n_sp):
        peer = lax.rem(me + d, n_sp)
        sends.append(
            copy_to(
                sg_ref.at[rows_of(peer, MAIN)],
                arr.at[rows_of(me, MAIN)],
                m_send.at[d],
                m_recv.at[me],
                peer,
                tp,
            )
        )
        sends.append(
            copy_to(
                rext.at[rows_of(peer, xrows)],
                arrx.at[rows_of(me, xrows)],
                x_send.at[d],
                x_recv.at[me],
                peer,
                tp,
            )
        )
    for c in own + sends:
        c.start()
    for c in own:
        c.wait()
    for d in range(1, n_sp):
        source = lax.rem(me + n_sp - d, n_sp)
        copy_to(
            sg_ref.at[rows_of(source, MAIN)],
            arr.at[rows_of(source, MAIN)],
            m_send.at[d],
            m_recv.at[source],
            source,
            tp,
        ).wait_recv()
        copy_to(
            rext.at[rows_of(source, xrows)],
            arrx.at[rows_of(source, xrows)],
            x_send.at[d],
            x_recv.at[source],
            source,
            tp,
        ).wait_recv()
    back = mm(pick, arr[...])
    backx = jnp.concatenate(
        [mm(pickx, arrx[pl.ds(b, n_sp * extra, stride=cuts), :].astype(BF16)) for b in range(cuts)],
        axis=1,
    )
    full[tp] = (og_ref[...].astype(F32) + (back + backx)).astype(BF16)

    half = tokens // 2

    def piece(quarter, h, send_sem, recv_sem, to):
        ref = full.at[quarter, pl.ds(h * half, half)]
        return copy_to(ref, ref, send_sem, recv_sem, me, to)

    for h in (0, 1):
        sends.append(piece(tp, h, a_send.at[h], fl_recv.at[h], right))
        sends.append(piece(tp, 1 - h, a_send.at[3 - h], fr_recv.at[1 - h], left))
        sends[-2].start()
        sends[-1].start()

    lru = lru_ref[...]

    def use(quarter):
        part = full[quarter]
        wide = mm(part, lru, 0, 0).astype(BF16)
        prod[pl.ds(quarter * (chips // 4), chips // 4)] = wide.reshape(
            chips // 4, 2, wide.shape[0] // (chips // 2), wide.shape[1]
        )
        return mm(part, wout_ref[pl.ds(pl.multiple_of(quarter * feat, feat), feat), :])

    mixer = use(tp)
    piece(left, 0, a_send.at[0], fl_recv.at[0], right).wait_recv()
    sends.append(piece(left, 0, a_send.at[4], ff_recv.at[0], right))
    sends[-1].start()
    piece(right, 1, a_send.at[0], fr_recv.at[1], left).wait_recv()
    sends.append(piece(right, 1, a_send.at[5], ff_recv.at[1], left))
    sends[-1].start()
    piece(left, 1, a_send.at[0], fl_recv.at[1], right).wait_recv()
    mixer = mixer + use(left)
    piece(right, 0, a_send.at[0], fr_recv.at[0], left).wait_recv()
    mixer = mixer + use(right)
    piece(far, 0, a_send.at[0], ff_recv.at[0], right).wait_recv()
    piece(far, 1, a_send.at[0], ff_recv.at[1], left).wait_recv()
    mixer = mixer + use(far)

    trade = copy_to(prod.at[:, 1 - core], pair, p_sems.at[0], p_sems.at[1], partner, tp)
    trade.start()

    decay = rec_ref[0]
    row = lax.broadcasted_iota(jnp.int32, decay.shape, 0)
    ggp_ref[...] = mixer * rec_ref[2]
    gain, tail = scan_rows(shifted(decay, -1, 1.0, row), mixer * rec_ref[1], -1)
    last = decay[0:1, :] * tail[0:1, :]
    term[0] = last
    terms[me] = last
    for d in range(1, n_sp):
        sends.append(
            copy_to(
                term.at[0], terms.at[me], t_send.at[d], t_recv.at[me], lax.rem(me + d, n_sp), tp
            )
        )
        sends[-1].start()

    trade.wait()
    summed[...] = (prod[:, core].astype(F32) + pair[...].astype(F32)).astype(BF16)
    for d in range(1, chips):
        to = lax.rem(chip + d, chips)
        sends.append(
            copy_to(
                summed.at[to], owned.at[chip], o_send.at[d], o_recv.at[chip], to * 2 + core, tp
            )
        )
        sends[-1].start()
    owned[chip] = summed[chip]

    for d in range(1, n_sp):
        source = lax.rem(me + n_sp - d, n_sp)
        copy_to(term.at[0], terms.at[source], t_send.at[d], t_recv.at[source], source, tp).wait_recv()
    later = jnp.zeros_like(last)
    for s in range(n_sp - 1, -1, -1):
        later = jnp.where(s > me, gain_ref[s, 0:1, :] * later + terms[s], later)
    grad = tail + gain * later
    d_recall = (grad * rec_ref[4]).astype(BF16)
    d_admit = (grad * rec_ref[5]).astype(BF16)
    direct = grad * rec_ref[3]
    blocks = direct.shape[1] // LANE
    for b in range(blocks):
        cols = slice(b * LANE, (b + 1) * LANE)
        gin_ref[:, cols] = (
            direct[:, cols]
            + mm(d_recall[:, cols], wr_ref[tp * blocks + b], 1, 1)
            + mm(d_admit[:, cols], wi_ref[tp * blocks + b], 1, 1)
        )

    for d in range(1, chips):
        source = lax.rem(chip + chips - d, chips)
        copy_to(
            summed.at[source],
            owned.at[source],
            o_send.at[d],
            o_recv.at[source],
            source * 2 + core,
            tp,
        ).wait_recv()
    total = owned[0].astype(F32)
    for j in range(1, chips):
        total = total + owned[j].astype(F32)
    gop_ref[...] = total
    for c in sends:
        c.wait_send()


def tail(n_sp, own, fwd, bwd, og, routes, wout, wr, wi, rec, lru, gains):
    tokens, feat = og.shape
    chans = lru.shape[1]
    chips = n_sp // 2
    share = wout.shape[0] // n_sp
    vmem = pl.BlockSpec(memory_space=pltpu.VMEM)
    dma = pltpu.SemaphoreType.DMA
    xrows = 2 * feat // LANE
    return pl.pallas_call(
        functools.partial(tail_kernel, n_sp),
        out_shape=(
            jax.ShapeDtypeStruct((share, chans), F32),
            jax.ShapeDtypeStruct((tokens, chans), F32),
            jax.ShapeDtypeStruct((tokens, chans), F32),
        ),
        in_specs=[vmem] * 11,
        out_specs=(vmem,) * 3,
        scratch_shapes=[
            pltpu.VMEM(own.shape, BF16),
            pltpu.VMEM((n_sp * xrows, LANE), F32),
            pltpu.VMEM((n_sp * MAIN, feat), BF16),
            pltpu.VMEM((n_sp * xrows, LANE), F32),
            pltpu.VMEM((4, tokens, feat), BF16),
            pltpu.VMEM((chips, 2, share, chans), BF16),
            pltpu.VMEM((chips, share, chans), BF16),
            pltpu.VMEM((chips, share, chans), BF16),
            pltpu.VMEM((chips, share, chans), BF16),
            pltpu.VMEM((1, 1, chans), F32),
            pltpu.VMEM((n_sp, 1, chans), F32),
            dma((n_sp,)),
            dma((n_sp,)),
            dma((n_sp,)),
            dma((n_sp,)),
            dma((2,)),
            dma((6,)),
            dma((2,)),
            dma((2,)),
            dma((2,)),
            dma((2,)),
            dma((chips,)),
            dma((chips,)),
            dma((n_sp,)),
            dma((n_sp,)),
        ],
        compiler_params=pltpu.CompilerParams(
            collective_id=1, has_side_effects=True, vmem_limit_bytes=40 * 1024 * 1024
        ),
        name="tail",
    )(own, fwd, bwd, og, routes, wout, wr, wi, rec, lru, gains)


def per_device(
    n_sp,
    middle_stream,
    output_gradient,
    routes,
    chosen_expert_weight,
    expert_gate_weight,
    expert_up_weight,
    expert_down_weight,
    recurrent_output_weight,
    recurrence_input,
    output_gate_logits,
    recurrence_gate_weight,
    input_gate_weight,
    channel_decay_param,
    extra_log_decay,
):
    inputs, cotangent, hidden, d_gate, d_up, own, fwd, bwd, rec, lru, gains = dispatch(
        n_sp,
        middle_stream,
        output_gradient,
        routes.T,
        chosen_expert_weight.T,
        recurrence_input,
        output_gate_logits,
        recurrence_gate_weight,
        input_gate_weight,
        channel_decay_param[None],
        extra_log_decay,
        expert_gate_weight,
        expert_up_weight,
        expert_down_weight,
    )
    fwd = lax.ppermute(fwd, "tp", [(k, (k + 1) % 4) for k in range(4)])
    bwd = lax.ppermute(bwd, "tp", [(k, (k + 3) % 4) for k in range(4)])
    grad_down = mm(hidden, cotangent, 0, 0).astype(BF16)
    grad_gate = mm(inputs, d_gate, 0, 0).astype(BF16)
    grad_up = mm(inputs, d_up, 0, 0).astype(BF16)
    grad_out_proj, grad_input, grad_gate_pre = tail(
        n_sp,
        own,
        fwd,
        bwd,
        output_gradient,
        routes,
        recurrent_output_weight,
        recurrence_gate_weight,
        input_gate_weight,
        rec,
        lru,
        gains,
    )
    return (
        grad_gate[None],
        grad_up[None],
        grad_down[None],
        grad_out_proj,
        grad_input,
        grad_gate_pre,
    )


def solution(mesh):
    placed = (
        P("sp", "tp"),
        P("sp", "tp"),
        P("sp", None),
        P("sp", None),
        P("sp", None, "tp"),
        P("sp", None, "tp"),
        P("sp", "tp", None),
        P(None, "tp"),
        P("sp", "tp"),
        P("sp", "tp"),
        P(),
        P(),
        P("tp"),
        P("sp", "tp"),
    )
    return jax.shard_map(
        functools.partial(per_device, mesh.shape["sp"]),
        mesh=mesh,
        in_specs=placed,
        out_specs=(
            P("sp", None, "tp"),
            P("sp", None, "tp"),
            P("sp", "tp", None),
            P("sp", "tp"),
            P("sp", "tp"),
            P("sp", "tp"),
        ),
        check_vma=False,
    )
```

```python
import functools

import jax
import jax.numpy as jnp
from jax import lax
from jax.experimental import pallas as pl
from jax.experimental.pallas import tpu as pltpu
from jax.sharding import PartitionSpec as P

BF16 = jnp.bfloat16
F32 = jnp.float32
MESH = pl.DeviceIdType.MESH
LANE = 128
MAIN = 16


def mm(a, b, ca=1, cb=0):
    return lax.dot_general(a, b, (((ca,), (cb,)), ((), ())), preferred_element_type=F32)


def iota(shape, dim):
    return lax.broadcasted_iota(jnp.int32, shape, dim).astype(F32)


def copy_to(src, dst, send_sem, recv_sem, sp, tp):
    return pltpu.make_async_remote_copy(
        src_ref=src,
        dst_ref=dst,
        send_sem=send_sem,
        recv_sem=recv_sem,
        device_id=(sp, tp),
        device_id_type=MESH,
    )


def greet(targets):
    barrier = pltpu.get_barrier_semaphore()
    for sp, tp in targets:
        pl.semaphore_signal(barrier, inc=1, device_id=(sp, tp), device_id_type=MESH)


def met(count):
    pl.semaphore_wait(pltpu.get_barrier_semaphore(), count)


def in_blocks(body, total, size=256):
    def step(n, c):
        body(pl.multiple_of(n * size, size), size)
        return c

    lax.fori_loop(0, total // size, step, 0)
    if total % size:
        body(total - total % size, total % size)


def shifted(value, by, fill, row):
    rows = value.shape[0]
    if by > 0:
        return jnp.where(row >= by, pltpu.roll(value, by, 0), fill)
    return jnp.where(row < rows + by, pltpu.roll(value, rows + by, 0), fill)


def scan_rows(gain, value, sign):
    rows = value.shape[0]
    row = lax.broadcasted_iota(jnp.int32, value.shape, 0)
    step = 1
    while step < rows:
        value = value + gain * shifted(value, sign * step, 0.0, row)
        gain = gain * shifted(gain, sign * step, 1.0, row)
        step *= 2
    return gain, value


def log1p_of(z):
    series = z * (1.0 - z * (0.5 - z * (1.0 / 3.0 - z * (0.25 - z * (0.2 - z / 6.0)))))
    return jnp.where(z < 0.03, series, jnp.log(1.0 + z))


def one_less_exp(y):
    part = 1.0 + y / 7.0
    for k in (6.0, 5.0, 4.0, 3.0, 2.0):
        part = 1.0 + (y / k) * part
    return jnp.where(y > -0.5, -y * part, 1.0 - jnp.exp(y))


def gelu_both(x):
    c = 0.7978845608028654
    t = jnp.tanh(c * (x + 0.044715 * x * x * x))
    value = 0.5 * x * (1.0 + t)
    slope = 0.5 * (1.0 + t) + 0.5 * x * (1.0 - t * t) * c * (1.0 + 3.0 * 0.044715 * x * x)
    return value, slope


def dispatch_kernel(
    n_sp,
    x_ref,
    g_ref,
    rt_ref,
    wt_ref,
    u_ref,
    ogl_ref,
    wr_ref,
    wi_ref,
    cdp_ref,
    eld_ref,
    wg_ref,
    wu_ref,
    wd_ref,
    rows_out,
    cot_out,
    hid_out,
    dg_out,
    du_out,
    own_out,
    fwd_out,
    bwd_out,
    rec_out,
    lru_out,
    gain_out,
    send,
    recv,
    picked,
    pre_in,
    x_far,
    send_far,
    recv_far,
    pre_send,
    pre_recv,
    h_send,
    h_recv,
    ext,
    stat,
    stats,
    wg,
    wu,
    wd,
    rows_ref,
    cot_ref,
    acc_g,
    acc_u,
    acc_d,
    hid,
    dg,
    du,
    far_out,
    far_in,
    right_dx,
    left_dx,
    own_sum,
    fwd_sum,
    bwd_sum,
    rec_ref,
    lru_ref,
    w_sems,
    out_sems,
    f_send,
    f_recv,
    d_send,
    d_recv,
    own_sem,
    r_send,
    l_send,
    y_send,
    fl_recv,
    fr_recv,
    ff_recv,
    s_send,
    s_recv,
):
    me, tp = lax.axis_index("sp"), lax.axis_index("tp")
    right, left, far = (lax.rem(tp + k, 4) for k in (1, 3, 2))
    tokens, feat = x_ref.shape
    extra = 2
    groups = 8
    per = n_sp // groups
    loads = [
        pltpu.make_async_copy(src.at[0], dst, w_sems.at[i])
        for i, (src, dst) in enumerate(((wg_ref, wg), (wu_ref, wu), (wd_ref, wd)))
    ]
    for c in loads:
        c.start()
    greet([(lax.rem(me + d, n_sp), tp) for d in range(1, n_sp)] + [(me, right), (me, left)])

    r0 = rt_ref[0:1, :].astype(F32)
    r1 = rt_ref[1:2, :].astype(F32)
    w0 = wt_ref[0:1, :]
    w1 = wt_ref[1:2, :]
    expert = iota((n_sp, tokens), 0)
    h0 = expert == r0
    h1 = expert == r1
    held = (h0 | h1).astype(F32).astype(BF16)
    before = (iota((tokens, tokens), 0) < iota((tokens, tokens), 1)).astype(F32).astype(BF16)
    rank = mm(held, before)
    k0 = jnp.sum(jnp.where(h0, rank, 0.0), axis=0, keepdims=True)
    k1 = jnp.sum(jnp.where(h1, rank, 0.0), axis=0, keepdims=True)
    m0 = jnp.where(k0 < MAIN, r0 * MAIN + k0, -1.0)
    m1 = jnp.where(k1 < MAIN, r1 * MAIN + k1, -1.0)
    e0 = jnp.where(k0 < MAIN, -1.0, r0 * extra + k0 - MAIN)
    e1 = jnp.where(k1 < MAIN, -1.0, r1 * extra + k1 - MAIN)
    x = x_ref[...]
    g = g_ref[...]
    block = 128
    for at in range(0, n_sp * MAIN, block):
        slot = iota((block, tokens), 0) + float(at)
        p0 = slot == m0
        p1 = slot == m1
        pick = (p0 | p1).astype(F32).astype(BF16)
        weight = jnp.sum(jnp.where(p0, w0, 0.0) + jnp.where(p1, w1, 0.0), axis=1, keepdims=True)
        picked[at : at + block, :] = pick
        send[at : at + block, 0:feat] = mm(pick, x).astype(BF16)
        send[at : at + block, feat : 2 * feat] = (mm(pick, g) * weight).astype(BF16)
    slot = iota((n_sp * extra, tokens), 0)
    p0 = slot == e0
    p1 = slot == e1
    pick = (p0 | p1).astype(F32).astype(BF16)
    weight = jnp.sum(jnp.where(p0, w0, 0.0) + jnp.where(p1, w1, 0.0), axis=1, keepdims=True)
    ex = mm(pick, x)
    eg = mm(pick, g) * weight
    cuts = feat // LANE
    for b in range(cuts):
        ext[pl.ds(b, n_sp * extra, stride=2 * cuts), :] = ex[:, b * LANE : (b + 1) * LANE]
        ext[pl.ds(cuts + b, n_sp * extra, stride=2 * cuts), :] = eg[:, b * LANE : (b + 1) * LANE]
    send[:, 2 * feat : 2 * feat + LANE] = ext[...].astype(BF16)

    met(n_sp + 1)

    def dispatch(peer, sem):
        return copy_to(
            send.at[pl.ds(pl.multiple_of(peer * MAIN, MAIN), MAIN)],
            recv.at[tp, pl.ds(pl.multiple_of(me * MAIN, MAIN), MAIN)],
            d_send.at[sem],
            d_recv.at[me],
            peer,
            tp,
        )

    def arrival(source):
        return copy_to(
            send.at[pl.ds(0, MAIN)],
            recv.at[tp, pl.ds(pl.multiple_of(source * MAIN, MAIN), MAIN)],
            d_send.at[0],
            d_recv.at[source],
            source,
            tp,
        )

    own = pltpu.make_async_copy(
        send.at[pl.ds(pl.multiple_of(me * MAIN, MAIN), MAIN)],
        recv.at[tp, pl.ds(pl.multiple_of(me * MAIN, MAIN), MAIN)],
        own_sem,
    )
    own.start()
    own_half = me // (n_sp // 2)
    quad = groups // 2
    g0 = me // per
    mid = tokens // 2

    def ahead(n, src, dst, to):
        return copy_to(src, dst, pre_send.at[n], pre_recv.at[n], me, to)

    first_hop = [
        ahead(0, x_ref.at[pl.ds(0, mid)], pre_in.at[0], right),
        ahead(1, x_ref.at[pl.ds(mid, mid)], pre_in.at[1], left),
    ]
    next_hop = [
        ahead(2, pre_in.at[0], x_far.at[pl.ds(0, mid)], right),
        ahead(3, pre_in.at[1], x_far.at[pl.ds(mid, mid)], left),
    ]
    for c in first_hop:
        c.start()

    def taker(i, k):
        group = lax.rem(own_half + i // quad, 2) * quad + lax.rem(g0 + groups - i, quad)
        return group * per + lax.rem(me + k, per)

    sends = []
    for i in range(groups):
        for k in range(per):
            if i + k > 0:
                sends.append(dispatch(taker(i, k), i * per + k))
    for s in sends:
        s.start()

    u = u_ref[...]
    uf = u.astype(F32)
    blocks = u.shape[1] // LANE
    pre_r = []
    pre_i = []
    for b in range(blocks):
        ub = u[:, b * LANE : (b + 1) * LANE]
        pre_r.append(mm(ub, wr_ref[tp * blocks + b]))
        pre_i.append(mm(ub, wi_ref[tp * blocks + b]))
    forget = jax.nn.sigmoid(jnp.concatenate(pre_r, axis=1))
    admit = jax.nn.sigmoid(jnp.concatenate(pre_i, axis=1))
    p = cdp_ref[...]
    base = jnp.maximum(-p, 0.0) + log1p_of(jnp.exp(-jnp.abs(p)))
    log_decay = -8.0 * forget * base + eld_ref[...]
    decay = jnp.exp(log_decay)
    scale = jnp.sqrt(one_less_exp(2.0 * log_decay))
    gain, local = scan_rows(decay, uf * admit * scale, 1)
    stat[0, 0:1, :] = gain[tokens - 1 : tokens, :]
    stat[0, 1:2, :] = local[tokens - 1 : tokens, :]
    stats[me, 0:1, :] = gain[tokens - 1 : tokens, :]
    stats[me, 1:2, :] = local[tokens - 1 : tokens, :]
    told = [
        copy_to(
            stat.at[0], stats.at[me], s_send.at[d], s_recv.at[me], lax.rem(me + n_sp - d, n_sp), tp
        )
        for d in range(1, n_sp)
    ]
    for s in told:
        s.start()

    size = per * MAIN

    def group_of(i):
        return lax.rem(own_half + i // quad, 2) * quad + lax.rem(g0 + i, quad)

    def span(i):
        return pl.ds(pl.multiple_of(group_of(i) * size, size), size)

    def pass_on(quarter, i, send_sem, recv_sem, to):
        return copy_to(
            recv.at[quarter, span(i)], recv.at[quarter, span(i)], send_sem, recv_sem, me, to
        )

    def pass_far(quarter, i, to):
        part = recv.at[quarter, span(i), pl.ds(feat, feat + LANE)]
        return copy_to(part, part, y_send.at[i], ff_recv.at[i], me, to)

    def hand_over(peer, sem):
        return copy_to(
            send_far.at[pl.ds(pl.multiple_of(peer * MAIN, MAIN), MAIN)],
            recv_far.at[pl.ds(pl.multiple_of(me * MAIN, MAIN), MAIN)],
            h_send.at[sem],
            h_recv.at[me],
            peer,
            tp,
        )

    def handed(source):
        part = recv_far.at[pl.ds(pl.multiple_of(source * MAIN, MAIN), MAIN)]
        return copy_to(part, part, h_send.at[0], h_recv.at[source], source, tp)

    started = []
    hidden = wg.shape[1]

    main = n_sp * MAIN
    wide = main // 2

    def from_half(h):
        return pl.ds(pl.multiple_of(lax.rem(own_half + h, 2) * wide, wide), wide)

    def place(k, x_from, halves, with_extra):
        cols = pl.ds(pl.multiple_of(k * feat, feat), feat)
        for h in halves:
            rows_ref[h * wide : (h + 1) * wide, cols] = x_from(from_half(h))
            cot_ref[h * wide : (h + 1) * wide, cols] = recv[k, from_half(h), feat : 2 * feat]
        if with_extra:
            ext[...] = recv[k, :, 2 * feat : 2 * feat + LANE].astype(F32)
            for b in range(cuts):
                at = pl.ds(pl.multiple_of(k * feat + b * LANE, LANE), LANE)
                rows_ref[main:, at] = ext[pl.ds(b, n_sp * extra, stride=2 * cuts), :].astype(BF16)
                cot_ref[main:, at] = ext[
                    pl.ds(cuts + b, n_sp * extra, stride=2 * cuts), :
                ].astype(BF16)

    def contract(k, lo, hi, first):
        cols = pl.ds(pl.multiple_of(k * feat, feat), feat)

        def columns(at, size):
            here = pl.ds(at, size)
            for acc, made in (
                (acc_g, lambda: mm(rows_ref[lo:hi, cols], wg[cols, here])),
                (acc_u, lambda: mm(rows_ref[lo:hi, cols], wu[cols, here])),
                (acc_d, lambda: mm(cot_ref[lo:hi, cols], wd[here, cols], 1, 1)),
            ):
                acc[lo:hi, here] = made() if first else acc[lo:hi, here] + made()

        in_blocks(columns, hidden)

    def near_half(k, h, odd, sent, arrived, to):
        for i in range(h * quad + odd, (h + 1) * quad, 2):
            pass_on(k, i, sent.at[i], arrived.at[i], to).wait_recv()
        place(k, lambda rows: recv[k, rows, 0:feat], (h,), h == 1)
        contract(k, h * wide, main + n_sp * extra if h else wide, False)

    def relay(i):
        if i % 2 == 0:
            pass_on(left, i, l_send.at[i], fl_recv.at[i], right).wait_recv()
            c = pass_far(left, i, right)
        else:
            pass_on(right, i, r_send.at[i], fr_recv.at[i], left).wait_recv()
            c = pass_far(right, i, left)
        c.start()
        started.append(c)

    for c, n in zip(first_hop, next_hop):
        c.wait_recv()
        n.start()
    for i in range(groups):
        if i == 0:
            own.wait()
        if i == 3:
            for c in next_hop:
                c.wait_recv()
            for at in range(0, main, block):
                send_far[at : at + block, :] = mm(picked[at : at + block, :], x_far[...]).astype(
                    BF16
                )
            kept = pl.ds(pl.multiple_of(me * MAIN, MAIN), MAIN)
            recv_far[kept, :] = send_far[kept, :]
            for n in range(1, n_sp):
                c = hand_over(taker(n // per, n % per), n)
                c.start()
                started.append(c)
        for k in range(per):
            source = group_of(i) * per + k
            if i == 0:

                @pl.when(source != me)
                def _():
                    arrival(source).wait_recv()
            else:
                arrival(source).wait_recv()
        for c in (
            pass_on(tp, i, r_send.at[i], fl_recv.at[i], right),
            pass_on(tp, i, l_send.at[i], fr_recv.at[i], left),
        ):
            c.start()
            started.append(c)
        if i == quad - 1:
            for n in range(quad):
                relay(n)

    for c in loads:
        c.wait()
    place(tp, lambda rows: recv[tp, rows, 0:feat], (0, 1), True)
    contract(tp, 0, main + n_sp * extra, True)
    near_half(left, 0, 1, l_send, fl_recv, right)
    near_half(right, 0, 0, r_send, fr_recv, left)
    for d in range(1, n_sp):
        source = lax.rem(me + d, n_sp)
        copy_to(stat.at[0], stats.at[source], s_send.at[0], s_recv.at[source], source, tp).wait_recv()
    carry = jnp.zeros((1, u.shape[1]), F32)
    for s in range(n_sp):
        carry = jnp.where(s < me, stats[s, 0:1, :] * carry + stats[s, 1:2, :], carry)
    states = local + gain * carry
    row = lax.broadcasted_iota(jnp.int32, states.shape, 0)
    prev = jnp.where(row == 0, carry, pltpu.roll(states, 1, 0))
    gelu, slope = gelu_both(ogl_ref[...].astype(F32))
    lru_ref[...] = (states * gelu).astype(BF16)
    rec_ref[0] = decay
    rec_ref[1] = gelu
    rec_ref[2] = states * slope
    rec_ref[3] = admit * scale
    rec_ref[4] = (
        (prev * decay - uf * admit * decay * decay / scale) * (-8.0 * base) * forget * (1.0 - forget)
    )
    rec_ref[5] = uf * scale * admit * (1.0 - admit)

    outs = []

    def put(src, dst):
        outs.append(pltpu.make_async_copy(src, dst, out_sems.at[len(outs)]))
        outs[-1].start()

    strip = 32

    def activate(i, c):
        at = pl.ds(pl.multiple_of(i * strip, strip), strip)
        gate = acc_g[at, :]
        up = acc_u[at, :]
        d_hidden = acc_d[at, :]
        sig = jax.nn.sigmoid(gate)
        silu = gate * sig
        hid[at, :] = (silu * up).astype(BF16)
        dg[at, :] = (d_hidden * up * sig * (1.0 + gate * (1.0 - sig))).astype(BF16)
        du[at, :] = (d_hidden * silu).astype(BF16)
        return c

    def back_to(k, lo, hi, store):
        def columns(at, size):
            here = pl.ds(pl.multiple_of(k * feat + at, LANE), size)
            store(
                pl.ds(at, size),
                mm(dg[lo:hi, :], wg[here, :], 1, 1) + mm(du[lo:hi, :], wu[here, :], 1, 1),
            )

        in_blocks(columns, feat)

    slots = rows_ref.shape[0]
    crossing = []

    def finish_far(h):
        lo, hi = (wide, slots) if h else (0, wide)
        for i in range(h * quad, (h + 1) * quad):
            pass_far(far, i, right).wait_recv()
            for k in range(per):
                source = group_of(i) * per + k
                if i == 0:

                    @pl.when(source != me)
                    def _():
                        handed(source).wait_recv()
                else:
                    handed(source).wait_recv()
        place(far, lambda rows: recv_far[rows, :], (h,), h == 1)
        if h == 1:
            put(rows_ref, rows_out)
            put(cot_ref, cot_out)
            put(rec_ref, rec_out)
            put(lru_ref, lru_out)
            put(stats, gain_out)
        contract(far, lo, hi, False)
        lax.fori_loop(lo // strip, hi // strip, activate, 0)

        def to_far(here, value):
            far_out[lo:hi, here] = value.astype(BF16)

        back_to(far, lo, hi, to_far)
        cut = (hi - lo) // 2
        for n, (at, to) in enumerate(((lo, right), (lo + cut, left))):
            rows = pl.ds(at, cut)
            c = copy_to(
                far_out.at[rows], far_in.at[rows], f_send.at[2 * h + n], f_recv.at[2 * h + n], me, to
            )
            c.start()
            crossing.append((c, n, at, at + cut))

    def finish_near(h):
        lo, hi = (wide, slots) if h else (0, wide)

        def to_own(here, value):
            own_sum[lo:hi, here] = value.astype(BF16)

        def to_right(here, value):
            right_dx[lo:hi, here] = value

        def to_left(here, value):
            left_dx[lo:hi, here] = value

        back_to(tp, lo, hi, to_own)
        back_to(right, lo, hi, to_right)
        back_to(left, lo, hi, to_left)

    finish_far(0)
    relay(quad)
    relay(quad + 1)
    finish_near(0)
    relay(quad + 2)
    relay(quad + 3)
    near_half(left, 1, 1, l_send, fl_recv, right)
    near_half(right, 1, 0, r_send, fr_recv, left)
    finish_far(1)
    put(hid, hid_out)
    put(dg, dg_out)
    put(du, du_out)
    finish_near(1)
    put(own_sum, own_out)
    for c, n, lo, hi in crossing:
        mine = bwd_sum if n == 0 else fwd_sum
        total = fwd_sum if n == 0 else bwd_sum
        mine[lo:hi, :] = (left_dx if n == 0 else right_dx)[lo:hi, :].astype(BF16)
        c.wait_recv()
        total[lo:hi, :] = (
            (right_dx if n == 0 else left_dx)[lo:hi, :] + far_in[lo:hi, :].astype(F32)
        ).astype(BF16)
    put(fwd_sum, fwd_out)
    put(bwd_sum, bwd_out)
    for c in outs:
        c.wait()
    for c in first_hop + next_hop + sends + told + started + [c[0] for c in crossing]:
        c.wait_send()


def dispatch(n_sp, x, g, rt, wt, u, ogl, wr, wi, cdp, eld, wg, wu, wd):
    tokens, feat = x.shape
    chans = u.shape[1]
    slots = n_sp * (MAIN + 2)
    width = 2 * feat + LANE
    hidden = wg.shape[2]
    shape = jax.ShapeDtypeStruct
    anywhere = pl.BlockSpec(memory_space=pl.ANY)
    vmem = pl.BlockSpec(memory_space=pltpu.VMEM)
    dma = pltpu.SemaphoreType.DMA
    return pl.pallas_call(
        functools.partial(dispatch_kernel, n_sp),
        out_shape=(
            shape((slots, 4 * feat), BF16),
            shape((slots, 4 * feat), BF16),
            shape((slots, hidden), BF16),
            shape((slots, hidden), BF16),
            shape((slots, hidden), BF16),
            shape((slots, feat), BF16),
            shape((slots, feat), BF16),
            shape((slots, feat), BF16),
            shape((6, tokens, chans), F32),
            shape((tokens, chans), BF16),
            shape((n_sp, 2, chans), F32),
        ),
        in_specs=[vmem] * 10 + [anywhere] * 3,
        out_specs=(anywhere,) * 11,
        scratch_shapes=[
            pltpu.VMEM((n_sp * MAIN, width), BF16),
            pltpu.VMEM((4, n_sp * MAIN, width), BF16),
            pltpu.VMEM((n_sp * MAIN, tokens), BF16),
            pltpu.VMEM((2, tokens // 2, feat), BF16),
            pltpu.VMEM((tokens, feat), BF16),
            pltpu.VMEM((n_sp * MAIN, feat), BF16),
            pltpu.VMEM((n_sp * MAIN, feat), BF16),
            dma((4,)),
            dma((4,)),
            dma((n_sp,)),
            dma((n_sp,)),
            pltpu.VMEM((n_sp * MAIN, LANE), F32),
            pltpu.VMEM((1, 2, chans), F32),
            pltpu.VMEM((n_sp, 2, chans), F32),
            pltpu.VMEM((4 * feat, hidden), BF16),
            pltpu.VMEM((4 * feat, hidden), BF16),
            pltpu.VMEM((hidden, 4 * feat), BF16),
            pltpu.VMEM((slots, 4 * feat), BF16),
            pltpu.VMEM((slots, 4 * feat), BF16),
            pltpu.VMEM((slots, hidden), F32),
            pltpu.VMEM((slots, hidden), F32),
            pltpu.VMEM((slots, hidden), F32),
            pltpu.VMEM((slots, hidden), BF16),
            pltpu.VMEM((slots, hidden), BF16),
            pltpu.VMEM((slots, hidden), BF16),
            pltpu.VMEM((slots, feat), BF16),
            pltpu.VMEM((slots, feat), BF16),
            pltpu.VMEM((slots, feat), F32),
            pltpu.VMEM((slots, feat), F32),
            pltpu.VMEM((slots, feat), BF16),
            pltpu.VMEM((slots, feat), BF16),
            pltpu.VMEM((slots, feat), BF16),
            pltpu.VMEM((6, tokens, chans), F32),
            pltpu.VMEM((tokens, chans), BF16),
            dma((3,)),
            dma((11,)),
            dma((4,)),
            dma((4,)),
            dma((n_sp,)),
            dma((n_sp,)),
            dma,
            dma((8,)),
            dma((8,)),
            dma((8,)),
            dma((8,)),
            dma((8,)),
            dma((8,)),
            dma((n_sp,)),
            dma((n_sp,)),
        ],
        compiler_params=pltpu.CompilerParams(
            collective_id=0, has_side_effects=True, vmem_limit_bytes=60 * 1024 * 1024
        ),
        name="dispatch",
    )(x, g, rt, wt, u, ogl, wr, wi, cdp, eld, wg, wu, wd)


def tail_kernel(
    n_sp,
    own_ref,
    fwd_ref,
    bwd_ref,
    og_ref,
    routes_ref,
    wout_ref,
    wr_ref,
    wi_ref,
    rec_ref,
    lru_ref,
    gain_ref,
    gop_ref,
    gin_ref,
    ggp_ref,
    sg_ref,
    rext,
    arr,
    full,
    prod,
    pair,
    summed,
    owned,
    term,
    terms,
    m_send,
    m_recv,
    own_sems,
    a_send,
    fl_recv,
    fr_recv,
    ff_recv,
    p_send,
    p_recv,
    o_send,
    o_recv,
    t_send,
    t_recv,
):
    me, tp = lax.axis_index("sp"), lax.axis_index("tp")
    right, left, far = (lax.rem(tp + k, 4) for k in (1, 3, 2))
    core = lax.rem(me, 2)
    chip = me // 2
    partner = me + 1 - 2 * core
    chips = n_sp // 2
    tokens, feat = og_ref.shape
    extra = 2
    cuts = feat // LANE
    greet([(lax.rem(me + d, n_sp), tp) for d in range(1, n_sp)] + [(me, right), (me, left)])

    main = n_sp * MAIN
    total = own_ref[...].astype(F32) + (fwd_ref[...].astype(F32) + bwd_ref[...].astype(F32))
    sg_ref[:, 0:feat] = total[0:main, :].astype(BF16)
    rext[...] = jnp.zeros_like(rext)
    for b in range(cuts):
        rext[pl.ds(b, n_sp * extra, stride=2 * cuts), :] = total[main:, b * LANE : (b + 1) * LANE]
    wide = main // 2
    for h in (0, 1):
        source_half = lax.rem(me // (n_sp // 2) + h, 2)
        sg_ref[h * wide : (h + 1) * wide, feat : feat + LANE] = rext[
            pl.ds(pl.multiple_of(source_half * wide, wide), wide), :
        ].astype(BF16)
    r0 = routes_ref[:, 0:1].astype(F32)
    r1 = routes_ref[:, 1:2].astype(F32)
    expert = iota((tokens, n_sp), 1)
    h0 = expert == r0
    h1 = expert == r1
    held = (h0 | h1).astype(F32).astype(BF16)
    before = (iota((tokens, tokens), 1) < iota((tokens, tokens), 0)).astype(F32).astype(BF16)
    rank = mm(before, held)
    k0 = jnp.sum(jnp.where(h0, rank, 0.0), axis=1, keepdims=True)
    k1 = jnp.sum(jnp.where(h1, rank, 0.0), axis=1, keepdims=True)
    m0 = jnp.where(k0 < MAIN, r0 * MAIN + k0, -1.0)
    m1 = jnp.where(k1 < MAIN, r1 * MAIN + k1, -1.0)
    e0 = jnp.where(k0 < MAIN, -1.0, r0 * extra + k0 - MAIN)
    e1 = jnp.where(k1 < MAIN, -1.0, r1 * extra + k1 - MAIN)
    slot = iota((tokens, main), 1)
    pick = ((slot == m0) | (slot == m1)).astype(F32).astype(BF16)
    slot = iota((tokens, n_sp * extra), 1)
    pickx = ((slot == e0) | (slot == e1)).astype(F32).astype(BF16)

    met(n_sp + 1)

    def rows_of(index, size):
        return pl.ds(pl.multiple_of(index * size, size), size)

    def held_for(peer):
        half = n_sp // 2
        at = lax.rem(peer // half + me // half, 2) * half + lax.rem(peer, half)
        return rows_of(at, MAIN)

    own = pltpu.make_async_copy(
        sg_ref.at[held_for(me)], arr.at[rows_of(me, MAIN)], own_sems.at[0]
    )

    def give(d, peer, source):
        return copy_to(
            sg_ref.at[held_for(peer)],
            arr.at[rows_of(source, MAIN)],
            m_send.at[d],
            m_recv.at[source],
            peer,
            tp,
        )

    sends = [give(d, lax.rem(me + d, n_sp), me) for d in range(1, n_sp)]
    own.start()
    for c in sends:
        c.start()
    own.wait()

    half = tokens // 2

    def piece(quarter, h, send_sem, recv_sem, to):
        ref = full.at[quarter, pl.ds(h * half, half)]
        return copy_to(ref, ref, a_send.at[send_sem], recv_sem, me, to)

    def from_left(h):
        return piece(left, h, 0, fl_recv.at[h], right)

    def from_right(h):
        return piece(right, h, 0, fr_recv.at[h], left)

    for d in range(1, n_sp):
        source = lax.rem(me + n_sp - d, n_sp)
        give(d, source, source).wait_recv()
    rext[...] = arr[:, feat : feat + LANE].astype(F32)
    for h in (0, 1):
        rows = slice(h * half, (h + 1) * half)
        back = mm(pick[rows, :], arr[:, 0:feat])
        backx = jnp.concatenate(
            [
                mm(pickx[rows, :], rext[pl.ds(b, n_sp * extra, stride=2 * cuts), :].astype(BF16))
                for b in range(cuts)
            ],
            axis=1,
        )
        full[tp, rows, :] = (og_ref[rows, :].astype(F32) + (back + backx)).astype(BF16)
    for h in (0, 1):
        sends.append(piece(tp, h, h, fl_recv.at[h], right))
        sends[-1].start()
        sends.append(piece(tp, 1 - h, 2 + h, fr_recv.at[1 - h], left))
        sends[-1].start()

    lru = lru_ref[...]
    share = chips // 4

    def use(quarter, n):
        part = full[quarter]
        spread = mm(part, lru, 0, 0).astype(BF16)
        mine = pl.ds(quarter * share, share)
        prod[mine] = spread.reshape(share, 2, feat // (2 * share), spread.shape[1])
        trade(quarter, n).start()
        return mm(part, wout_ref[pl.ds(pl.multiple_of(quarter * feat, feat), feat), :])

    def trade(quarter, n):
        mine = pl.ds(quarter * share, share)
        return copy_to(
            prod.at[mine, 1 - core], pair.at[mine], p_send.at[n], p_recv.at[n], partner, tp
        )

    def to_owner(at, source):
        return copy_to(
            summed.at[at], owned.at[source], o_send.at[at], o_recv.at[source], at * 2 + core, tp
        )

    def settle(quarter, n):
        trade(quarter, n).wait_recv()
        mine = pl.ds(quarter * share, share)
        summed[mine] = (prod[mine, core].astype(F32) + pair[mine].astype(F32)).astype(BF16)
        for k in range(share):
            at = quarter * share + k

            @pl.when(at != chip)
            def _():
                to_owner(at, chip).start()

    mixer = use(tp, 0)
    from_left(0).wait_recv()
    sends.append(piece(left, 0, 4, ff_recv.at[0], right))
    sends[-1].start()
    from_right(1).wait_recv()
    sends.append(piece(right, 1, 5, ff_recv.at[1], left))
    sends[-1].start()
    settle(tp, 0)
    from_left(1).wait_recv()
    mixer = mixer + use(left, 1)
    from_right(0).wait_recv()
    mixer = mixer + use(right, 2)
    settle(left, 1)
    settle(right, 2)
    for h in (0, 1):
        piece(far, h, 0, ff_recv.at[h], right).wait_recv()
    mixer = mixer + use(far, 3)

    decay = rec_ref[0]
    row = lax.broadcasted_iota(jnp.int32, decay.shape, 0)
    ggp_ref[...] = mixer * rec_ref[2]
    gain, tail = scan_rows(shifted(decay, -1, 1.0, row), mixer * rec_ref[1], -1)
    last = decay[0:1, :] * tail[0:1, :]
    term[0] = last
    terms[me] = last
    for d in range(1, n_sp):
        sends.append(
            copy_to(
                term.at[0], terms.at[me], t_send.at[d], t_recv.at[me], lax.rem(me + d, n_sp), tp
            )
        )
        sends[-1].start()

    settle(far, 3)
    owned[chip] = summed[chip]

    for d in range(1, n_sp):
        source = lax.rem(me + n_sp - d, n_sp)
        copy_to(term.at[0], terms.at[source], t_send.at[d], t_recv.at[source], source, tp).wait_recv()
    later = jnp.zeros_like(last)
    for s in range(n_sp - 1, -1, -1):
        later = jnp.where(s > me, gain_ref[s, 0:1, :] * later + terms[s], later)
    grad = tail + gain * later
    d_recall = (grad * rec_ref[4]).astype(BF16)
    d_admit = (grad * rec_ref[5]).astype(BF16)
    direct = grad * rec_ref[3]
    blocks = direct.shape[1] // LANE
    for b in range(blocks):
        cols = slice(b * LANE, (b + 1) * LANE)
        gin_ref[:, cols] = (
            direct[:, cols]
            + mm(d_recall[:, cols], wr_ref[tp * blocks + b], 1, 1)
            + mm(d_admit[:, cols], wi_ref[tp * blocks + b], 1, 1)
        )

    for d in range(1, chips):
        source = lax.rem(chip + chips - d, chips)
        to_owner(source, source).wait_recv()
    total = owned[0].astype(F32)
    for j in range(1, chips):
        total = total + owned[j].astype(F32)
    gop_ref[...] = total
    for n, quarter in enumerate((tp, left, right, far)):
        trade(quarter, n).wait_send()
    for d in range(1, chips):
        to_owner(lax.rem(chip + d, chips), chip).wait_send()
    for c in sends:
        c.wait_send()


def tail(n_sp, own, fwd, bwd, og, routes, wout, wr, wi, rec, lru, gains):
    tokens, feat = og.shape
    chans = lru.shape[1]
    chips = n_sp // 2
    share = wout.shape[0] // n_sp
    vmem = pl.BlockSpec(memory_space=pltpu.VMEM)
    dma = pltpu.SemaphoreType.DMA
    return pl.pallas_call(
        functools.partial(tail_kernel, n_sp),
        out_shape=(
            jax.ShapeDtypeStruct((share, chans), F32),
            jax.ShapeDtypeStruct((tokens, chans), F32),
            jax.ShapeDtypeStruct((tokens, chans), F32),
        ),
        in_specs=[vmem] * 11,
        out_specs=(vmem,) * 3,
        scratch_shapes=[
            pltpu.VMEM((n_sp * MAIN, feat + LANE), BF16),
            pltpu.VMEM((n_sp * MAIN, LANE), F32),
            pltpu.VMEM((n_sp * MAIN, feat + LANE), BF16),
            pltpu.VMEM((4, tokens, feat), BF16),
            pltpu.VMEM((chips, 2, share, chans), BF16),
            pltpu.VMEM((chips, share, chans), BF16),
            pltpu.VMEM((chips, share, chans), BF16),
            pltpu.VMEM((chips, share, chans), BF16),
            pltpu.VMEM((1, 1, chans), F32),
            pltpu.VMEM((n_sp, 1, chans), F32),
            dma((n_sp,)),
            dma((n_sp,)),
            dma((1,)),
            dma((6,)),
            dma((2,)),
            dma((2,)),
            dma((2,)),
            dma((4,)),
            dma((4,)),
            dma((chips,)),
            dma((chips,)),
            dma((n_sp,)),
            dma((n_sp,)),
        ],
        compiler_params=pltpu.CompilerParams(
            collective_id=1, has_side_effects=True, vmem_limit_bytes=40 * 1024 * 1024
        ),
        name="tail",
    )(own, fwd, bwd, og, routes, wout, wr, wi, rec, lru, gains)


def into_weights_kernel(x_ref, dg_ref, du_ref, gate_ref, up_ref):
    flipped = jnp.transpose(x_ref[...])
    gate_ref[...] = mm(flipped, dg_ref[...]).astype(BF16)
    up_ref[...] = mm(flipped, du_ref[...]).astype(BF16)


def from_weights_kernel(h_ref, c_ref, down_ref, flipped):
    @pl.when(pl.program_id(0) == 0)
    def _():
        flipped[...] = jnp.transpose(h_ref[...])

    down_ref[...] = mm(flipped[...], c_ref[...]).astype(BF16)


def weight_gradients(x, cot, hid, dg, du, block=512):
    slots, width = x.shape
    hidden = hid.shape[1]
    whole = pl.BlockSpec((slots, hidden), lambda i: (0, 0))
    strip = pl.BlockSpec((slots, block), lambda i: (0, i))
    flops = 2 * slots * width * hidden

    def cost(n):
        moved = 2 * (slots * width + n * slots * hidden + n * width * hidden)
        return pl.CostEstimate(flops=n * flops, bytes_accessed=moved, transcendentals=0)

    gate, up = pl.pallas_call(
        into_weights_kernel,
        grid=(width // block,),
        out_shape=(jax.ShapeDtypeStruct((width, hidden), BF16),) * 2,
        in_specs=[strip, whole, whole],
        out_specs=(pl.BlockSpec((block, hidden), lambda i: (i, 0)),) * 2,
        compiler_params=pltpu.CompilerParams(vmem_limit_bytes=40 * 1024 * 1024),
        cost_estimate=cost(2),
        name="grads_into",
    )(x, dg, du)
    down = pl.pallas_call(
        from_weights_kernel,
        grid=(width // block,),
        out_shape=jax.ShapeDtypeStruct((hidden, width), BF16),
        in_specs=[whole, strip],
        out_specs=pl.BlockSpec((hidden, block), lambda i: (0, i)),
        scratch_shapes=[pltpu.VMEM((hidden, slots), BF16)],
        compiler_params=pltpu.CompilerParams(vmem_limit_bytes=67043328),
        cost_estimate=cost(1),
        name="grads_from",
    )(hid, cot)
    return gate, up, down


def per_device(
    n_sp,
    middle_stream,
    output_gradient,
    routes,
    chosen_expert_weight,
    expert_gate_weight,
    expert_up_weight,
    expert_down_weight,
    recurrent_output_weight,
    recurrence_input,
    output_gate_logits,
    recurrence_gate_weight,
    input_gate_weight,
    channel_decay_param,
    extra_log_decay,
):
    inputs, cotangent, hidden, d_gate, d_up, own, fwd, bwd, rec, lru, gains = dispatch(
        n_sp,
        middle_stream,
        output_gradient,
        routes.T,
        chosen_expert_weight.T,
        recurrence_input,
        output_gate_logits,
        recurrence_gate_weight,
        input_gate_weight,
        channel_decay_param[None],
        extra_log_decay,
        expert_gate_weight,
        expert_up_weight,
        expert_down_weight,
    )
    fwd = lax.ppermute(fwd, "tp", [(k, (k + 1) % 4) for k in range(4)])
    bwd = lax.ppermute(bwd, "tp", [(k, (k + 3) % 4) for k in range(4)])
    grad_gate, grad_up, grad_down = weight_gradients(inputs, cotangent, hidden, d_gate, d_up)
    grad_out_proj, grad_input, grad_gate_pre = tail(
        n_sp,
        own,
        fwd,
        bwd,
        output_gradient,
        routes,
        recurrent_output_weight,
        recurrence_gate_weight,
        input_gate_weight,
        rec,
        lru,
        gains,
    )
    return (
        grad_gate[None],
        grad_up[None],
        grad_down[None],
        grad_out_proj,
        grad_input,
        grad_gate_pre,
    )


def solution(mesh):
    placed = (
        P("sp", "tp"),
        P("sp", "tp"),
        P("sp", None),
        P("sp", None),
        P("sp", None, "tp"),
        P("sp", None, "tp"),
        P("sp", "tp", None),
        P(None, "tp"),
        P("sp", "tp"),
        P("sp", "tp"),
        P(),
        P(),
        P("tp"),
        P("sp", "tp"),
    )
    return jax.shard_map(
        functools.partial(per_device, mesh.shape["sp"]),
        mesh=mesh,
        in_specs=placed,
        out_specs=(
            P("sp", None, "tp"),
            P("sp", None, "tp"),
            P("sp", "tp", None),
            P("sp", "tp"),
            P("sp", "tp"),
            P("sp", "tp"),
        ),
        check_vma=False,
    )
```

```python
import functools

import jax
import jax.numpy as jnp
from jax import lax
from jax.experimental import pallas as pl
from jax.experimental.pallas import tpu as pltpu
from jax.sharding import PartitionSpec as P

BF16 = jnp.bfloat16
F32 = jnp.float32
MESH = pl.DeviceIdType.MESH
LANE = 128
MAIN = 16


def mm(a, b, ca=1, cb=0):
    return lax.dot_general(a, b, (((ca,), (cb,)), ((), ())), preferred_element_type=F32)


def iota(shape, dim):
    return lax.broadcasted_iota(jnp.int32, shape, dim).astype(F32)


def copy_to(src, dst, send_sem, recv_sem, sp, tp):
    return pltpu.make_async_remote_copy(
        src_ref=src,
        dst_ref=dst,
        send_sem=send_sem,
        recv_sem=recv_sem,
        device_id=(sp, tp),
        device_id_type=MESH,
    )


def greet(targets):
    barrier = pltpu.get_barrier_semaphore()
    for sp, tp in targets:
        pl.semaphore_signal(barrier, inc=1, device_id=(sp, tp), device_id_type=MESH)


def met(count):
    pl.semaphore_wait(pltpu.get_barrier_semaphore(), count)


def in_blocks(body, total, size=256):
    def step(n, c):
        body(pl.multiple_of(n * size, size), size)
        return c

    lax.fori_loop(0, total // size, step, 0)
    if total % size:
        body(total - total % size, total % size)


def shifted(value, by, fill, row):
    rows = value.shape[0]
    if by > 0:
        return jnp.where(row >= by, pltpu.roll(value, by, 0), fill)
    return jnp.where(row < rows + by, pltpu.roll(value, rows + by, 0), fill)


def scan_rows(gain, value, sign):
    rows = value.shape[0]
    row = lax.broadcasted_iota(jnp.int32, value.shape, 0)
    step = 1
    while step < rows:
        value = value + gain * shifted(value, sign * step, 0.0, row)
        gain = gain * shifted(gain, sign * step, 1.0, row)
        step *= 2
    return gain, value


def log1p_of(z):
    series = z * (1.0 - z * (0.5 - z * (1.0 / 3.0 - z * (0.25 - z * (0.2 - z / 6.0)))))
    return jnp.where(z < 0.03, series, jnp.log(1.0 + z))


def one_less_exp(y):
    part = 1.0 + y / 7.0
    for k in (6.0, 5.0, 4.0, 3.0, 2.0):
        part = 1.0 + (y / k) * part
    return jnp.where(y > -0.5, -y * part, 1.0 - jnp.exp(y))


def gelu_both(x):
    c = 0.7978845608028654
    t = jnp.tanh(c * (x + 0.044715 * x * x * x))
    value = 0.5 * x * (1.0 + t)
    slope = 0.5 * (1.0 + t) + 0.5 * x * (1.0 - t * t) * c * (1.0 + 3.0 * 0.044715 * x * x)
    return value, slope


def dispatch_kernel(
    n_sp,
    x_ref,
    g_ref,
    rt_ref,
    wt_ref,
    u_ref,
    ogl_ref,
    wr_ref,
    wi_ref,
    cdp_ref,
    eld_ref,
    wg_ref,
    wu_ref,
    wd_ref,
    rows_out,
    cot_out,
    hid_out,
    dg_out,
    du_out,
    own_out,
    fwd_out,
    bwd_out,
    rec_out,
    lru_out,
    gain_out,
    send,
    recv,
    picked,
    pre_in,
    x_far,
    send_far,
    recv_far,
    pre_send,
    pre_recv,
    h_send,
    h_recv,
    ext,
    stat,
    stats,
    wg,
    wu,
    wd,
    rows_ref,
    cot_ref,
    acc_g,
    acc_u,
    acc_d,
    hid,
    dg,
    du,
    far_out,
    far_in,
    right_dx,
    left_dx,
    own_sum,
    fwd_sum,
    bwd_sum,
    rec_ref,
    lru_ref,
    w_sems,
    out_sems,
    f_send,
    f_recv,
    d_send,
    d_recv,
    own_sem,
    r_send,
    l_send,
    y_send,
    fl_recv,
    fr_recv,
    ff_recv,
    s_send,
    s_recv,
):
    me, tp = lax.axis_index("sp"), lax.axis_index("tp")
    right, left, far = (lax.rem(tp + k, 4) for k in (1, 3, 2))
    tokens, feat = x_ref.shape
    extra = 2
    groups = 8
    per = n_sp // groups
    loads = [
        pltpu.make_async_copy(src.at[0], dst, w_sems.at[i])
        for i, (src, dst) in enumerate(((wg_ref, wg), (wu_ref, wu), (wd_ref, wd)))
    ]
    for c in loads:
        c.start()
    greet([(lax.rem(me + d, n_sp), tp) for d in range(1, n_sp)] + [(me, right), (me, left)])

    r0 = rt_ref[0:1, :].astype(F32)
    r1 = rt_ref[1:2, :].astype(F32)
    w0 = wt_ref[0:1, :]
    w1 = wt_ref[1:2, :]
    expert = iota((n_sp, tokens), 0)
    h0 = expert == r0
    h1 = expert == r1
    held = (h0 | h1).astype(F32).astype(BF16)
    before = (iota((tokens, tokens), 0) < iota((tokens, tokens), 1)).astype(F32).astype(BF16)
    rank = mm(held, before)
    k0 = jnp.sum(jnp.where(h0, rank, 0.0), axis=0, keepdims=True)
    k1 = jnp.sum(jnp.where(h1, rank, 0.0), axis=0, keepdims=True)
    m0 = jnp.where(k0 < MAIN, r0 * MAIN + k0, -1.0)
    m1 = jnp.where(k1 < MAIN, r1 * MAIN + k1, -1.0)
    e0 = jnp.where(k0 < MAIN, -1.0, r0 * extra + k0 - MAIN)
    e1 = jnp.where(k1 < MAIN, -1.0, r1 * extra + k1 - MAIN)
    x = x_ref[...]
    g = g_ref[...]
    block = 128
    for at in range(0, n_sp * MAIN, block):
        slot = iota((block, tokens), 0) + float(at)
        p0 = slot == m0
        p1 = slot == m1
        pick = (p0 | p1).astype(F32).astype(BF16)
        weight = jnp.sum(jnp.where(p0, w0, 0.0) + jnp.where(p1, w1, 0.0), axis=1, keepdims=True)
        picked[at : at + block, :] = pick
        send[at : at + block, 0:feat] = mm(pick, x).astype(BF16)
        send[at : at + block, feat : 2 * feat] = (mm(pick, g) * weight).astype(BF16)
    slot = iota((n_sp * extra, tokens), 0)
    p0 = slot == e0
    p1 = slot == e1
    pick = (p0 | p1).astype(F32).astype(BF16)
    weight = jnp.sum(jnp.where(p0, w0, 0.0) + jnp.where(p1, w1, 0.0), axis=1, keepdims=True)
    ex = mm(pick, x)
    eg = mm(pick, g) * weight
    cuts = feat // LANE
    for b in range(cuts):
        ext[pl.ds(b, n_sp * extra, stride=2 * cuts), :] = ex[:, b * LANE : (b + 1) * LANE]
        ext[pl.ds(cuts + b, n_sp * extra, stride=2 * cuts), :] = eg[:, b * LANE : (b + 1) * LANE]
    send[:, 2 * feat : 2 * feat + LANE] = ext[...].astype(BF16)

    met(n_sp + 1)

    def dispatch(peer, sem):
        return copy_to(
            send.at[pl.ds(pl.multiple_of(peer * MAIN, MAIN), MAIN)],
            recv.at[tp, pl.ds(pl.multiple_of(me * MAIN, MAIN), MAIN)],
            d_send.at[sem],
            d_recv.at[me],
            peer,
            tp,
        )

    def arrival(source):
        return copy_to(
            send.at[pl.ds(0, MAIN)],
            recv.at[tp, pl.ds(pl.multiple_of(source * MAIN, MAIN), MAIN)],
            d_send.at[0],
            d_recv.at[source],
            source,
            tp,
        )

    own = pltpu.make_async_copy(
        send.at[pl.ds(pl.multiple_of(me * MAIN, MAIN), MAIN)],
        recv.at[tp, pl.ds(pl.multiple_of(me * MAIN, MAIN), MAIN)],
        own_sem,
    )
    own.start()
    own_half = me // (n_sp // 2)
    quad = groups // 2
    g0 = me // per
    mid = tokens // 2

    def ahead(n, src, dst, to):
        return copy_to(src, dst, pre_send.at[n], pre_recv.at[n], me, to)

    first_hop = [
        ahead(0, x_ref.at[pl.ds(0, mid)], pre_in.at[0], right),
        ahead(1, x_ref.at[pl.ds(mid, mid)], pre_in.at[1], left),
    ]
    next_hop = [
        ahead(2, pre_in.at[0], x_far.at[pl.ds(0, mid)], right),
        ahead(3, pre_in.at[1], x_far.at[pl.ds(mid, mid)], left),
    ]
    for c in first_hop:
        c.start()

    def taker(i, k):
        group = lax.rem(own_half + i // quad, 2) * quad + lax.rem(g0 + groups - i, quad)
        return group * per + lax.rem(me + k, per)

    sends = []
    for i in range(groups):
        for k in range(per):
            if i + k > 0:
                sends.append(dispatch(taker(i, k), i * per + k))
    for s in sends:
        s.start()

    u = u_ref[...]
    uf = u.astype(F32)
    blocks = u.shape[1] // LANE
    pre_r = []
    pre_i = []
    for b in range(blocks):
        ub = u[:, b * LANE : (b + 1) * LANE]
        pre_r.append(mm(ub, wr_ref[tp * blocks + b]))
        pre_i.append(mm(ub, wi_ref[tp * blocks + b]))
    forget = jax.nn.sigmoid(jnp.concatenate(pre_r, axis=1))
    admit = jax.nn.sigmoid(jnp.concatenate(pre_i, axis=1))
    p = cdp_ref[...]
    base = jnp.maximum(-p, 0.0) + log1p_of(jnp.exp(-jnp.abs(p)))
    log_decay = -8.0 * forget * base + eld_ref[...]
    decay = jnp.exp(log_decay)
    scale = jnp.sqrt(one_less_exp(2.0 * log_decay))
    gain, local = scan_rows(decay, uf * admit * scale, 1)
    stat[0, 0:1, :] = gain[tokens - 1 : tokens, :]
    stat[0, 1:2, :] = local[tokens - 1 : tokens, :]
    stats[me, 0:1, :] = gain[tokens - 1 : tokens, :]
    stats[me, 1:2, :] = local[tokens - 1 : tokens, :]
    told = [
        copy_to(
            stat.at[0], stats.at[me], s_send.at[d], s_recv.at[me], lax.rem(me + n_sp - d, n_sp), tp
        )
        for d in range(1, n_sp)
    ]
    for s in told:
        s.start()

    size = per * MAIN

    def group_of(i):
        return lax.rem(own_half + i // quad, 2) * quad + lax.rem(g0 + i, quad)

    def span(i):
        return pl.ds(pl.multiple_of(group_of(i) * size, size), size)

    def pass_on(quarter, i, send_sem, recv_sem, to):
        return copy_to(
            recv.at[quarter, span(i)], recv.at[quarter, span(i)], send_sem, recv_sem, me, to
        )

    def pass_far(quarter, i, to):
        part = recv.at[quarter, span(i), pl.ds(feat, feat + LANE)]
        return copy_to(part, part, y_send.at[i], ff_recv.at[i], me, to)

    def hand_over(peer, sem):
        return copy_to(
            send_far.at[pl.ds(pl.multiple_of(peer * MAIN, MAIN), MAIN)],
            recv_far.at[pl.ds(pl.multiple_of(me * MAIN, MAIN), MAIN)],
            h_send.at[sem],
            h_recv.at[me],
            peer,
            tp,
        )

    def handed(source):
        part = recv_far.at[pl.ds(pl.multiple_of(source * MAIN, MAIN), MAIN)]
        return copy_to(part, part, h_send.at[0], h_recv.at[source], source, tp)

    started = []
    hidden = wg.shape[1]

    main = n_sp * MAIN
    wide = main // 2

    def from_half(h):
        return pl.ds(pl.multiple_of(lax.rem(own_half + h, 2) * wide, wide), wide)

    def place(k, x_from, halves, with_extra):
        cols = pl.ds(pl.multiple_of(k * feat, feat), feat)
        for h in halves:
            rows_ref[h * wide : (h + 1) * wide, cols] = x_from(from_half(h))
            cot_ref[h * wide : (h + 1) * wide, cols] = recv[k, from_half(h), feat : 2 * feat]
        if with_extra:
            ext[...] = recv[k, :, 2 * feat : 2 * feat + LANE].astype(F32)
            for b in range(cuts):
                at = pl.ds(pl.multiple_of(k * feat + b * LANE, LANE), LANE)
                rows_ref[main:, at] = ext[pl.ds(b, n_sp * extra, stride=2 * cuts), :].astype(BF16)
                cot_ref[main:, at] = ext[
                    pl.ds(cuts + b, n_sp * extra, stride=2 * cuts), :
                ].astype(BF16)

    def contract(k, lo, hi, first):
        cols = pl.ds(pl.multiple_of(k * feat, feat), feat)

        def columns(at, size):
            here = pl.ds(at, size)
            for acc, made in (
                (acc_g, lambda: mm(rows_ref[lo:hi, cols], wg[cols, here])),
                (acc_u, lambda: mm(rows_ref[lo:hi, cols], wu[cols, here])),
                (acc_d, lambda: mm(cot_ref[lo:hi, cols], wd[here, cols], 1, 1)),
            ):
                acc[lo:hi, here] = made() if first else acc[lo:hi, here] + made()

        in_blocks(columns, hidden)

    def near_half(k, h, odd, sent, arrived, to):
        for i in range(h * quad + odd, (h + 1) * quad, 2):
            pass_on(k, i, sent.at[i], arrived.at[i], to).wait_recv()
        place(k, lambda rows: recv[k, rows, 0:feat], (h,), h == 1)
        contract(k, h * wide, main + n_sp * extra if h else wide, False)

    def relay(i):
        if i % 2 == 0:
            pass_on(left, i, l_send.at[i], fl_recv.at[i], right).wait_recv()
            c = pass_far(left, i, right)
        else:
            pass_on(right, i, r_send.at[i], fr_recv.at[i], left).wait_recv()
            c = pass_far(right, i, left)
        c.start()
        started.append(c)

    for c, n in zip(first_hop, next_hop):
        c.wait_recv()
        n.start()
    for i in range(groups):
        if i == 0:
            own.wait()
        if i == 3:
            for c in next_hop:
                c.wait_recv()
            for at in range(0, main, block):
                send_far[at : at + block, :] = mm(picked[at : at + block, :], x_far[...]).astype(
                    BF16
                )
            kept = pl.ds(pl.multiple_of(me * MAIN, MAIN), MAIN)
            recv_far[kept, :] = send_far[kept, :]
            for n in range(1, n_sp):
                c = hand_over(taker(n // per, n % per), n)
                c.start()
                started.append(c)
        for k in range(per):
            source = group_of(i) * per + k
            if i == 0:

                @pl.when(source != me)
                def _():
                    arrival(source).wait_recv()
            else:
                arrival(source).wait_recv()
        for c in (
            pass_on(tp, i, r_send.at[i], fl_recv.at[i], right),
            pass_on(tp, i, l_send.at[i], fr_recv.at[i], left),
        ):
            c.start()
            started.append(c)
        if i == quad - 1:
            for n in range(quad):
                relay(n)

    for c in loads:
        c.wait()
    place(tp, lambda rows: recv[tp, rows, 0:feat], (0, 1), True)
    contract(tp, 0, main + n_sp * extra, True)
    near_half(left, 0, 1, l_send, fl_recv, right)
    near_half(right, 0, 0, r_send, fr_recv, left)
    for d in range(1, n_sp):
        source = lax.rem(me + d, n_sp)
        copy_to(stat.at[0], stats.at[source], s_send.at[0], s_recv.at[source], source, tp).wait_recv()
    carry = jnp.zeros((1, u.shape[1]), F32)
    for s in range(n_sp):
        carry = jnp.where(s < me, stats[s, 0:1, :] * carry + stats[s, 1:2, :], carry)
    states = local + gain * carry
    row = lax.broadcasted_iota(jnp.int32, states.shape, 0)
    prev = jnp.where(row == 0, carry, pltpu.roll(states, 1, 0))
    gelu, slope = gelu_both(ogl_ref[...].astype(F32))
    lru_ref[...] = (states * gelu).astype(BF16)
    rec_ref[0] = decay
    rec_ref[1] = gelu
    rec_ref[2] = states * slope
    rec_ref[3] = admit * scale
    rec_ref[4] = (
        (prev * decay - uf * admit * decay * decay / scale) * (-8.0 * base) * forget * (1.0 - forget)
    )
    rec_ref[5] = uf * scale * admit * (1.0 - admit)

    outs = []

    def put(src, dst):
        outs.append(pltpu.make_async_copy(src, dst, out_sems.at[len(outs)]))
        outs[-1].start()

    strip = 32

    def activate(i, c):
        at = pl.ds(pl.multiple_of(i * strip, strip), strip)
        gate = acc_g[at, :]
        up = acc_u[at, :]
        d_hidden = acc_d[at, :]
        sig = jax.nn.sigmoid(gate)
        silu = gate * sig
        hid[at, :] = (silu * up).astype(BF16)
        dg[at, :] = (d_hidden * up * sig * (1.0 + gate * (1.0 - sig))).astype(BF16)
        du[at, :] = (d_hidden * silu).astype(BF16)
        return c

    def back_to(k, lo, hi, store):
        def columns(at, size):
            here = pl.ds(pl.multiple_of(k * feat + at, LANE), size)
            store(
                pl.ds(at, size),
                mm(dg[lo:hi, :], wg[here, :], 1, 1) + mm(du[lo:hi, :], wu[here, :], 1, 1),
            )

        in_blocks(columns, feat)

    slots = rows_ref.shape[0]
    crossing = []

    def finish_far(h):
        lo, hi = (wide, slots) if h else (0, wide)
        for i in range(h * quad, (h + 1) * quad):
            pass_far(far, i, right).wait_recv()
            for k in range(per):
                source = group_of(i) * per + k
                if i == 0:

                    @pl.when(source != me)
                    def _():
                        handed(source).wait_recv()
                else:
                    handed(source).wait_recv()
        place(far, lambda rows: recv_far[rows, :], (h,), h == 1)
        if h == 1:
            put(rows_ref, rows_out)
            put(cot_ref, cot_out)
            put(rec_ref, rec_out)
            put(lru_ref, lru_out)
            put(stats, gain_out)
        contract(far, lo, hi, False)
        lax.fori_loop(lo // strip, hi // strip, activate, 0)

        def to_far(here, value):
            far_out[lo:hi, here] = value.astype(BF16)

        back_to(far, lo, hi, to_far)
        cut = (hi - lo) // 2
        for n, (at, to) in enumerate(((lo, right), (lo + cut, left))):
            rows = pl.ds(at, cut)
            c = copy_to(
                far_out.at[rows], far_in.at[rows], f_send.at[2 * h + n], f_recv.at[2 * h + n], me, to
            )
            crossing.append((c, n, at, at + cut))

    def finish_near(h):
        lo, hi = (wide, slots) if h else (0, wide)

        def to_own(here, value):
            own_sum[lo:hi, here] = value.astype(BF16)

        def to_right(here, value):
            right_dx[lo:hi, here] = value

        def to_left(here, value):
            left_dx[lo:hi, here] = value

        back_to(tp, lo, hi, to_own)
        back_to(right, lo, hi, to_right)
        back_to(left, lo, hi, to_left)

    finish_far(0)
    relay(quad)
    relay(quad + 1)
    finish_near(0)
    relay(quad + 2)
    relay(quad + 3)
    for c in crossing:
        c[0].start()
    near_half(left, 1, 1, l_send, fl_recv, right)
    near_half(right, 1, 0, r_send, fr_recv, left)
    finish_far(1)
    for c in crossing[2:]:
        c[0].start()
    put(hid, hid_out)
    put(dg, dg_out)
    put(du, du_out)
    finish_near(1)
    put(own_sum, own_out)
    for c, n, lo, hi in crossing:
        mine = bwd_sum if n == 0 else fwd_sum
        total = fwd_sum if n == 0 else bwd_sum
        mine[lo:hi, :] = (left_dx if n == 0 else right_dx)[lo:hi, :].astype(BF16)
        c.wait_recv()
        total[lo:hi, :] = (
            (right_dx if n == 0 else left_dx)[lo:hi, :] + far_in[lo:hi, :].astype(F32)
        ).astype(BF16)
    put(fwd_sum, fwd_out)
    put(bwd_sum, bwd_out)
    for c in outs:
        c.wait()
    for c in first_hop + next_hop + sends + told + started + [c[0] for c in crossing]:
        c.wait_send()


def dispatch(n_sp, x, g, rt, wt, u, ogl, wr, wi, cdp, eld, wg, wu, wd):
    tokens, feat = x.shape
    chans = u.shape[1]
    slots = n_sp * (MAIN + 2)
    width = 2 * feat + LANE
    hidden = wg.shape[2]
    shape = jax.ShapeDtypeStruct
    anywhere = pl.BlockSpec(memory_space=pl.ANY)
    vmem = pl.BlockSpec(memory_space=pltpu.VMEM)
    dma = pltpu.SemaphoreType.DMA
    return pl.pallas_call(
        functools.partial(dispatch_kernel, n_sp),
        out_shape=(
            shape((slots, 4 * feat), BF16),
            shape((slots, 4 * feat), BF16),
            shape((slots, hidden), BF16),
            shape((slots, hidden), BF16),
            shape((slots, hidden), BF16),
            shape((slots, feat), BF16),
            shape((slots, feat), BF16),
            shape((slots, feat), BF16),
            shape((6, tokens, chans), F32),
            shape((tokens, chans), BF16),
            shape((n_sp, 2, chans), F32),
        ),
        in_specs=[vmem] * 10 + [anywhere] * 3,
        out_specs=(anywhere,) * 11,
        scratch_shapes=[
            pltpu.VMEM((n_sp * MAIN, width), BF16),
            pltpu.VMEM((4, n_sp * MAIN, width), BF16),
            pltpu.VMEM((n_sp * MAIN, tokens), BF16),
            pltpu.VMEM((2, tokens // 2, feat), BF16),
            pltpu.VMEM((tokens, feat), BF16),
            pltpu.VMEM((n_sp * MAIN, feat), BF16),
            pltpu.VMEM((n_sp * MAIN, feat), BF16),
            dma((4,)),
            dma((4,)),
            dma((n_sp,)),
            dma((n_sp,)),
            pltpu.VMEM((n_sp * MAIN, LANE), F32),
            pltpu.VMEM((1, 2, chans), F32),
            pltpu.VMEM((n_sp, 2, chans), F32),
            pltpu.VMEM((4 * feat, hidden), BF16),
            pltpu.VMEM((4 * feat, hidden), BF16),
            pltpu.VMEM((hidden, 4 * feat), BF16),
            pltpu.VMEM((slots, 4 * feat), BF16),
            pltpu.VMEM((slots, 4 * feat), BF16),
            pltpu.VMEM((slots, hidden), F32),
            pltpu.VMEM((slots, hidden), F32),
            pltpu.VMEM((slots, hidden), F32),
            pltpu.VMEM((slots, hidden), BF16),
            pltpu.VMEM((slots, hidden), BF16),
            pltpu.VMEM((slots, hidden), BF16),
            pltpu.VMEM((slots, feat), BF16),
            pltpu.VMEM((slots, feat), BF16),
            pltpu.VMEM((slots, feat), F32),
            pltpu.VMEM((slots, feat), F32),
            pltpu.VMEM((slots, feat), BF16),
            pltpu.VMEM((slots, feat), BF16),
            pltpu.VMEM((slots, feat), BF16),
            pltpu.VMEM((6, tokens, chans), F32),
            pltpu.VMEM((tokens, chans), BF16),
            dma((3,)),
            dma((11,)),
            dma((4,)),
            dma((4,)),
            dma((n_sp,)),
            dma((n_sp,)),
            dma,
            dma((8,)),
            dma((8,)),
            dma((8,)),
            dma((8,)),
            dma((8,)),
            dma((8,)),
            dma((n_sp,)),
            dma((n_sp,)),
        ],
        compiler_params=pltpu.CompilerParams(
            collective_id=0, has_side_effects=True, vmem_limit_bytes=60 * 1024 * 1024
        ),
        name="dispatch",
    )(x, g, rt, wt, u, ogl, wr, wi, cdp, eld, wg, wu, wd)


def tail_kernel(
    n_sp,
    own_ref,
    fwd_ref,
    bwd_ref,
    og_ref,
    routes_ref,
    wout_ref,
    wr_ref,
    wi_ref,
    rec_ref,
    lru_ref,
    gain_ref,
    gop_ref,
    gin_ref,
    ggp_ref,
    sg_ref,
    rext,
    arr,
    full,
    prod,
    pair,
    summed,
    owned,
    term,
    terms,
    m_send,
    m_recv,
    own_sems,
    a_send,
    fl_recv,
    fr_recv,
    ff_recv,
    p_send,
    p_recv,
    o_send,
    o_recv,
    t_send,
    t_recv,
):
    me, tp = lax.axis_index("sp"), lax.axis_index("tp")
    right, left, far = (lax.rem(tp + k, 4) for k in (1, 3, 2))
    core = lax.rem(me, 2)
    chip = me // 2
    partner = me + 1 - 2 * core
    chips = n_sp // 2
    tokens, feat = og_ref.shape
    extra = 2
    cuts = feat // LANE
    greet([(lax.rem(me + d, n_sp), tp) for d in range(1, n_sp)] + [(me, right), (me, left)])

    main = n_sp * MAIN
    total = own_ref[...].astype(F32) + (fwd_ref[...].astype(F32) + bwd_ref[...].astype(F32))
    sg_ref[:, 0:feat] = total[0:main, :].astype(BF16)
    rext[...] = jnp.zeros_like(rext)
    for b in range(cuts):
        rext[pl.ds(b, n_sp * extra, stride=2 * cuts), :] = total[main:, b * LANE : (b + 1) * LANE]
    wide = main // 2
    for h in (0, 1):
        source_half = lax.rem(me // (n_sp // 2) + h, 2)
        sg_ref[h * wide : (h + 1) * wide, feat : feat + LANE] = rext[
            pl.ds(pl.multiple_of(source_half * wide, wide), wide), :
        ].astype(BF16)
    r0 = routes_ref[:, 0:1].astype(F32)
    r1 = routes_ref[:, 1:2].astype(F32)
    expert = iota((tokens, n_sp), 1)
    h0 = expert == r0
    h1 = expert == r1
    held = (h0 | h1).astype(F32).astype(BF16)
    before = (iota((tokens, tokens), 1) < iota((tokens, tokens), 0)).astype(F32).astype(BF16)
    rank = mm(before, held)
    k0 = jnp.sum(jnp.where(h0, rank, 0.0), axis=1, keepdims=True)
    k1 = jnp.sum(jnp.where(h1, rank, 0.0), axis=1, keepdims=True)
    m0 = jnp.where(k0 < MAIN, r0 * MAIN + k0, -1.0)
    m1 = jnp.where(k1 < MAIN, r1 * MAIN + k1, -1.0)
    e0 = jnp.where(k0 < MAIN, -1.0, r0 * extra + k0 - MAIN)
    e1 = jnp.where(k1 < MAIN, -1.0, r1 * extra + k1 - MAIN)
    slot = iota((tokens, main), 1)
    pick = ((slot == m0) | (slot == m1)).astype(F32).astype(BF16)
    slot = iota((tokens, n_sp * extra), 1)
    pickx = ((slot == e0) | (slot == e1)).astype(F32).astype(BF16)

    met(n_sp + 1)

    def rows_of(index, size):
        return pl.ds(pl.multiple_of(index * size, size), size)

    def held_for(peer):
        half = n_sp // 2
        at = lax.rem(peer // half + me // half, 2) * half + lax.rem(peer, half)
        return rows_of(at, MAIN)

    own = pltpu.make_async_copy(
        sg_ref.at[held_for(me)], arr.at[rows_of(me, MAIN)], own_sems.at[0]
    )

    def give(d, peer, source):
        return copy_to(
            sg_ref.at[held_for(peer)],
            arr.at[rows_of(source, MAIN)],
            m_send.at[d],
            m_recv.at[source],
            peer,
            tp,
        )

    sends = [give(d, lax.rem(me + d, n_sp), me) for d in range(1, n_sp)]
    own.start()
    for c in sends:
        c.start()
    own.wait()

    half = tokens // 2

    def piece(quarter, h, send_sem, recv_sem, to):
        ref = full.at[quarter, pl.ds(h * half, half)]
        return copy_to(ref, ref, a_send.at[send_sem], recv_sem, me, to)

    def from_left(h):
        return piece(left, h, 0, fl_recv.at[h], right)

    def from_right(h):
        return piece(right, h, 0, fr_recv.at[h], left)

    for d in range(1, n_sp):
        source = lax.rem(me + n_sp - d, n_sp)
        give(d, source, source).wait_recv()
    rext[...] = arr[:, feat : feat + LANE].astype(F32)
    for h in (0, 1):
        rows = slice(h * half, (h + 1) * half)
        back = mm(pick[rows, :], arr[:, 0:feat])
        backx = jnp.concatenate(
            [
                mm(pickx[rows, :], rext[pl.ds(b, n_sp * extra, stride=2 * cuts), :].astype(BF16))
                for b in range(cuts)
            ],
            axis=1,
        )
        full[tp, rows, :] = (og_ref[rows, :].astype(F32) + (back + backx)).astype(BF16)
    for h in (0, 1):
        sends.append(piece(tp, h, h, fl_recv.at[h], right))
        sends[-1].start()
        sends.append(piece(tp, 1 - h, 2 + h, fr_recv.at[1 - h], left))
        sends[-1].start()

    lru = lru_ref[...]
    share = chips // 4

    def use(quarter, n):
        part = full[quarter]
        spread = mm(part, lru, 0, 0).astype(BF16)
        mine = pl.ds(quarter * share, share)
        prod[mine] = spread.reshape(share, 2, feat // (2 * share), spread.shape[1])
        trade(quarter, n).start()
        return mm(part, wout_ref[pl.ds(pl.multiple_of(quarter * feat, feat), feat), :])

    def trade(quarter, n):
        mine = pl.ds(quarter * share, share)
        return copy_to(
            prod.at[mine, 1 - core], pair.at[mine], p_send.at[n], p_recv.at[n], partner, tp
        )

    def to_owner(at, source):
        return copy_to(
            summed.at[at], owned.at[source], o_send.at[at], o_recv.at[source], at * 2 + core, tp
        )

    def settle(quarter, n):
        trade(quarter, n).wait_recv()
        mine = pl.ds(quarter * share, share)
        summed[mine] = (prod[mine, core].astype(F32) + pair[mine].astype(F32)).astype(BF16)
        for k in range(share):
            at = quarter * share + k

            @pl.when(at != chip)
            def _():
                to_owner(at, chip).start()

    mixer = use(tp, 0)
    settle(tp, 0)
    from_left(0).wait_recv()
    sends.append(piece(left, 0, 4, ff_recv.at[0], right))
    sends[-1].start()
    from_right(1).wait_recv()
    sends.append(piece(right, 1, 5, ff_recv.at[1], left))
    sends[-1].start()
    from_left(1).wait_recv()
    mixer = mixer + use(left, 1)
    from_right(0).wait_recv()
    mixer = mixer + use(right, 2)
    settle(left, 1)
    settle(right, 2)
    for h in (0, 1):
        piece(far, h, 0, ff_recv.at[h], right).wait_recv()
    mixer = mixer + use(far, 3)

    decay = rec_ref[0]
    row = lax.broadcasted_iota(jnp.int32, decay.shape, 0)
    ggp_ref[...] = mixer * rec_ref[2]
    gain, tail = scan_rows(shifted(decay, -1, 1.0, row), mixer * rec_ref[1], -1)
    last = decay[0:1, :] * tail[0:1, :]
    term[0] = last
    terms[me] = last
    for d in range(1, n_sp):
        sends.append(
            copy_to(
                term.at[0], terms.at[me], t_send.at[d], t_recv.at[me], lax.rem(me + d, n_sp), tp
            )
        )
        sends[-1].start()

    settle(far, 3)
    owned[chip] = summed[chip]

    for d in range(1, n_sp):
        source = lax.rem(me + n_sp - d, n_sp)
        copy_to(term.at[0], terms.at[source], t_send.at[d], t_recv.at[source], source, tp).wait_recv()
    later = jnp.zeros_like(last)
    for s in range(n_sp - 1, -1, -1):
        later = jnp.where(s > me, gain_ref[s, 0:1, :] * later + terms[s], later)
    grad = tail + gain * later
    d_recall = (grad * rec_ref[4]).astype(BF16)
    d_admit = (grad * rec_ref[5]).astype(BF16)
    direct = grad * rec_ref[3]
    blocks = direct.shape[1] // LANE
    for b in range(blocks):
        cols = slice(b * LANE, (b + 1) * LANE)
        gin_ref[:, cols] = (
            direct[:, cols]
            + mm(d_recall[:, cols], wr_ref[tp * blocks + b], 1, 1)
            + mm(d_admit[:, cols], wi_ref[tp * blocks + b], 1, 1)
        )

    for d in range(1, chips):
        source = lax.rem(chip + chips - d, chips)
        to_owner(source, source).wait_recv()
    total = owned[0].astype(F32)
    for j in range(1, chips):
        total = total + owned[j].astype(F32)
    gop_ref[...] = total
    for n, quarter in enumerate((tp, left, right, far)):
        trade(quarter, n).wait_send()
    for d in range(1, chips):
        to_owner(lax.rem(chip + d, chips), chip).wait_send()
    for c in sends:
        c.wait_send()


def tail(n_sp, own, fwd, bwd, og, routes, wout, wr, wi, rec, lru, gains):
    tokens, feat = og.shape
    chans = lru.shape[1]
    chips = n_sp // 2
    share = wout.shape[0] // n_sp
    vmem = pl.BlockSpec(memory_space=pltpu.VMEM)
    dma = pltpu.SemaphoreType.DMA
    return pl.pallas_call(
        functools.partial(tail_kernel, n_sp),
        out_shape=(
            jax.ShapeDtypeStruct((share, chans), F32),
            jax.ShapeDtypeStruct((tokens, chans), F32),
            jax.ShapeDtypeStruct((tokens, chans), F32),
        ),
        in_specs=[vmem] * 11,
        out_specs=(vmem,) * 3,
        scratch_shapes=[
            pltpu.VMEM((n_sp * MAIN, feat + LANE), BF16),
            pltpu.VMEM((n_sp * MAIN, LANE), F32),
            pltpu.VMEM((n_sp * MAIN, feat + LANE), BF16),
            pltpu.VMEM((4, tokens, feat), BF16),
            pltpu.VMEM((chips, 2, share, chans), BF16),
            pltpu.VMEM((chips, share, chans), BF16),
            pltpu.VMEM((chips, share, chans), BF16),
            pltpu.VMEM((chips, share, chans), BF16),
            pltpu.VMEM((1, 1, chans), F32),
            pltpu.VMEM((n_sp, 1, chans), F32),
            dma((n_sp,)),
            dma((n_sp,)),
            dma((1,)),
            dma((6,)),
            dma((2,)),
            dma((2,)),
            dma((2,)),
            dma((4,)),
            dma((4,)),
            dma((chips,)),
            dma((chips,)),
            dma((n_sp,)),
            dma((n_sp,)),
        ],
        compiler_params=pltpu.CompilerParams(
            collective_id=1, has_side_effects=True, vmem_limit_bytes=40 * 1024 * 1024
        ),
        name="tail",
    )(own, fwd, bwd, og, routes, wout, wr, wi, rec, lru, gains)


def into_weights_kernel(x_ref, dg_ref, du_ref, gate_ref, up_ref):
    flipped = jnp.transpose(x_ref[...])
    gate_ref[...] = mm(flipped, dg_ref[...]).astype(BF16)
    up_ref[...] = mm(flipped, du_ref[...]).astype(BF16)


def from_weights_kernel(h_ref, c_ref, down_ref, flipped):
    @pl.when(pl.program_id(0) == 0)
    def _():
        flipped[...] = jnp.transpose(h_ref[...])

    down_ref[...] = mm(flipped[...], c_ref[...]).astype(BF16)


def weight_gradients(x, cot, hid, dg, du, block=512):
    slots, width = x.shape
    hidden = hid.shape[1]
    whole = pl.BlockSpec((slots, hidden), lambda i: (0, 0))
    strip = pl.BlockSpec((slots, block), lambda i: (0, i))
    flops = 2 * slots * width * hidden

    def cost(n):
        moved = 2 * (slots * width + n * slots * hidden + n * width * hidden)
        return pl.CostEstimate(flops=n * flops, bytes_accessed=moved, transcendentals=0)

    gate, up = pl.pallas_call(
        into_weights_kernel,
        grid=(width // block,),
        out_shape=(jax.ShapeDtypeStruct((width, hidden), BF16),) * 2,
        in_specs=[strip, whole, whole],
        out_specs=(pl.BlockSpec((block, hidden), lambda i: (i, 0)),) * 2,
        compiler_params=pltpu.CompilerParams(vmem_limit_bytes=40 * 1024 * 1024),
        cost_estimate=cost(2),
        name="grads_into",
    )(x, dg, du)
    down = pl.pallas_call(
        from_weights_kernel,
        grid=(width // block,),
        out_shape=jax.ShapeDtypeStruct((hidden, width), BF16),
        in_specs=[whole, strip],
        out_specs=pl.BlockSpec((hidden, block), lambda i: (0, i)),
        scratch_shapes=[pltpu.VMEM((hidden, slots), BF16)],
        compiler_params=pltpu.CompilerParams(vmem_limit_bytes=40 * 1024 * 1024),
        cost_estimate=cost(1),
        name="grads_from",
    )(hid, cot)
    return gate, up, down


def per_device(
    n_sp,
    middle_stream,
    output_gradient,
    routes,
    chosen_expert_weight,
    expert_gate_weight,
    expert_up_weight,
    expert_down_weight,
    recurrent_output_weight,
    recurrence_input,
    output_gate_logits,
    recurrence_gate_weight,
    input_gate_weight,
    channel_decay_param,
    extra_log_decay,
):
    inputs, cotangent, hidden, d_gate, d_up, own, fwd, bwd, rec, lru, gains = dispatch(
        n_sp,
        middle_stream,
        output_gradient,
        routes.T,
        chosen_expert_weight.T,
        recurrence_input,
        output_gate_logits,
        recurrence_gate_weight,
        input_gate_weight,
        channel_decay_param[None],
        extra_log_decay,
        expert_gate_weight,
        expert_up_weight,
        expert_down_weight,
    )
    fwd = lax.ppermute(fwd, "tp", [(k, (k + 1) % 4) for k in range(4)])
    bwd = lax.ppermute(bwd, "tp", [(k, (k + 3) % 4) for k in range(4)])
    grad_gate, grad_up, grad_down = weight_gradients(inputs, cotangent, hidden, d_gate, d_up)
    grad_out_proj, grad_input, grad_gate_pre = tail(
        n_sp,
        own,
        fwd,
        bwd,
        output_gradient,
        routes,
        recurrent_output_weight,
        recurrence_gate_weight,
        input_gate_weight,
        rec,
        lru,
        gains,
    )
    return (
        grad_gate[None],
        grad_up[None],
        grad_down[None],
        grad_out_proj,
        grad_input,
        grad_gate_pre,
    )


def solution(mesh):
    placed = (
        P("sp", "tp"),
        P("sp", "tp"),
        P("sp", None),
        P("sp", None),
        P("sp", None, "tp"),
        P("sp", None, "tp"),
        P("sp", "tp", None),
        P(None, "tp"),
        P("sp", "tp"),
        P("sp", "tp"),
        P(),
        P(),
        P("tp"),
        P("sp", "tp"),
    )
    return jax.shard_map(
        functools.partial(per_device, mesh.shape["sp"]),
        mesh=mesh,
        in_specs=placed,
        out_specs=(
            P("sp", None, "tp"),
            P("sp", None, "tp"),
            P("sp", "tp", None),
            P("sp", "tp"),
            P("sp", "tp"),
            P("sp", "tp"),
        ),
        check_vma=False,
    )
```

```python
import functools

import jax
import jax.numpy as jnp
from jax import lax
from jax.experimental import pallas as pl
from jax.experimental.pallas import tpu as pltpu
from jax.sharding import PartitionSpec as P

BF16 = jnp.bfloat16
F32 = jnp.float32
MESH = pl.DeviceIdType.MESH
LANE = 128
MAIN = 16


def mm(a, b, ca=1, cb=0):
    return lax.dot_general(a, b, (((ca,), (cb,)), ((), ())), preferred_element_type=F32)


def iota(shape, dim):
    return lax.broadcasted_iota(jnp.int32, shape, dim).astype(F32)


def copy_to(src, dst, send_sem, recv_sem, sp, tp):
    return pltpu.make_async_remote_copy(
        src_ref=src,
        dst_ref=dst,
        send_sem=send_sem,
        recv_sem=recv_sem,
        device_id=(sp, tp),
        device_id_type=MESH,
    )


def greet(targets):
    barrier = pltpu.get_barrier_semaphore()
    for sp, tp in targets:
        pl.semaphore_signal(barrier, inc=1, device_id=(sp, tp), device_id_type=MESH)


def met(count):
    pl.semaphore_wait(pltpu.get_barrier_semaphore(), count)


def in_blocks(body, total, size=256):
    def step(n, c):
        body(pl.multiple_of(n * size, size), size)
        return c

    lax.fori_loop(0, total // size, step, 0)
    if total % size:
        body(total - total % size, total % size)


def shifted(value, by, fill, row):
    rows = value.shape[0]
    if by > 0:
        return jnp.where(row >= by, pltpu.roll(value, by, 0), fill)
    return jnp.where(row < rows + by, pltpu.roll(value, rows + by, 0), fill)


def scan_rows(gain, value, sign):
    rows = value.shape[0]
    row = lax.broadcasted_iota(jnp.int32, value.shape, 0)
    step = 1
    while step < rows:
        value = value + gain * shifted(value, sign * step, 0.0, row)
        gain = gain * shifted(gain, sign * step, 1.0, row)
        step *= 2
    return gain, value


def log1p_of(z):
    series = z * (1.0 - z * (0.5 - z * (1.0 / 3.0 - z * (0.25 - z * (0.2 - z / 6.0)))))
    return jnp.where(z < 0.03, series, jnp.log(1.0 + z))


def one_less_exp(y):
    part = 1.0 + y / 7.0
    for k in (6.0, 5.0, 4.0, 3.0, 2.0):
        part = 1.0 + (y / k) * part
    return jnp.where(y > -0.5, -y * part, 1.0 - jnp.exp(y))


def gelu_both(x):
    c = 0.7978845608028654
    t = jnp.tanh(c * (x + 0.044715 * x * x * x))
    value = 0.5 * x * (1.0 + t)
    slope = 0.5 * (1.0 + t) + 0.5 * x * (1.0 - t * t) * c * (1.0 + 3.0 * 0.044715 * x * x)
    return value, slope


def dispatch_kernel(
    n_sp,
    x_ref,
    g_ref,
    rt_ref,
    wt_ref,
    u_ref,
    ogl_ref,
    wr_ref,
    wi_ref,
    cdp_ref,
    eld_ref,
    wg_ref,
    wu_ref,
    wd_ref,
    rows_out,
    cot_out,
    hid_out,
    dg_out,
    du_out,
    own_out,
    fwd_out,
    bwd_out,
    rec_out,
    lru_out,
    gain_out,
    send,
    recv,
    picked,
    pre_in,
    x_far,
    send_far,
    recv_far,
    pre_send,
    pre_recv,
    h_send,
    h_recv,
    ext,
    stat,
    stats,
    wg,
    wu,
    wd,
    rows_ref,
    cot_ref,
    acc_g,
    acc_u,
    acc_d,
    hid,
    dg,
    du,
    far_out,
    far_in,
    right_dx,
    left_dx,
    own_sum,
    fwd_sum,
    bwd_sum,
    rec_ref,
    lru_ref,
    w_sems,
    out_sems,
    f_send,
    f_recv,
    d_send,
    d_recv,
    own_sem,
    r_send,
    l_send,
    y_send,
    fl_recv,
    fr_recv,
    ff_recv,
    s_send,
    s_recv,
):
    me, tp = lax.axis_index("sp"), lax.axis_index("tp")
    right, left, far = (lax.rem(tp + k, 4) for k in (1, 3, 2))
    tokens, feat = x_ref.shape
    extra = 2
    groups = 8
    per = n_sp // groups
    loads = [
        pltpu.make_async_copy(src.at[0], dst, w_sems.at[i])
        for i, (src, dst) in enumerate(((wg_ref, wg), (wu_ref, wu), (wd_ref, wd)))
    ]
    for c in loads:
        c.start()
    greet([(lax.rem(me + d, n_sp), tp) for d in range(1, n_sp)] + [(me, right), (me, left)])

    r0 = rt_ref[0:1, :].astype(F32)
    r1 = rt_ref[1:2, :].astype(F32)
    w0 = wt_ref[0:1, :]
    w1 = wt_ref[1:2, :]
    expert = iota((n_sp, tokens), 0)
    h0 = expert == r0
    h1 = expert == r1
    held = (h0 | h1).astype(F32).astype(BF16)
    before = (iota((tokens, tokens), 0) < iota((tokens, tokens), 1)).astype(F32).astype(BF16)
    rank = mm(held, before)
    k0 = jnp.sum(jnp.where(h0, rank, 0.0), axis=0, keepdims=True)
    k1 = jnp.sum(jnp.where(h1, rank, 0.0), axis=0, keepdims=True)
    m0 = jnp.where(k0 < MAIN, r0 * MAIN + k0, -1.0)
    m1 = jnp.where(k1 < MAIN, r1 * MAIN + k1, -1.0)
    e0 = jnp.where(k0 < MAIN, -1.0, r0 * extra + k0 - MAIN)
    e1 = jnp.where(k1 < MAIN, -1.0, r1 * extra + k1 - MAIN)
    x = x_ref[...]
    g = g_ref[...]
    block = 128
    for at in range(0, n_sp * MAIN, block):
        slot = iota((block, tokens), 0) + float(at)
        p0 = slot == m0
        p1 = slot == m1
        pick = (p0 | p1).astype(F32).astype(BF16)
        weight = jnp.sum(jnp.where(p0, w0, 0.0) + jnp.where(p1, w1, 0.0), axis=1, keepdims=True)
        picked[at : at + block, :] = pick
        send[at : at + block, 0:feat] = mm(pick, x).astype(BF16)
        send[at : at + block, feat : 2 * feat] = (mm(pick, g) * weight).astype(BF16)
    slot = iota((n_sp * extra, tokens), 0)
    p0 = slot == e0
    p1 = slot == e1
    pick = (p0 | p1).astype(F32).astype(BF16)
    weight = jnp.sum(jnp.where(p0, w0, 0.0) + jnp.where(p1, w1, 0.0), axis=1, keepdims=True)
    ex = mm(pick, x)
    eg = mm(pick, g) * weight
    cuts = feat // LANE
    for b in range(cuts):
        ext[pl.ds(b, n_sp * extra, stride=2 * cuts), :] = ex[:, b * LANE : (b + 1) * LANE]
        ext[pl.ds(cuts + b, n_sp * extra, stride=2 * cuts), :] = eg[:, b * LANE : (b + 1) * LANE]
    send[:, 2 * feat : 2 * feat + LANE] = ext[...].astype(BF16)

    met(n_sp + 1)

    def dispatch(peer, sem):
        return copy_to(
            send.at[pl.ds(pl.multiple_of(peer * MAIN, MAIN), MAIN)],
            recv.at[tp, pl.ds(pl.multiple_of(me * MAIN, MAIN), MAIN)],
            d_send.at[sem],
            d_recv.at[me],
            peer,
            tp,
        )

    def arrival(source):
        return copy_to(
            send.at[pl.ds(0, MAIN)],
            recv.at[tp, pl.ds(pl.multiple_of(source * MAIN, MAIN), MAIN)],
            d_send.at[0],
            d_recv.at[source],
            source,
            tp,
        )

    own = pltpu.make_async_copy(
        send.at[pl.ds(pl.multiple_of(me * MAIN, MAIN), MAIN)],
        recv.at[tp, pl.ds(pl.multiple_of(me * MAIN, MAIN), MAIN)],
        own_sem,
    )
    own.start()
    own_half = me // (n_sp // 2)
    quad = groups // 2
    g0 = me // per
    mid = tokens // 2

    def ahead(n, src, dst, to):
        return copy_to(src, dst, pre_send.at[n], pre_recv.at[n], me, to)

    first_hop = [
        ahead(0, x_ref.at[pl.ds(0, mid)], pre_in.at[0], right),
        ahead(1, x_ref.at[pl.ds(mid, mid)], pre_in.at[1], left),
    ]
    next_hop = [
        ahead(2, pre_in.at[0], x_far.at[pl.ds(0, mid)], right),
        ahead(3, pre_in.at[1], x_far.at[pl.ds(mid, mid)], left),
    ]
    for c in first_hop:
        c.start()

    def taker(i, k):
        group = lax.rem(own_half + i // quad, 2) * quad + lax.rem(g0 + groups - i, quad)
        return group * per + lax.rem(me + k, per)

    sends = []
    for i in range(groups):
        for k in range(per):
            if i + k > 0:
                sends.append(dispatch(taker(i, k), i * per + k))
    for s in sends:
        s.start()

    u = u_ref[...]
    uf = u.astype(F32)
    blocks = u.shape[1] // LANE
    pre_r = []
    pre_i = []
    for b in range(blocks):
        ub = u[:, b * LANE : (b + 1) * LANE]
        pre_r.append(mm(ub, wr_ref[tp * blocks + b]))
        pre_i.append(mm(ub, wi_ref[tp * blocks + b]))
    forget = jax.nn.sigmoid(jnp.concatenate(pre_r, axis=1))
    admit = jax.nn.sigmoid(jnp.concatenate(pre_i, axis=1))
    p = cdp_ref[...]
    base = jnp.maximum(-p, 0.0) + log1p_of(jnp.exp(-jnp.abs(p)))
    log_decay = -8.0 * forget * base + eld_ref[...]
    decay = jnp.exp(log_decay)
    scale = jnp.sqrt(one_less_exp(2.0 * log_decay))
    gain, local = scan_rows(decay, uf * admit * scale, 1)
    stat[0, 0:1, :] = gain[tokens - 1 : tokens, :]
    stat[0, 1:2, :] = local[tokens - 1 : tokens, :]
    stats[me, 0:1, :] = gain[tokens - 1 : tokens, :]
    stats[me, 1:2, :] = local[tokens - 1 : tokens, :]
    told = [
        copy_to(
            stat.at[0], stats.at[me], s_send.at[d], s_recv.at[me], lax.rem(me + n_sp - d, n_sp), tp
        )
        for d in range(1, n_sp)
    ]
    for s in told:
        s.start()

    size = per * MAIN

    def group_of(i):
        return lax.rem(own_half + i // quad, 2) * quad + lax.rem(g0 + i, quad)

    def span(i):
        return pl.ds(pl.multiple_of(group_of(i) * size, size), size)

    def pass_on(quarter, i, send_sem, recv_sem, to):
        return copy_to(
            recv.at[quarter, span(i)], recv.at[quarter, span(i)], send_sem, recv_sem, me, to
        )

    def pass_far(quarter, i, to):
        part = recv.at[quarter, span(i), pl.ds(feat, feat + LANE)]
        return copy_to(part, part, y_send.at[i], ff_recv.at[i], me, to)

    def hand_over(peer, sem):
        return copy_to(
            send_far.at[pl.ds(pl.multiple_of(peer * MAIN, MAIN), MAIN)],
            recv_far.at[pl.ds(pl.multiple_of(me * MAIN, MAIN), MAIN)],
            h_send.at[sem],
            h_recv.at[me],
            peer,
            tp,
        )

    def handed(source):
        part = recv_far.at[pl.ds(pl.multiple_of(source * MAIN, MAIN), MAIN)]
        return copy_to(part, part, h_send.at[0], h_recv.at[source], source, tp)

    started = []
    hidden = wg.shape[1]

    main = n_sp * MAIN
    wide = main // 2

    def from_half(h):
        return pl.ds(pl.multiple_of(lax.rem(own_half + h, 2) * wide, wide), wide)

    def place(k, x_from, halves, with_extra):
        cols = pl.ds(pl.multiple_of(k * feat, feat), feat)
        for h in halves:
            rows_ref[h * wide : (h + 1) * wide, cols] = x_from(from_half(h))
            cot_ref[h * wide : (h + 1) * wide, cols] = recv[k, from_half(h), feat : 2 * feat]
        if with_extra:
            ext[...] = recv[k, :, 2 * feat : 2 * feat + LANE].astype(F32)
            for b in range(cuts):
                at = pl.ds(pl.multiple_of(k * feat + b * LANE, LANE), LANE)
                rows_ref[main:, at] = ext[pl.ds(b, n_sp * extra, stride=2 * cuts), :].astype(BF16)
                cot_ref[main:, at] = ext[
                    pl.ds(cuts + b, n_sp * extra, stride=2 * cuts), :
                ].astype(BF16)

    def contract(k, lo, hi, first):
        cols = pl.ds(pl.multiple_of(k * feat, feat), feat)

        def columns(at, size):
            here = pl.ds(at, size)
            for acc, made in (
                (acc_g, lambda: mm(rows_ref[lo:hi, cols], wg[cols, here])),
                (acc_u, lambda: mm(rows_ref[lo:hi, cols], wu[cols, here])),
                (acc_d, lambda: mm(cot_ref[lo:hi, cols], wd[here, cols], 1, 1)),
            ):
                acc[lo:hi, here] = made() if first else acc[lo:hi, here] + made()

        in_blocks(columns, hidden)

    def near_half(k, h, odd, sent, arrived, to):
        for i in range(h * quad + odd, (h + 1) * quad, 2):
            pass_on(k, i, sent.at[i], arrived.at[i], to).wait_recv()
        place(k, lambda rows: recv[k, rows, 0:feat], (h,), h == 1)
        contract(k, h * wide, main + n_sp * extra if h else wide, False)

    def relay(i):
        if i % 2 == 0:
            pass_on(left, i, l_send.at[i], fl_recv.at[i], right).wait_recv()
            c = pass_far(left, i, right)
        else:
            pass_on(right, i, r_send.at[i], fr_recv.at[i], left).wait_recv()
            c = pass_far(right, i, left)
        c.start()
        started.append(c)

    for c, n in zip(first_hop, next_hop):
        c.wait_recv()
        n.start()
    for i in range(groups):
        if i == 0:
            own.wait()
        if i == 3:
            for c in next_hop:
                c.wait_recv()
            for at in range(0, main, block):
                send_far[at : at + block, :] = mm(picked[at : at + block, :], x_far[...]).astype(
                    BF16
                )
            kept = pl.ds(pl.multiple_of(me * MAIN, MAIN), MAIN)
            recv_far[kept, :] = send_far[kept, :]
            for n in range(1, n_sp):
                c = hand_over(taker(n // per, n % per), n)
                c.start()
                started.append(c)
        for k in range(per):
            source = group_of(i) * per + k
            if i == 0:

                @pl.when(source != me)
                def _():
                    arrival(source).wait_recv()
            else:
                arrival(source).wait_recv()
        for c in (
            pass_on(tp, i, r_send.at[i], fl_recv.at[i], right),
            pass_on(tp, i, l_send.at[i], fr_recv.at[i], left),
        ):
            c.start()
            started.append(c)
        if i == quad - 1:
            for n in range(quad):
                relay(n)

    for c in loads:
        c.wait()
    place(tp, lambda rows: recv[tp, rows, 0:feat], (0, 1), True)
    contract(tp, 0, main + n_sp * extra, True)
    near_half(left, 0, 1, l_send, fl_recv, right)
    near_half(right, 0, 0, r_send, fr_recv, left)
    for d in range(1, n_sp):
        source = lax.rem(me + d, n_sp)
        copy_to(stat.at[0], stats.at[source], s_send.at[0], s_recv.at[source], source, tp).wait_recv()
    carry = jnp.zeros((1, u.shape[1]), F32)
    for s in range(n_sp):
        carry = jnp.where(s < me, stats[s, 0:1, :] * carry + stats[s, 1:2, :], carry)
    states = local + gain * carry
    row = lax.broadcasted_iota(jnp.int32, states.shape, 0)
    prev = jnp.where(row == 0, carry, pltpu.roll(states, 1, 0))
    gelu, slope = gelu_both(ogl_ref[...].astype(F32))
    lru_ref[...] = (states * gelu).astype(BF16)
    rec_ref[0] = decay
    rec_ref[1] = gelu
    rec_ref[2] = states * slope
    rec_ref[3] = admit * scale
    rec_ref[4] = (
        (prev * decay - uf * admit * decay * decay / scale) * (-8.0 * base) * forget * (1.0 - forget)
    )
    rec_ref[5] = uf * scale * admit * (1.0 - admit)

    outs = []

    def put(src, dst):
        outs.append(pltpu.make_async_copy(src, dst, out_sems.at[len(outs)]))
        outs[-1].start()

    strip = 32

    def activate(i, c):
        at = pl.ds(pl.multiple_of(i * strip, strip), strip)
        gate = acc_g[at, :]
        up = acc_u[at, :]
        d_hidden = acc_d[at, :]
        sig = jax.nn.sigmoid(gate)
        silu = gate * sig
        hid[at, :] = (silu * up).astype(BF16)
        dg[at, :] = (d_hidden * up * sig * (1.0 + gate * (1.0 - sig))).astype(BF16)
        du[at, :] = (d_hidden * silu).astype(BF16)
        return c

    def back_to(k, lo, hi, store):
        def columns(at, size):
            here = pl.ds(pl.multiple_of(k * feat + at, LANE), size)
            store(
                pl.ds(at, size),
                mm(dg[lo:hi, :], wg[here, :], 1, 1) + mm(du[lo:hi, :], wu[here, :], 1, 1),
            )

        in_blocks(columns, feat)

    slots = rows_ref.shape[0]
    crossing = []

    def finish_far(h):
        lo, hi = (wide, slots) if h else (0, wide)
        for i in range(h * quad, (h + 1) * quad):
            pass_far(far, i, right).wait_recv()
            for k in range(per):
                source = group_of(i) * per + k
                if i == 0:

                    @pl.when(source != me)
                    def _():
                        handed(source).wait_recv()
                else:
                    handed(source).wait_recv()
        place(far, lambda rows: recv_far[rows, :], (h,), h == 1)
        if h == 1:
            put(rows_ref, rows_out)
            put(cot_ref, cot_out)
            put(rec_ref, rec_out)
            put(lru_ref, lru_out)
            put(stats, gain_out)
        contract(far, lo, hi, False)
        lax.fori_loop(lo // strip, hi // strip, activate, 0)

        def to_far(here, value):
            far_out[lo:hi, here] = value.astype(BF16)

        back_to(far, lo, hi, to_far)
        cut = (hi - lo) // 2
        for n, (at, to) in enumerate(((lo, right), (lo + cut, left))):
            rows = pl.ds(at, cut)
            c = copy_to(
                far_out.at[rows], far_in.at[rows], f_send.at[2 * h + n], f_recv.at[2 * h + n], me, to
            )
            crossing.append((c, n, at, at + cut))

    def finish_near(h):
        lo, hi = (wide, slots) if h else (0, wide)

        def to_own(here, value):
            own_sum[lo:hi, here] = value.astype(BF16)

        def to_right(here, value):
            right_dx[lo:hi, here] = value

        def to_left(here, value):
            left_dx[lo:hi, here] = value

        back_to(tp, lo, hi, to_own)
        back_to(right, lo, hi, to_right)
        back_to(left, lo, hi, to_left)

    def put_acts(lo, hi):
        rows = pl.ds(lo, hi - lo)
        for src, dst in ((hid, hid_out), (dg, dg_out), (du, du_out)):
            put(src.at[rows], dst.at[rows])

    finish_far(0)
    put_acts(0, wide)
    relay(quad)
    relay(quad + 1)
    finish_near(0)
    relay(quad + 2)
    relay(quad + 3)
    for c in crossing:
        c[0].start()
    near_half(left, 1, 1, l_send, fl_recv, right)
    near_half(right, 1, 0, r_send, fr_recv, left)
    finish_far(1)
    for c in crossing[2:]:
        c[0].start()
    put_acts(wide, slots)
    finish_near(1)
    put(own_sum, own_out)
    for c, n, lo, hi in crossing:
        mine = bwd_sum if n == 0 else fwd_sum
        total = fwd_sum if n == 0 else bwd_sum
        mine[lo:hi, :] = (left_dx if n == 0 else right_dx)[lo:hi, :].astype(BF16)
        c.wait_recv()
        total[lo:hi, :] = (
            (right_dx if n == 0 else left_dx)[lo:hi, :] + far_in[lo:hi, :].astype(F32)
        ).astype(BF16)
        rows = pl.ds(lo, hi - lo)
        put(fwd_sum.at[rows], fwd_out.at[rows])
        put(bwd_sum.at[rows], bwd_out.at[rows])
    for c in outs:
        c.wait()
    for c in first_hop + next_hop + sends + told + started + [c[0] for c in crossing]:
        c.wait_send()


def dispatch(n_sp, x, g, rt, wt, u, ogl, wr, wi, cdp, eld, wg, wu, wd):
    tokens, feat = x.shape
    chans = u.shape[1]
    slots = n_sp * (MAIN + 2)
    width = 2 * feat + LANE
    hidden = wg.shape[2]
    shape = jax.ShapeDtypeStruct
    anywhere = pl.BlockSpec(memory_space=pl.ANY)
    vmem = pl.BlockSpec(memory_space=pltpu.VMEM)
    dma = pltpu.SemaphoreType.DMA
    return pl.pallas_call(
        functools.partial(dispatch_kernel, n_sp),
        out_shape=(
            shape((slots, 4 * feat), BF16),
            shape((slots, 4 * feat), BF16),
            shape((slots, hidden), BF16),
            shape((slots, hidden), BF16),
            shape((slots, hidden), BF16),
            shape((slots, feat), BF16),
            shape((slots, feat), BF16),
            shape((slots, feat), BF16),
            shape((6, tokens, chans), F32),
            shape((tokens, chans), BF16),
            shape((n_sp, 2, chans), F32),
        ),
        in_specs=[vmem] * 10 + [anywhere] * 3,
        out_specs=(anywhere,) * 11,
        scratch_shapes=[
            pltpu.VMEM((n_sp * MAIN, width), BF16),
            pltpu.VMEM((4, n_sp * MAIN, width), BF16),
            pltpu.VMEM((n_sp * MAIN, tokens), BF16),
            pltpu.VMEM((2, tokens // 2, feat), BF16),
            pltpu.VMEM((tokens, feat), BF16),
            pltpu.VMEM((n_sp * MAIN, feat), BF16),
            pltpu.VMEM((n_sp * MAIN, feat), BF16),
            dma((4,)),
            dma((4,)),
            dma((n_sp,)),
            dma((n_sp,)),
            pltpu.VMEM((n_sp * MAIN, LANE), F32),
            pltpu.VMEM((1, 2, chans), F32),
            pltpu.VMEM((n_sp, 2, chans), F32),
            pltpu.VMEM((4 * feat, hidden), BF16),
            pltpu.VMEM((4 * feat, hidden), BF16),
            pltpu.VMEM((hidden, 4 * feat), BF16),
            pltpu.VMEM((slots, 4 * feat), BF16),
            pltpu.VMEM((slots, 4 * feat), BF16),
            pltpu.VMEM((slots, hidden), F32),
            pltpu.VMEM((slots, hidden), F32),
            pltpu.VMEM((slots, hidden), F32),
            pltpu.VMEM((slots, hidden), BF16),
            pltpu.VMEM((slots, hidden), BF16),
            pltpu.VMEM((slots, hidden), BF16),
            pltpu.VMEM((slots, feat), BF16),
            pltpu.VMEM((slots, feat), BF16),
            pltpu.VMEM((slots, feat), F32),
            pltpu.VMEM((slots, feat), F32),
            pltpu.VMEM((slots, feat), BF16),
            pltpu.VMEM((slots, feat), BF16),
            pltpu.VMEM((slots, feat), BF16),
            pltpu.VMEM((6, tokens, chans), F32),
            pltpu.VMEM((tokens, chans), BF16),
            dma((3,)),
            dma((20,)),
            dma((4,)),
            dma((4,)),
            dma((n_sp,)),
            dma((n_sp,)),
            dma,
            dma((8,)),
            dma((8,)),
            dma((8,)),
            dma((8,)),
            dma((8,)),
            dma((8,)),
            dma((n_sp,)),
            dma((n_sp,)),
        ],
        compiler_params=pltpu.CompilerParams(
            collective_id=0, has_side_effects=True, vmem_limit_bytes=60 * 1024 * 1024
        ),
        name="dispatch",
    )(x, g, rt, wt, u, ogl, wr, wi, cdp, eld, wg, wu, wd)


def tail_kernel(
    n_sp,
    own_ref,
    fwd_ref,
    bwd_ref,
    og_ref,
    routes_ref,
    wout_ref,
    wr_ref,
    wi_ref,
    rec_ref,
    lru_ref,
    gain_ref,
    gop_ref,
    gin_ref,
    ggp_ref,
    sg_ref,
    rext,
    arr,
    full,
    prod,
    pair,
    summed,
    owned,
    term,
    terms,
    m_send,
    m_recv,
    own_sems,
    a_send,
    fl_recv,
    fr_recv,
    ff_recv,
    p_send,
    p_recv,
    o_send,
    o_recv,
    t_send,
    t_recv,
):
    me, tp = lax.axis_index("sp"), lax.axis_index("tp")
    right, left, far = (lax.rem(tp + k, 4) for k in (1, 3, 2))
    core = lax.rem(me, 2)
    chip = me // 2
    partner = me + 1 - 2 * core
    chips = n_sp // 2
    tokens, feat = og_ref.shape
    extra = 2
    cuts = feat // LANE
    greet([(lax.rem(me + d, n_sp), tp) for d in range(1, n_sp)] + [(me, right), (me, left)])

    main = n_sp * MAIN
    total = own_ref[...].astype(F32) + (fwd_ref[...].astype(F32) + bwd_ref[...].astype(F32))
    sg_ref[:, 0:feat] = total[0:main, :].astype(BF16)
    rext[...] = jnp.zeros_like(rext)
    for b in range(cuts):
        rext[pl.ds(b, n_sp * extra, stride=2 * cuts), :] = total[main:, b * LANE : (b + 1) * LANE]
    wide = main // 2
    for h in (0, 1):
        source_half = lax.rem(me // (n_sp // 2) + h, 2)
        sg_ref[h * wide : (h + 1) * wide, feat : feat + LANE] = rext[
            pl.ds(pl.multiple_of(source_half * wide, wide), wide), :
        ].astype(BF16)
    r0 = routes_ref[:, 0:1].astype(F32)
    r1 = routes_ref[:, 1:2].astype(F32)
    expert = iota((tokens, n_sp), 1)
    h0 = expert == r0
    h1 = expert == r1
    held = (h0 | h1).astype(F32).astype(BF16)
    before = (iota((tokens, tokens), 1) < iota((tokens, tokens), 0)).astype(F32).astype(BF16)
    rank = mm(before, held)
    k0 = jnp.sum(jnp.where(h0, rank, 0.0), axis=1, keepdims=True)
    k1 = jnp.sum(jnp.where(h1, rank, 0.0), axis=1, keepdims=True)
    m0 = jnp.where(k0 < MAIN, r0 * MAIN + k0, -1.0)
    m1 = jnp.where(k1 < MAIN, r1 * MAIN + k1, -1.0)
    e0 = jnp.where(k0 < MAIN, -1.0, r0 * extra + k0 - MAIN)
    e1 = jnp.where(k1 < MAIN, -1.0, r1 * extra + k1 - MAIN)
    slot = iota((tokens, main), 1)
    pick = ((slot == m0) | (slot == m1)).astype(F32).astype(BF16)
    slot = iota((tokens, n_sp * extra), 1)
    pickx = ((slot == e0) | (slot == e1)).astype(F32).astype(BF16)

    met(n_sp + 1)

    def rows_of(index, size):
        return pl.ds(pl.multiple_of(index * size, size), size)

    def held_for(peer):
        half = n_sp // 2
        at = lax.rem(peer // half + me // half, 2) * half + lax.rem(peer, half)
        return rows_of(at, MAIN)

    own = pltpu.make_async_copy(
        sg_ref.at[held_for(me)], arr.at[rows_of(me, MAIN)], own_sems.at[0]
    )

    def give(d, peer, source):
        return copy_to(
            sg_ref.at[held_for(peer)],
            arr.at[rows_of(source, MAIN)],
            m_send.at[d],
            m_recv.at[source],
            peer,
            tp,
        )

    sends = [give(d, lax.rem(me + d, n_sp), me) for d in range(1, n_sp)]
    own.start()
    for c in sends:
        c.start()
    own.wait()

    half = tokens // 2

    def piece(quarter, h, send_sem, recv_sem, to):
        ref = full.at[quarter, pl.ds(h * half, half)]
        return copy_to(ref, ref, a_send.at[send_sem], recv_sem, me, to)

    def from_left(h):
        return piece(left, h, 0, fl_recv.at[h], right)

    def from_right(h):
        return piece(right, h, 0, fr_recv.at[h], left)

    for d in range(1, n_sp):
        source = lax.rem(me + n_sp - d, n_sp)
        give(d, source, source).wait_recv()
    rext[...] = arr[:, feat : feat + LANE].astype(F32)
    for h in (0, 1):
        rows = slice(h * half, (h + 1) * half)
        back = mm(pick[rows, :], arr[:, 0:feat])
        backx = jnp.concatenate(
            [
                mm(pickx[rows, :], rext[pl.ds(b, n_sp * extra, stride=2 * cuts), :].astype(BF16))
                for b in range(cuts)
            ],
            axis=1,
        )
        full[tp, rows, :] = (og_ref[rows, :].astype(F32) + (back + backx)).astype(BF16)
    for h in (0, 1):
        sends.append(piece(tp, h, h, fl_recv.at[h], right))
        sends[-1].start()
        sends.append(piece(tp, 1 - h, 2 + h, fr_recv.at[1 - h], left))
        sends[-1].start()

    lru = lru_ref[...]
    share = chips // 4

    def use(quarter, n):
        part = full[quarter]
        spread = mm(part, lru, 0, 0).astype(BF16)
        mine = pl.ds(quarter * share, share)
        prod[mine] = spread.reshape(share, 2, feat // (2 * share), spread.shape[1])
        trade(quarter, n).start()
        return mm(part, wout_ref[pl.ds(pl.multiple_of(quarter * feat, feat), feat), :])

    def trade(quarter, n):
        mine = pl.ds(quarter * share, share)
        return copy_to(
            prod.at[mine, 1 - core], pair.at[mine], p_send.at[n], p_recv.at[n], partner, tp
        )

    def to_owner(at, source):
        return copy_to(
            summed.at[at], owned.at[source], o_send.at[at], o_recv.at[source], at * 2 + core, tp
        )

    def settle(quarter, n):
        trade(quarter, n).wait_recv()
        mine = pl.ds(quarter * share, share)
        summed[mine] = (prod[mine, core].astype(F32) + pair[mine].astype(F32)).astype(BF16)
        for k in range(share):
            at = quarter * share + k

            @pl.when(at != chip)
            def _():
                to_owner(at, chip).start()

    mixer = use(tp, 0)
    settle(tp, 0)
    from_left(0).wait_recv()
    sends.append(piece(left, 0, 4, ff_recv.at[0], right))
    sends[-1].start()
    from_right(1).wait_recv()
    sends.append(piece(right, 1, 5, ff_recv.at[1], left))
    sends[-1].start()
    from_left(1).wait_recv()
    mixer = mixer + use(left, 1)
    from_right(0).wait_recv()
    mixer = mixer + use(right, 2)
    settle(left, 1)
    settle(right, 2)
    for h in (0, 1):
        piece(far, h, 0, ff_recv.at[h], right).wait_recv()
    mixer = mixer + use(far, 3)

    decay = rec_ref[0]
    row = lax.broadcasted_iota(jnp.int32, decay.shape, 0)
    ggp_ref[...] = mixer * rec_ref[2]
    gain, tail = scan_rows(shifted(decay, -1, 1.0, row), mixer * rec_ref[1], -1)
    last = decay[0:1, :] * tail[0:1, :]
    term[0] = last
    terms[me] = last
    for d in range(1, n_sp):
        sends.append(
            copy_to(
                term.at[0], terms.at[me], t_send.at[d], t_recv.at[me], lax.rem(me + d, n_sp), tp
            )
        )
        sends[-1].start()

    settle(far, 3)
    owned[chip] = summed[chip]

    for d in range(1, n_sp):
        source = lax.rem(me + n_sp - d, n_sp)
        copy_to(term.at[0], terms.at[source], t_send.at[d], t_recv.at[source], source, tp).wait_recv()
    later = jnp.zeros_like(last)
    for s in range(n_sp - 1, -1, -1):
        later = jnp.where(s > me, gain_ref[s, 0:1, :] * later + terms[s], later)
    grad = tail + gain * later
    d_recall = (grad * rec_ref[4]).astype(BF16)
    d_admit = (grad * rec_ref[5]).astype(BF16)
    direct = grad * rec_ref[3]
    blocks = direct.shape[1] // LANE
    for b in range(blocks):
        cols = slice(b * LANE, (b + 1) * LANE)
        gin_ref[:, cols] = (
            direct[:, cols]
            + mm(d_recall[:, cols], wr_ref[tp * blocks + b], 1, 1)
            + mm(d_admit[:, cols], wi_ref[tp * blocks + b], 1, 1)
        )

    for d in range(1, chips):
        source = lax.rem(chip + chips - d, chips)
        to_owner(source, source).wait_recv()
    total = owned[0].astype(F32)
    for j in range(1, chips):
        total = total + owned[j].astype(F32)
    gop_ref[...] = total
    for n, quarter in enumerate((tp, left, right, far)):
        trade(quarter, n).wait_send()
    for d in range(1, chips):
        to_owner(lax.rem(chip + d, chips), chip).wait_send()
    for c in sends:
        c.wait_send()


def tail(n_sp, own, fwd, bwd, og, routes, wout, wr, wi, rec, lru, gains):
    tokens, feat = og.shape
    chans = lru.shape[1]
    chips = n_sp // 2
    share = wout.shape[0] // n_sp
    vmem = pl.BlockSpec(memory_space=pltpu.VMEM)
    dma = pltpu.SemaphoreType.DMA
    return pl.pallas_call(
        functools.partial(tail_kernel, n_sp),
        out_shape=(
            jax.ShapeDtypeStruct((share, chans), F32),
            jax.ShapeDtypeStruct((tokens, chans), F32),
            jax.ShapeDtypeStruct((tokens, chans), F32),
        ),
        in_specs=[vmem] * 11,
        out_specs=(vmem,) * 3,
        scratch_shapes=[
            pltpu.VMEM((n_sp * MAIN, feat + LANE), BF16),
            pltpu.VMEM((n_sp * MAIN, LANE), F32),
            pltpu.VMEM((n_sp * MAIN, feat + LANE), BF16),
            pltpu.VMEM((4, tokens, feat), BF16),
            pltpu.VMEM((chips, 2, share, chans), BF16),
            pltpu.VMEM((chips, share, chans), BF16),
            pltpu.VMEM((chips, share, chans), BF16),
            pltpu.VMEM((chips, share, chans), BF16),
            pltpu.VMEM((1, 1, chans), F32),
            pltpu.VMEM((n_sp, 1, chans), F32),
            dma((n_sp,)),
            dma((n_sp,)),
            dma((1,)),
            dma((6,)),
            dma((2,)),
            dma((2,)),
            dma((2,)),
            dma((4,)),
            dma((4,)),
            dma((chips,)),
            dma((chips,)),
            dma((n_sp,)),
            dma((n_sp,)),
        ],
        compiler_params=pltpu.CompilerParams(
            collective_id=1, has_side_effects=True, vmem_limit_bytes=40 * 1024 * 1024
        ),
        name="tail",
    )(own, fwd, bwd, og, routes, wout, wr, wi, rec, lru, gains)


def into_weights_kernel(x_ref, dg_ref, du_ref, gate_ref, up_ref):
    flipped = jnp.transpose(x_ref[...])
    gate_ref[...] = mm(flipped, dg_ref[...]).astype(BF16)
    up_ref[...] = mm(flipped, du_ref[...]).astype(BF16)


def from_weights_kernel(h_ref, c_ref, down_ref, flipped):
    @pl.when(pl.program_id(0) == 0)
    def _():
        flipped[...] = jnp.transpose(h_ref[...])

    down_ref[...] = mm(flipped[...], c_ref[...]).astype(BF16)


def weight_gradients(x, cot, hid, dg, du, block=512):
    slots, width = x.shape
    hidden = hid.shape[1]
    whole = pl.BlockSpec((slots, hidden), lambda i: (0, 0))
    strip = pl.BlockSpec((slots, block), lambda i: (0, i))
    flops = 2 * slots * width * hidden

    def cost(n):
        moved = 2 * (slots * width + n * slots * hidden + n * width * hidden)
        return pl.CostEstimate(flops=n * flops, bytes_accessed=moved, transcendentals=0)

    gate, up = pl.pallas_call(
        into_weights_kernel,
        grid=(width // block,),
        out_shape=(jax.ShapeDtypeStruct((width, hidden), BF16),) * 2,
        in_specs=[strip, whole, whole],
        out_specs=(pl.BlockSpec((block, hidden), lambda i: (i, 0)),) * 2,
        compiler_params=pltpu.CompilerParams(vmem_limit_bytes=40 * 1024 * 1024),
        cost_estimate=cost(2),
        name="grads_into",
    )(x, dg, du)
    down = pl.pallas_call(
        from_weights_kernel,
        grid=(width // block,),
        out_shape=jax.ShapeDtypeStruct((hidden, width), BF16),
        in_specs=[whole, strip],
        out_specs=pl.BlockSpec((hidden, block), lambda i: (0, i)),
        scratch_shapes=[pltpu.VMEM((hidden, slots), BF16)],
        compiler_params=pltpu.CompilerParams(vmem_limit_bytes=40 * 1024 * 1024),
        cost_estimate=cost(1),
        name="grads_from",
    )(hid, cot)
    return gate, up, down


def per_device(
    n_sp,
    middle_stream,
    output_gradient,
    routes,
    chosen_expert_weight,
    expert_gate_weight,
    expert_up_weight,
    expert_down_weight,
    recurrent_output_weight,
    recurrence_input,
    output_gate_logits,
    recurrence_gate_weight,
    input_gate_weight,
    channel_decay_param,
    extra_log_decay,
):
    inputs, cotangent, hidden, d_gate, d_up, own, fwd, bwd, rec, lru, gains = dispatch(
        n_sp,
        middle_stream,
        output_gradient,
        routes.T,
        chosen_expert_weight.T,
        recurrence_input,
        output_gate_logits,
        recurrence_gate_weight,
        input_gate_weight,
        channel_decay_param[None],
        extra_log_decay,
        expert_gate_weight,
        expert_up_weight,
        expert_down_weight,
    )
    fwd = lax.ppermute(fwd, "tp", [(k, (k + 1) % 4) for k in range(4)])
    bwd = lax.ppermute(bwd, "tp", [(k, (k + 3) % 4) for k in range(4)])
    grad_gate, grad_up, grad_down = weight_gradients(inputs, cotangent, hidden, d_gate, d_up)
    grad_out_proj, grad_input, grad_gate_pre = tail(
        n_sp,
        own,
        fwd,
        bwd,
        output_gradient,
        routes,
        recurrent_output_weight,
        recurrence_gate_weight,
        input_gate_weight,
        rec,
        lru,
        gains,
    )
    return (
        grad_gate[None],
        grad_up[None],
        grad_down[None],
        grad_out_proj,
        grad_input,
        grad_gate_pre,
    )


def solution(mesh):
    placed = (
        P("sp", "tp"),
        P("sp", "tp"),
        P("sp", None),
        P("sp", None),
        P("sp", None, "tp"),
        P("sp", None, "tp"),
        P("sp", "tp", None),
        P(None, "tp"),
        P("sp", "tp"),
        P("sp", "tp"),
        P(),
        P(),
        P("tp"),
        P("sp", "tp"),
    )
    return jax.shard_map(
        functools.partial(per_device, mesh.shape["sp"]),
        mesh=mesh,
        in_specs=placed,
        out_specs=(
            P("sp", None, "tp"),
            P("sp", None, "tp"),
            P("sp", "tp", None),
            P("sp", "tp"),
            P("sp", "tp"),
            P("sp", "tp"),
        ),
        check_vma=False,
    )
```
